256 devices in a mesh: sp: 32 (over z, y), tp: 8 (over x, core).
Axes of the slice: x: 4, y: 4, z: 8, core: 2. Of those that a mesh axis runs over, the one named last changes fastest.
Arguments:
- hidden: bfloat16 [4096, 2048], P('sp'), may hold values from -6 to 6
- value_weight: bfloat16 [2048, 4096], P(None, 'tp'), may hold values from -0.125 to 0.125
- key_vecs: bfloat16 [4096, 8, 128], P('sp', 'tp'), may hold values from -0.29882812 to 0.29882812
- queries: bfloat16 [4096, 8, 128], P('sp', 'tp'), may hold values from -0.29882812 to 0.29882812
- decay_pre: float32 [4096, 64], P('sp', 'tp'), may hold values from -4 to 4
- decay_rate: float32 [64], P('tp'), may hold values from 1.4648437e-05 to 0.0009033203
- cotangent: bfloat16 [4096, 64, 64], P('sp', 'tp'), may hold values from -1.1953125 to 1.1953125
Outputs:
- grad_keys: bfloat16 [4096, 8, 128], P('sp', 'tp')
- grad_queries: bfloat16 [4096, 8, 128], P('sp', 'tp')
- grad_decay: float32 [4096, 64], P('sp', 'tp')
- grad_hidden: bfloat16 [4096, 2048], P(('sp', 'tp'))
- grad_weight: float32 [2048, 4096], P('sp', 'tp')
The draws below stay inside these ranges and needn't reach their ends.
All inputs are finite; a program needn't handle non-finite values.
Results may differ from the reference program's by a relative error of at most 0.003.
Values sent between devices are 32-bit elements.
A program may use at most 64 MiB of HBM per device.

```python
import math
import jax
import jax.numpy as jnp
from jax import lax

D = 2048
HEADS = 64
HEAD_DIM = 64
GROUPS = 8
STATE = 128
TOK_DEV = 128
INNER = 4096
TOKENS = 4096


def shard_levels(rng, shape, pieces, smallest, top_value):
    level = 1.0
    for axis_at, shards_of in pieces:
        heights = jax.random.uniform(jax.random.fold_in(jax.random.fold_in(rng, 6), axis_at), (shards_of,), jnp.float32, smallest / len(pieces), top_value / len(pieces))
        level = level * jnp.repeat(jnp.exp(heights), shape[axis_at] // shards_of).reshape((-1,) + (1,) * (len(shape) - 1 - axis_at))
    return level


def bell_draw(rng, dims, scale, limit, shards=(), kind=jnp.bfloat16):
    entries = scale * jax.random.normal(rng, dims, jnp.float32)
    if shards:
        entries = entries * shard_levels(rng, dims, shards, -0.22, 0.18)
    return jnp.clip(entries, -limit, limit).astype(kind)


def setup_inputs(seed: int = 0) -> dict:
    splits = jax.random.split(jax.random.key(seed), 8)
    return {
        "hidden": bell_draw(splits[0], (TOKENS, D), 1.0, 6.0, ((0, 32),)),
        "value_weight": bell_draw(splits[1], (D, INNER), D ** -0.5, 0.125, ((1, 8),)),
        "key_vecs": bell_draw(splits[2], (TOKENS, GROUPS, STATE), 0.05, 0.29882812, ((0, 32), (1, 8))),
        "queries": bell_draw(splits[3], (TOKENS, GROUPS, STATE), 0.05, 0.29882812, ((0, 32), (1, 8))),
        "decay_pre": bell_draw(splits[4], (TOKENS, HEADS), 1.0, 4.0, ((0, 32), (1, 8)), jnp.float32),
        "decay_rate": jnp.clip(jnp.exp(math.log(0.0009033203) - 4.1217436 * jax.random.uniform(splits[5], (HEADS,), jnp.float32) ** shard_levels(splits[5], (HEADS,), ((0, 8),), -0.2, 0.2)), 1.4648437172581907e-05, 0.0009033203),
        "cotangent": bell_draw(splits[6], (TOKENS, HEADS, HEAD_DIM), 0.2, 1.1953125, ((0, 32), (1, 8))),
    }


highest = lax.Precision.HIGHEST

def local_mixer(values_f, keys_f, queries_f, decay_pre, decay_rate, state_in):
    heads_here = values_f.shape[1]
    per_group = heads_here // keys_f.shape[1]
    key_heads = jnp.repeat(keys_f, per_group, axis=1)
    query_heads = jnp.repeat(queries_f, per_group, axis=1)
    log_decay = -decay_rate[None, :] * jax.nn.softplus(decay_pre)
    cumulative = jnp.cumsum(log_decay, axis=0)
    length = values_f.shape[0]
    causal = jnp.tril(jnp.ones((length, length), dtype=bool))[None]
    across = cumulative.T[:, :, None] - cumulative.T[:, None, :]
    damping = jnp.where(causal, jnp.exp(jnp.where(causal, across, 0.0)), 0.0)
    scores = jnp.einsum('thn,shn->hts', query_heads, key_heads, precision=highest)
    outputs = jnp.einsum('hts,shp->thp', scores * damping, values_f, precision=highest)
    carried = jnp.einsum('thn,hpn->thp', query_heads, state_in, precision=highest)
    outputs = outputs + jnp.exp(cumulative)[:, :, None] * carried
    to_end = jnp.exp(cumulative[-1][None, :] - cumulative)
    state_out = jnp.exp(cumulative[-1])[:, None, None] * state_in + jnp.einsum('sh,shp,shn->hpn', to_end, values_f, key_heads, precision=highest)
    return (outputs, state_out)

def reference(hidden, value_weight, key_vecs, queries, decay_pre, decay_rate, cotangent):
    values = jnp.dot(hidden, value_weight, preferred_element_type=jnp.float32).astype(jnp.bfloat16)
    tokens_all = hidden.shape[0]
    block_count = tokens_all // TOK_DEV
    head_count = decay_rate.shape[0]

    def to_blocks(tensor):
        return tensor.reshape((block_count, TOK_DEV) + tensor.shape[1:])

    def whole_seq(values_in, keys_in, queries_in, pre_in):

        def advance(state_now, inputs):
            block_out, state_next = local_mixer(inputs[0], inputs[1], inputs[2], inputs[3], decay_rate, state_now)
            return (state_next, block_out)
        start_state = jnp.zeros((head_count, HEAD_DIM, STATE), jnp.float32)
        final_state, block_outs = lax.scan(advance, start_state, (to_blocks(values_in), to_blocks(keys_in), to_blocks(queries_in), to_blocks(pre_in)))
        return block_outs.reshape((tokens_all,) + block_outs.shape[2:])
    values_f = values.reshape(tokens_all, head_count, HEAD_DIM).astype(jnp.float32)
    primal, pullback = jax.vjp(whole_seq, values_f, key_vecs.astype(jnp.float32), queries.astype(jnp.float32), decay_pre)
    grad_values, grad_keys, grad_queries, grad_decay = pullback(cotangent.astype(jnp.float32))
    grad_flat = grad_values.reshape(tokens_all, -1).astype(jnp.bfloat16)
    grad_hidden = lax.dot_general(grad_flat, value_weight, (((1,), (1,)), ((), ())), preferred_element_type=jnp.float32).astype(jnp.bfloat16)
    grad_weight = lax.dot_general(hidden, grad_flat, (((0,), (0,)), ((), ())), preferred_element_type=jnp.float32)
    return (grad_keys.astype(jnp.bfloat16), grad_queries.astype(jnp.bfloat16), grad_decay, grad_hidden, grad_weight)
```

```python
import functools

import jax
import jax.numpy as jnp
from jax import lax
from jax.experimental import pallas as pl
from jax.experimental.pallas import tpu as pltpu
from jax.sharding import PartitionSpec as P

MESH = pl.DeviceIdType.MESH
F32 = jnp.float32
BF16 = jnp.bfloat16


def inner_size(count):
    size = 1
    while size * size * 4 <= count:
        size *= 2
    while count % size:
        size -= 1
    return size


def remote(src, dst, send, recv, axis, index):
    return pltpu.make_async_remote_copy(
        src_ref=src, dst_ref=dst, send_sem=send, recv_sem=recv, device_id={axis: index}, device_id_type=MESH
    )


def scan_kernel(ny, nz, ntp, both_ref, dec_ref, ht_ref, out_ref, hcol_ref,
                ybuf, ydec, tz, zbuf, cz, zcar, ob, scr, hg,
                dsend, drecv, ysend, yrecv, tsend, trecv, csend, crecv, osend, orecv, hsend, hrecv, fsend, frecv):
    me = lax.axis_index("sp")
    mine = lax.axis_index("tp")
    z, y = me // ny, me % ny
    heads = both_ref.shape[0]
    hq = heads // ny
    pr = zbuf.shape[3]
    state = both_ref.shape[3]
    halves = 2 if ntp % 2 == 0 else 1
    half = mine % halves
    other = mine + 1 - 2 * half
    hz = nz // halves
    ydev = [z * ny + (y + dy) % ny for dy in range(ny)]
    zdev = [((z + dz) % nz) * ny + y for dz in range(nz)]

    barrier = pltpu.get_barrier_semaphore()
    for dev in ydev[1:] + zdev[1:]:
        pl.semaphore_signal(barrier, inc=1, device_id={"sp": dev}, device_id_type=MESH)
    if halves == 2:
        pl.semaphore_signal(barrier, inc=1, device_id={"tp": other}, device_id_type=MESH)
    pl.semaphore_wait(barrier, ny - 1 + nz - 1 + halves - 1)

    def dcopy(dy, arrive=False):
        there = (y + dy) % ny
        slot = there if arrive else y
        return remote(dec_ref.at[pl.ds(there * hq, hq)], ydec.at[slot], dsend.at[there], drecv.at[slot], "sp", ydev[dy])

    def ycopy(h, dy, arrive=False):
        there = (y + dy) % ny
        slot = there if arrive else y
        return remote(both_ref.at[there * hq + h], ybuf.at[slot, h], ysend.at[there, h], yrecv.at[slot, h], "sp", ydev[dy])

    def tcopy(h, dz, arrive=False):
        there = (z + dz) % nz
        slot = there if arrive else z
        return remote(tz.at[there, h], zbuf.at[slot, h], tsend.at[there, h], trecv.at[slot, h], "sp", zdev[dz])

    def ccopy(h, dz, arrive=False):
        there = (z + dz) % nz
        slot = there if arrive else z
        return remote(cz.at[there, h], zcar.at[slot, h], csend.at[there, h], crecv.at[slot, h], "sp", zdev[dz])

    def ocopy(h, dy, arrive=False):
        there = (y + dy) % ny
        slot = there if arrive else y
        return remote(ob.at[there, h], scr.at[slot, h], osend.at[there, h], orecv.at[slot, h], "sp", ydev[dy])

    def part(k):
        return pl.ds(pl.multiple_of(k * hz, hz), hz)

    def hcopy(dy, arrive=False):
        there = (y + dy) % ny
        slot = there if arrive else y
        return remote(ht_ref.at[there, part(half)], hg.at[slot, part(half)], hsend.at[there], hrecv.at[slot], "sp", ydev[dy])

    def share(dy, which):
        there = (y + dy) % ny
        block = hg.at[there, part(which)]
        return remote(block, block, fsend.at[there], frecv.at[there], "tp", other)

    for dy in range(1, ny):
        dcopy(dy).start()
    for h in range(hq):
        for dy in range(1, ny):
            ycopy(h, dy).start()
    for dy in range(1, ny):
        hcopy(dy).start()

    ydec[y] = dec_ref[pl.ds(y * hq, hq)]
    ybuf[y] = both_ref[pl.ds(y * hq, hq)]
    for dy in range(1, ny):
        dcopy(dy, True).wait_recv()

    for h in range(hq):
        for dy in range(1, ny):
            ycopy(h, dy, True).wait_recv()
        up = ybuf[0, h, 0]
        down = ybuf[ny - 1, h, 1]
        prod = ydec[0, h]
        for yy in range(1, ny):
            up = ydec[yy, h][:1] * up + ybuf[yy, h, 0]
            down = ydec[ny - 1 - yy, h][:1] * down + ybuf[ny - 1 - yy, h, 1]
            prod = prod * ydec[yy, h]
        for p in range(nz):
            tz[p, h, 0] = up[p * pr:(p + 1) * pr]
            tz[p, h, 1] = down[p * pr:(p + 1) * pr]
            tz[p, h, 2] = prod[:pr]
        for dz in range(1, nz):
            tcopy(h, dz).start()
        zbuf[z, h] = tz[z, h]

    for h in range(hq):
        for dz in range(1, nz):
            tcopy(h, dz, True).wait_recv()
        run = jnp.zeros((pr, state), F32)
        for zz in range(nz):
            cz[zz, h, 0] = run
            run = zbuf[zz, h, 2] * run + zbuf[zz, h, 0]
        run = jnp.zeros((pr, state), F32)
        for zz in reversed(range(nz)):
            cz[zz, h, 1] = run
            run = zbuf[zz, h, 2] * run + zbuf[zz, h, 1]
        for dz in range(1, nz):
            ccopy(h, dz).start()
        zcar[z, h] = cz[z, h]

    for h in range(hq):
        for dz in range(1, nz):
            ccopy(h, dz, True).wait_recv()
        now = zcar[:, h, 0].reshape(nz * pr, state)
        for yy in range(ny):
            ob[yy, h, 0] = now
            now = ydec[yy, h][:1] * now + ybuf[yy, h, 0]
        now = zcar[:, h, 1].reshape(nz * pr, state)
        for yy in reversed(range(ny)):
            ob[yy, h, 1] = now
            now = ydec[yy, h][:1] * now + ybuf[yy, h, 1]
        for dy in range(1, ny):
            ocopy(h, dy).start()
        scr[y, h] = ob[y, h]

    length = hg.shape[3]
    for dy in range(1, ny):
        hcopy(dy, True).wait_recv()
        if halves == 2:
            share(dy, half).start()
    hcol_ref[:, :, pl.ds(pl.multiple_of(y * length, 128), length)] = ht_ref[y].astype(BF16)
    for dy in range(1, ny):
        there = (y + dy) % ny
        if halves == 2:
            share(dy, 1 - half).wait_recv()
        hcol_ref[:, :, pl.ds(pl.multiple_of(there * length, 128), length)] = hg[there].astype(BF16)

    for h in range(hq):
        for dy in range(1, ny):
            ocopy(h, dy, True).wait_recv()
    for yy in range(ny):
        out_ref[yy * hq:(yy + 1) * hq] = scr[yy]

    for dy in range(1, ny):
        dcopy(dy).wait_send()
        hcopy(dy).wait_send()
        if halves == 2:
            share(dy, half).wait_send()
    for h in range(hq):
        for dy in range(1, ny):
            ycopy(h, dy).wait_send()
            ocopy(h, dy).wait_send()
        for dz in range(1, nz):
            tcopy(h, dz).wait_send()
            ccopy(h, dz).wait_send()


def grads_kernel(ny, nz, ntp, width, gv_ref, hct_ref, ghp_ref, gw_ref, gh_ref,
                 gath, part, ring, pland, red, xland,
                 ysend, yrecv, rsend, rrecv, psend, precv, xsend, xrecv):
    me = lax.axis_index("sp")
    mine = lax.axis_index("tp")
    z, y = me // ny, me % ny
    rows = gw_ref.shape[0]
    chunks = gv_ref.shape[1] // width
    length = gv_ref.shape[0]
    halves = 2 if ntp % 2 == 0 else 1
    nx = ntp // halves
    core = mine % halves
    x = mine // halves
    ydev = [z * ny + (y + dy) % ny for dy in range(ny)]
    zup, zdn = ((z + 1) % nz) * ny + y, ((z + nz - 1) % nz) * ny + y

    barrier = pltpu.get_barrier_semaphore()
    for dev in ydev[1:] + [zup, zdn]:
        pl.semaphore_signal(barrier, inc=1, device_id={"sp": dev}, device_id_type=MESH)
    if halves == 2:
        pl.semaphore_signal(barrier, inc=1, device_id={"tp": mine + 1 - 2 * core}, device_id_type=MESH)
    for dx in range(1, nx):
        pl.semaphore_signal(barrier, inc=1, device_id={"tp": ((x + dx) % nx) * halves + core}, device_id_type=MESH)
    pl.semaphore_wait(barrier, ny - 1 + 2 + halves - 1 + nx - 1)

    def ycopy(c, dy, arrive=False):
        there = (y + dy) % ny
        slot = there if arrive else y
        return remote(gath.at[slot, c], gath.at[slot, c], ysend.at[there, c], yrecv.at[slot, c], "sp", ydev[dy])

    def pair():
        return remote(ghp_ref.at[1 - core], pland, psend, precv, "tp", mine + 1 - 2 * core)

    def xcopy(dx, arrive=False):
        there = (x + dx) % nx
        slot = there if arrive else x
        return remote(red.at[there], xland.at[slot], xsend.at[there], xrecv.at[slot], "tp", there * halves + core)

    def reach(c, d):
        far = nz // 2
        return far if (c + d) % 2 == 0 else nz - 1 - far

    def rcopy(c, d, j):
        target = (z + reach(c, d)) % nz if d == 0 else (z + nz - reach(c, d)) % nz
        src = part.at[c, target] if j == 0 else ring.at[d, c, j - 1]
        return remote(src, ring.at[d, c, j], rsend.at[d, c, j], rrecv.at[d, c, j], "sp", zup if d == 0 else zdn)

    for c in range(chunks):
        gath[y, c] = gv_ref[:, c * width:(c + 1) * width]
        for dy in range(1, ny):
            ycopy(c, dy).start()
    if halves == 2:
        pair().start()

    def multiply(c):
        for dy in range(1, ny):
            ycopy(c, dy, True).wait_recv()
        block = gath[:, c].reshape(ny * length, width).astype(BF16)
        part[c] = jnp.dot(hct_ref[...], block, preferred_element_type=F32).reshape(nz, rows, width)
        for d in range(2):
            if reach(c, d) > 0:
                rcopy(c, d, 0).start()

    def hop(c, d, j):
        rcopy(c, d, j).wait_recv()
        left = reach(c, d) - 1 - j
        if left > 0:
            target = (z + left) % nz if d == 0 else (z + nz - left) % nz
            ring[d, c, j] = ring[d, c, j] + part[c, target]
            rcopy(c, d, j + 1).start()

    def pairs():
        if halves == 2:
            pair().wait_recv()
            red[...] = ghp_ref[core] + pland[...]
        else:
            red[...] = ghp_ref[0]
        for dx in range(1, nx):
            xcopy(dx).start()

    tasks = [(0.0, pairs)]
    for c in range(chunks):
        ready = 4.0 + 2.5 * c
        tasks.append((ready, functools.partial(multiply, c)))
        for d in range(2):
            for j in range(reach(c, d)):
                tasks.append((ready + 3.4 * (j + 1), functools.partial(hop, c, d, j)))
    for _, task in sorted(tasks, key=lambda item: item[0]):
        task()

    for c in range(chunks):
        total = part[c, z]
        for d in range(2):
            if reach(c, d) > 0:
                total = total + ring[d, c, reach(c, d) - 1]
        gw_ref[:, c * width:(c + 1) * width] = total

    total = red[x]
    for dx in range(1, nx):
        xcopy(dx, True).wait_recv()
        total = total + xland[(x + dx) % nx]
    gh_ref[...] = total.astype(gh_ref.dtype)

    for c in range(chunks):
        for dy in range(1, ny):
            ycopy(c, dy).wait_send()
        for d in range(2):
            for j in range(reach(c, d)):
                rcopy(c, d, j).wait_send()
    if halves == 2:
        pair().wait_send()
    for dx in range(1, nx):
        xcopy(dx).wait_send()


VM = pl.BlockSpec(memory_space=pltpu.VMEM)
LIMIT = 48 * 1024 * 1024


def split(x):
    hi = lax.reduce_precision(x, 8, 7)
    return hi.astype(BF16), (x - hi).astype(BF16)


def two_pass(spec, x, y):
    hi, lo = split(x)
    return jnp.einsum(spec, hi, y, preferred_element_type=F32) + jnp.einsum(spec, lo, y, preferred_element_type=F32)


def per_device(sp, tp, hidden, value_weight, key_vecs, queries, decay_pre, decay_rate, cotangent):
    length = hidden.shape[0]
    heads = decay_rate.shape[0]
    head_width = cotangent.shape[2]
    groups = key_vecs.shape[1]
    state = key_vecs.shape[2]
    per = heads // groups
    features = hidden.shape[1]
    columns = value_weight.shape[1]
    ny = inner_size(sp)
    nz = sp // ny
    values = jnp.dot(hidden, value_weight, preferred_element_type=F32).astype(BF16)
    v = values.reshape(length, groups, per, head_width)
    cot = cotangent.reshape(length, groups, per, head_width)
    log_decay = -decay_rate[None, :] * jax.nn.softplus(decay_pre)
    tri = jnp.tril(jnp.ones((length, length), F32))
    cum = jnp.dot(tri, log_decay, precision=lax.Precision.HIGHEST)
    tot = cum[-1]
    to_end = jnp.exp(tot[None] - cum).reshape(length, groups, per, 1)
    ecum = jnp.exp(cum).reshape(length, groups, per, 1)
    local_state = two_pass("sgip,sgn->gipn", to_end * v.astype(F32), key_vecs)
    local_pull = two_pass("sgip,sgn->gipn", ecum * cot.astype(F32), queries)
    both = jnp.stack([local_state, local_pull], axis=2).reshape(heads, 2, head_width, state)
    rows = features // sp
    hq = heads // ny
    pr = head_width // nz
    halves = 2 if tp % 2 == 0 else 1
    dec = jnp.broadcast_to(jnp.exp(tot)[:, None, None], (heads, pr, state))
    ht = jnp.transpose(hidden.T.astype(F32).reshape(nz, ny, rows, length), (1, 0, 2, 3))
    scanned, hcol = pl.pallas_call(
        functools.partial(scan_kernel, ny, nz, tp),
        out_shape=(
            jax.ShapeDtypeStruct(both.shape, F32),
            jax.ShapeDtypeStruct((nz, rows, ny * length), BF16),
        ),
        in_specs=[VM] * 3,
        out_specs=(VM, VM),
        scratch_shapes=[
            pltpu.VMEM((ny, hq) + both.shape[1:], F32),
            pltpu.VMEM((ny, hq, pr, state), F32),
            pltpu.VMEM((nz, hq, 3, pr, state), F32),
            pltpu.VMEM((nz, hq, 3, pr, state), F32),
            pltpu.VMEM((nz, hq, 2, pr, state), F32),
            pltpu.VMEM((nz, hq, 2, pr, state), F32),
            pltpu.VMEM((ny, hq) + both.shape[1:], F32),
            pltpu.VMEM((ny, hq) + both.shape[1:], F32),
            pltpu.VMEM((ny, nz, rows, length), F32),
            pltpu.SemaphoreType.DMA((ny,)),
            pltpu.SemaphoreType.DMA((ny,)),
            pltpu.SemaphoreType.DMA((ny, hq)),
            pltpu.SemaphoreType.DMA((ny, hq)),
            pltpu.SemaphoreType.DMA((nz, hq)),
            pltpu.SemaphoreType.DMA((nz, hq)),
            pltpu.SemaphoreType.DMA((nz, hq)),
            pltpu.SemaphoreType.DMA((nz, hq)),
            pltpu.SemaphoreType.DMA((ny, hq)),
            pltpu.SemaphoreType.DMA((ny, hq)),
            pltpu.SemaphoreType.DMA((ny,)),
            pltpu.SemaphoreType.DMA((ny,)),
            pltpu.SemaphoreType.DMA((ny,)),
            pltpu.SemaphoreType.DMA((ny,)),
        ],
        compiler_params=pltpu.CompilerParams(collective_id=0, has_side_effects=True, vmem_limit_bytes=LIMIT),
        name="scan_states",
    )(both, dec, ht)
    state_in = scanned[:, 0].reshape(groups, per, head_width, state)
    state_grad = scanned[:, 1].reshape(groups, per, head_width, state)

    cum_h = cum.T
    causal = jnp.tril(jnp.ones((length, length), dtype=bool))[None]
    across = cum_h[:, :, None] - cum_h[:, None, :]
    damping = jnp.where(causal, jnp.exp(jnp.where(causal, across, 0.0)), 0.0).reshape(groups, per, length, length)
    scores = jnp.einsum("tgn,sgn->gts", queries, key_vecs, preferred_element_type=F32)
    pair = jnp.einsum("tgip,sgip->gits", cot, v, preferred_element_type=F32)
    dscore = pair * damping
    flux = dscore * scores[:, None]
    net = (jnp.sum(flux, axis=3) - jnp.sum(flux, axis=2)).reshape(heads, length).T
    dsum = jnp.sum(dscore, axis=1)
    mixed = scores[:, None] * damping
    gq_heads = ecum * two_pass("gipn,tgip->tgin", state_in, cot)
    gk_heads = to_end * two_pass("gipn,tgip->tgin", state_grad, v)
    gv = two_pass("gits,tgip->sgip", mixed, cot) + to_end * two_pass(
        "gipn,sgn->sgip", state_grad, key_vecs
    )
    gq = two_pass("gts,sgn->tgn", dsum, key_vecs) + jnp.sum(gq_heads, axis=2)
    gk = two_pass("gts,tgn->sgn", dsum, queries) + jnp.sum(gk_heads, axis=2)
    qgq = jnp.sum(gq_heads * queries.astype(F32)[:, :, None], axis=3).reshape(length, heads)
    kgk = jnp.sum(gk_heads * key_vecs.astype(F32)[:, :, None], axis=3).reshape(length, heads)
    through = jnp.exp(tot) * jnp.sum(state_in * state_grad, axis=(2, 3)).reshape(heads)
    suffix = jnp.dot(tri.T, net + qgq, precision=lax.Precision.HIGHEST)
    prefix = jnp.dot(tri - jnp.eye(length, dtype=F32), kgk, precision=lax.Precision.HIGHEST)
    grad_decay = (suffix + prefix + through[None]) * -decay_rate[None] * jax.nn.sigmoid(decay_pre)

    grad_flat = gv.reshape(length, columns).astype(BF16)
    ghp = lax.dot_general(grad_flat, value_weight, (((1,), (1,)), ((), ())), preferred_element_type=F32)
    width = min(columns, 128)
    chunks = columns // width
    own = length // tp
    far = nz // 2
    ghp = jnp.transpose(ghp.reshape(tp // halves, halves, own, features), (1, 0, 2, 3))
    grad_weight, grad_hidden = pl.pallas_call(
        functools.partial(grads_kernel, ny, nz, tp, width),
        out_shape=(
            jax.ShapeDtypeStruct((rows, columns), F32),
            jax.ShapeDtypeStruct((own, features), BF16),
        ),
        in_specs=[VM] * 3,
        out_specs=(VM, VM),
        scratch_shapes=[
            pltpu.VMEM((ny, chunks, length, width), F32),
            pltpu.VMEM((chunks, nz, rows, width), F32),
            pltpu.VMEM((2, chunks, far, rows, width), F32),
            pltpu.VMEM((tp // halves, own, features), F32),
            pltpu.VMEM((tp // halves, own, features), F32),
            pltpu.VMEM((tp // halves, own, features), F32),
            pltpu.SemaphoreType.DMA((ny, chunks)),
            pltpu.SemaphoreType.DMA((ny, chunks)),
            pltpu.SemaphoreType.DMA((2, chunks, far)),
            pltpu.SemaphoreType.DMA((2, chunks, far)),
            pltpu.SemaphoreType.DMA,
            pltpu.SemaphoreType.DMA,
            pltpu.SemaphoreType.DMA((tp // halves,)),
            pltpu.SemaphoreType.DMA((tp // halves,)),
        ],
        compiler_params=pltpu.CompilerParams(collective_id=1, has_side_effects=True, vmem_limit_bytes=LIMIT),
        name="weight_grads",
    )(grad_flat.astype(F32), hcol.reshape(nz * rows, ny * length), ghp)
    return (gq_cast(gk), gq_cast(gq), grad_decay, grad_hidden, grad_weight)


def gq_cast(x):
    return x.astype(BF16)


def solution(mesh):
    return jax.shard_map(
        functools.partial(per_device, mesh.shape["sp"], mesh.shape["tp"]),
        mesh=mesh,
        in_specs=(
            P("sp", None),
            P(None, "tp"),
            P("sp", "tp", None),
            P("sp", "tp", None),
            P("sp", "tp"),
            P("tp"),
            P("sp", "tp", None),
        ),
        out_specs=(
            P("sp", "tp", None),
            P("sp", "tp", None),
            P("sp", "tp"),
            P(("sp", "tp"), None),
            P("sp", "tp"),
        ),
        check_vma=False,
    )
```

```python
import functools

import jax
import jax.numpy as jnp
from jax import lax
from jax.experimental import pallas as pl
from jax.experimental.pallas import tpu as pltpu
from jax.sharding import PartitionSpec as P

MESH = pl.DeviceIdType.MESH
F32 = jnp.float32
BF16 = jnp.bfloat16
HIGH = lax.Precision.HIGHEST
LANES = 128
SUB = 8


def inner_size(count):
    size = 1
    while size * size * 4 <= count:
        size *= 2
    while count % size:
        size -= 1
    return size


def remote(src, dst, send, recv, axis, index):
    return pltpu.make_async_remote_copy(
        src_ref=src, dst_ref=dst, send_sem=send, recv_sem=recv, device_id={axis: index}, device_id_type=MESH
    )


def nn(a, b, precision=None):
    return jnp.dot(a, b, preferred_element_type=F32, precision=precision)


def nt(a, b, precision=None):
    return lax.dot_general(a, b, (((1,), (1,)), ((), ())), preferred_element_type=F32, precision=precision)


def split(x):
    hi = x.astype(BF16)
    return hi, (x - hi.astype(F32)).astype(BF16)


def mixer_kernel(ny, nz, ntp, hid_hbm, w_hbm, key_hbm, qry_hbm, pre_hbm, rate_ref, cot_hbm,
                 gk_ref, gq_ref, gd_ref, gh_ref, gw_ref,
                 hid, wt, key, qry, pre, cot,
                 ecot, tend, xval, damp, gvloc, gvb, kgs, rows8, cols8, gkl, gql,
                 sbuf, decb, ybuf, ydec, tz, zbuf, cz, zcar, ob, scr, ht, hg, hcol,
                 gath, part, ring, ghp, pland, red, xland,
                 insem, dsend, drecv, ysend, yrecv, tsend, trecv, csend, crecv, osend, orecv,
                 hsend, hrecv, fsend, frecv, gsend, grecv, rsend, rrecv, psend, precv, xsend, xrecv):
    me = lax.axis_index("sp")
    mine = lax.axis_index("tp")
    z, y = me // ny, me % ny
    length, features = hid.shape
    heads = rate_ref.shape[1]
    columns = cot.shape[1]
    width = columns // heads
    tiles = columns // LANES
    per = LANES // width
    state = key.shape[1]
    nr = state // nz
    rows = gw_ref.shape[0]
    own = gh_ref.shape[0]
    halves = 2 if ntp % 2 == 0 else 1
    core, x, nx = mine % halves, mine // halves, ntp // halves
    partner = mine + 1 - 2 * core
    hz = nz // halves
    steps = insem.shape[0] - 4
    depth = features // steps
    ydev = [z * ny + (y + dy) % ny for dy in range(ny)]
    zdev = [((z + dz) % nz) * ny + y for dz in range(nz)]

    small = [
        pltpu.make_async_copy(pre_hbm, pre, insem.at[0]),
        pltpu.make_async_copy(qry_hbm, qry, insem.at[1]),
        pltpu.make_async_copy(cot_hbm, cot, insem.at[2]),
        pltpu.make_async_copy(key_hbm, key, insem.at[3]),
    ]
    for copy in small:
        copy.start()
    wcopies, hcopies = [], []
    for k in range(steps):
        at = pl.ds(k * depth, depth)
        wcopies.append(pltpu.make_async_copy(w_hbm.at[at, :], wt.at[at, :], insem.at[4 + k]))
    hload = pltpu.make_async_copy(hid_hbm, hid, hsend.at[y])
    hload.start()
    for copy in wcopies:
        copy.start()

    barrier = pltpu.get_barrier_semaphore()
    for dev in ydev[1:] + zdev[1:]:
        pl.semaphore_signal(barrier, inc=1, device_id={"sp": dev}, device_id_type=MESH)
    if halves == 2:
        pl.semaphore_signal(barrier, inc=1, device_id={"tp": partner}, device_id_type=MESH)
    for dx in range(1, nx):
        pl.semaphore_signal(barrier, inc=1, device_id={"tp": ((x + dx) % nx) * halves + core}, device_id_type=MESH)

    def dcopy(dy, arrive=False):
        there = (y + dy) % ny
        slot = there if arrive else y
        return remote(decb.at[there], ydec.at[slot], dsend.at[there], drecv.at[slot], "sp", ydev[dy])

    def ycopy(m, dy, arrive=False):
        there = (y + dy) % ny
        slot = there if arrive else y
        return remote(sbuf.at[m, there], ybuf.at[m, slot], ysend.at[m, there], yrecv.at[m, slot], "sp", ydev[dy])

    def tcopy(m, dz, arrive=False):
        there = (z + dz) % nz
        slot = there if arrive else z
        return remote(tz.at[m, there], zbuf.at[m, slot], tsend.at[m, there], trecv.at[m, slot], "sp", zdev[dz])

    def ccopy(m, dz, arrive=False):
        there = (z + dz) % nz
        slot = there if arrive else z
        return remote(cz.at[m, there], zcar.at[m, slot], csend.at[m, there], crecv.at[m, slot], "sp", zdev[dz])

    def ocopy(m, dy, arrive=False):
        there = (y + dy) % ny
        slot = there if arrive else y
        return remote(ob.at[m, there], scr.at[m, slot], osend.at[m, there], orecv.at[m, slot], "sp", ydev[dy])

    def section(k):
        return pl.ds(pl.multiple_of(k * hz, hz), hz)

    def hcopy(dy, arrive=False):
        there = (y + dy) % ny
        slot = there if arrive else y
        return remote(
            ht.at[there, section(core)], hg.at[slot, section(core)], hsend.at[there], hrecv.at[slot], "sp", ydev[dy]
        )

    def share(dy, which):
        there = (y + dy) % ny
        block = hg.at[there, section(which)]
        return remote(block, block, fsend.at[there], frecv.at[there], "tp", partner)

    def gcopy(c, dy, arrive=False):
        there = (y + dy) % ny
        slot = there if arrive else y
        return remote(gath.at[slot, c], gath.at[slot, c], gsend.at[there, c], grecv.at[slot, c], "sp", ydev[dy])

    def pair():
        return remote(ghp.at[1 - core], pland, psend, precv, "tp", partner)

    def xcopy(dx, arrive=False):
        there = (x + dx) % nx
        slot = there if arrive else x
        return remote(red.at[there], xland.at[slot], xsend.at[there], xrecv.at[slot], "tp", there * halves + core)

    def reach(c, d):
        far = nz // 2
        return far if (c + d) % 2 == 0 else nz - 1 - far

    def rcopy(c, d, j):
        target = (z + reach(c, d)) % nz if d == 0 else (z + nz - reach(c, d)) % nz
        src = part.at[c, target] if j == 0 else ring.at[d, c, j - 1]
        return remote(
            src, ring.at[d, c, j], rsend.at[d, c, j], rrecv.at[d, c, j], "sp", zdev[1] if d == 0 else zdev[nz - 1]
        )

    row_at = lax.broadcasted_iota(jnp.int32, (length, length), 0)
    col_at = lax.broadcasted_iota(jnp.int32, (length, length), 1)
    eye = (row_at == col_at).astype(BF16)
    seg = (
        lax.broadcasted_iota(jnp.int32, (heads, columns), 1) // width
        == lax.broadcasted_iota(jnp.int32, (heads, columns), 0)
    ).astype(F32)
    lane = lax.broadcasted_iota(jnp.int32, (length, LANES), 1) // width

    def tile(q):
        return slice(q * LANES, (q + 1) * LANES)

    small[0].wait()
    p = pre[...]
    rate = rate_ref[...]
    log_decay = -rate * (jnp.maximum(p, 0.0) + jnp.log1p(jnp.exp(-jnp.abs(p))))
    cum = nn((row_at >= col_at).astype(F32), log_decay, HIGH)
    cumx = nn(cum, seg, HIGH)
    totx = cumx[length - 1:length]
    decx = jnp.exp(totx)
    small[1].wait()
    small[2].wait()
    ec = jnp.exp(cumx) * cot[...].astype(F32)
    ecot[...] = ec
    qryt = nt(eye, qry[...]).astype(BF16)
    hi, lo = split(ec)
    pull = nn(qryt, hi) + nn(qryt, lo)
    for q in range(tiles):
        sbuf[0, q] = pull[:, tile(q)]
        decb[q] = jnp.broadcast_to(decx[:, tile(q)], (SUB, LANES))

    pl.semaphore_wait(barrier, ny - 1 + nz - 1 + halves - 1 + nx - 1)
    for dy in range(1, ny):
        dcopy(dy).start()
        ycopy(0, dy).start()
    ydec[y] = decb[y]
    ybuf[0, y] = sbuf[0, y]

    tend[...] = jnp.exp(totx - cumx)
    small[3].wait()
    hload.wait()
    values = jnp.zeros((length, columns), F32)
    for k in range(steps):
        wcopies[k].wait()
        values = values + nn(hid[:, k * depth:(k + 1) * depth], wt[k * depth:(k + 1) * depth, :])
    vals = values.astype(BF16)
    xv = tend[...] * vals.astype(F32)
    xval[...] = xv
    keyt = nt(eye, key[...]).astype(BF16)
    hi, lo = split(xv)
    push = nn(keyt, hi) + nn(keyt, lo)
    for q in range(tiles):
        sbuf[1, q] = push[:, tile(q)]
    for dy in range(1, ny):
        ycopy(1, dy).start()
    ybuf[1, y] = sbuf[1, y]

    for b in range(features // LANES):
        block = nt(eye, hid[:, tile(b)])
        for i in range(LANES // rows):
            owner = b * LANES // rows + i
            ht[owner % ny, owner // ny] = block[i * rows:(i + 1) * rows]
    for dy in range(1, ny):
        hcopy(dy).start()
    hcol[:, :, pl.ds(pl.multiple_of(y * length, LANES), length)] = ht[y].astype(BF16)

    def stage_y(m):
        if m == 0:
            for dy in range(1, ny):
                dcopy(dy, True).wait_recv()
        for dy in range(1, ny):
            ycopy(m, dy, True).wait_recv()
        order = list(range(ny)) if m == 1 else list(reversed(range(ny)))
        run = ybuf[m, order[0]]
        for yy in order[1:]:
            run = ydec[yy][:1] * run + ybuf[m, yy]
        prod = ydec[0]
        for yy in range(1, ny):
            prod = prod * ydec[yy]
        for k in range(nz):
            tz[m, k, :nr] = run[k * nr:(k + 1) * nr]
            tz[m, k, nr:] = prod
        for dz in range(1, nz):
            tcopy(m, dz).start()
        zbuf[m, z] = tz[m, z]

    def stage_z(m):
        for dz in range(1, nz):
            tcopy(m, dz, True).wait_recv()
        run = jnp.zeros((nr, LANES), F32)
        for zz in (list(range(nz)) if m == 1 else list(reversed(range(nz)))):
            cz[m, zz] = run
            run = zbuf[m, zz, nr:nr + 1] * run + zbuf[m, zz, :nr]
        for dz in range(1, nz):
            ccopy(m, dz).start()
        zcar[m, z] = cz[m, z]

    def stage_c(m):
        for dz in range(1, nz):
            ccopy(m, dz, True).wait_recv()
        now = zcar[m].reshape(state, LANES)
        for yy in (list(range(ny)) if m == 1 else list(reversed(range(ny)))):
            ob[m, yy] = now
            now = ydec[yy][:1] * now + ybuf[m, yy]
        for dy in range(1, ny):
            ocopy(m, dy).start()
        scr[m, y] = ob[m, y]

    stage_y(0)

    cumt = nt((
        lax.broadcasted_iota(jnp.int32, (heads, heads), 0) == lax.broadcasted_iota(jnp.int32, (heads, heads), 1)
    ).astype(F32), cum, HIGH)
    causal = row_at <= col_at
    scores = nt(key[...], qry[...])
    for q in range(tiles):
        lefts, rights = [], []
        ct = cot[:, tile(q)]
        for i in range(per):
            h = q * per + i
            across = cumt[h:h + 1, :] - cum[:, h:h + 1]
            dm = jnp.where(causal, jnp.exp(jnp.where(causal, across, 0.0)), 0.0)
            damp[h] = dm
            lefts.extend(split(scores * dm))
            masked = jnp.where(lane == i, ct, jnp.zeros_like(ct))
            rights.extend([masked, masked])
        gvloc[q] = nn(jnp.concatenate(lefts, axis=1), jnp.concatenate(rights, axis=0))

    stage_y(1)

    dsum = jnp.zeros((length, length), F32)
    for q in range(tiles):
        vt = vals[:, tile(q)]
        both = nt(
            jnp.concatenate([jnp.where(lane == i, vt, jnp.zeros_like(vt)) for i in range(per)], axis=0),
            cot[:, tile(q)],
        )
        for i in range(per):
            h = q * per + i
            ds = both[i * length:(i + 1) * length] * damp[h]
            flux = ds * scores
            dsum = dsum + ds
            rows8[h:h + 1, :] = jnp.sum(flux, axis=0, keepdims=True)
            cols8[:, h:h + 1] = jnp.sum(flux, axis=1, keepdims=True)

    stage_z(0)

    hi, lo = split(dsum)
    gkl[...] = nn(hi, qry[...]) + nn(lo, qry[...])
    hi, lo = split(dsum.T)
    gql[...] = nn(hi, key[...]) + nn(lo, key[...])
    for dy in range(1, ny):
        hcopy(dy, True).wait_recv()
        if halves == 2:
            share(dy, core).start()

    stage_z(1)
    stage_c(0)

    for dy in range(1, ny):
        there = (y + dy) % ny
        if halves == 2:
            share(dy, 1 - core).wait_recv()
        hcol[:, :, pl.ds(pl.multiple_of(there * length, LANES), length)] = hg[there].astype(BF16)

    stage_c(1)

    for dy in range(1, ny):
        ocopy(0, dy, True).wait_recv()
    for q in range(tiles):
        hi, lo = split(scr[0, q])
        kg = nn(key[...], hi) + nn(key[...], lo)
        kgs[:, tile(q)] = kg
        gb = (gvloc[q] + tend[:, tile(q)] * kg).astype(BF16)
        gvb[:, tile(q)] = gb
        gath[y, q] = gb.astype(F32)
        for dy in range(1, ny):
            gcopy(q, dy).start()

    def multiply(c):
        for dy in range(1, ny):
            gcopy(c, dy, True).wait_recv()
        block = gath[:, c].reshape(ny * length, LANES).astype(BF16)
        part[c] = nn(hcol[...].reshape(nz * rows, ny * length), block).reshape(nz, rows, LANES)
        for d in range(2):
            if reach(c, d) > 0:
                rcopy(c, d, 0).start()

    def hop(c, d, j):
        rcopy(c, d, j).wait_recv()
        left = reach(c, d) - 1 - j
        if left > 0:
            target = (z + left) % nz if d == 0 else (z + nz - left) % nz
            ring[d, c, j] = ring[d, c, j] + part[c, target]
            rcopy(c, d, j + 1).start()

    def project():
        for t in range(ntp):
            block = nt(gvb[t * own:(t + 1) * own, :], wt[...]) if own % 16 else None
            if block is not None:
                ghp[t % halves, t // halves] = block
        if own % 16 == 0:
            block = nt(gvb[...], wt[...])
            for t in range(ntp):
                ghp[t % halves, t // halves] = block[t * own:(t + 1) * own]
        if halves == 2:
            pair().start()

    def pairs():
        if halves == 2:
            pair().wait_recv()
            red[...] = ghp[core] + pland[...]
        else:
            red[...] = ghp[0]
        for dx in range(1, nx):
            xcopy(dx).start()

    def state_grads():
        for dy in range(1, ny):
            ocopy(1, dy, True).wait_recv()
        gq = gql[...]
        gk = gkl[...]
        into, pulled, through = [], [], []
        for q in range(tiles):
            si, sg = scr[1, q], scr[0, q]
            sih, sil = split(si)
            sgh, sgl = split(sg)
            eq, xq = ecot[:, tile(q)], xval[:, tile(q)]
            eh, el = split(eq)
            xh, xl = split(xq)
            gq = gq + (nt(eh, sih) + nt(el, sih) + nt(eh, sil))
            gk = gk + (nt(xh, sgh) + nt(xl, sgh) + nt(xh, sgl))
            into.append(eq * (nn(qry[...], sih) + nn(qry[...], sil)))
            pulled.append(xq * kgs[:, tile(q)])
            through.append(jnp.sum(si * sg, axis=0, keepdims=True))
        gq_ref[...] = gq.astype(BF16)
        gk_ref[...] = gk.astype(BF16)
        suffix_in = nt(jnp.concatenate(into, axis=1), seg, HIGH) - cols8[...]
        prefix_in = nt(jnp.concatenate(pulled, axis=1), seg, HIGH)
        crossing = nt(jnp.broadcast_to(decx * jnp.concatenate(through, axis=1), (SUB, columns)), seg, HIGH)[:1]
        later = (row_at <= col_at).astype(F32)
        total = (
            nn(later, suffix_in, HIGH) + nt(later, rows8[...], HIGH)
            + nn((row_at > col_at).astype(F32), prefix_in, HIGH) + crossing
        )
        gd_ref[...] = total * -rate * (1.0 / (1.0 + jnp.exp(-p)))

    tasks = [(0.0, project), (4.5, pairs), (5.5, state_grads)]
    for c in range(tiles):
        ready = 5.0 + 2.5 * c
        tasks.append((ready, functools.partial(multiply, c)))
        for d in range(2):
            for j in range(reach(c, d)):
                tasks.append((ready + 3.4 * (j + 1), functools.partial(hop, c, d, j)))
    for _, task in sorted(tasks, key=lambda item: item[0]):
        task()

    total = red[x]
    for dx in range(1, nx):
        xcopy(dx, True).wait_recv()
        total = total + xland[(x + dx) % nx]
    gh_ref[...] = total.astype(gh_ref.dtype)

    for c in range(tiles):
        total = part[c, z]
        for d in range(2):
            if reach(c, d) > 0:
                total = total + ring[d, c, reach(c, d) - 1]
        gw_ref[:, tile(c)] = total

    for dy in range(1, ny):
        dcopy(dy).wait_send()
        hcopy(dy).wait_send()
        if halves == 2:
            share(dy, core).wait_send()
        for m in range(2):
            ycopy(m, dy).wait_send()
            ocopy(m, dy).wait_send()
        for c in range(tiles):
            gcopy(c, dy).wait_send()
    for dz in range(1, nz):
        for m in range(2):
            tcopy(m, dz).wait_send()
            ccopy(m, dz).wait_send()
    for c in range(tiles):
        for d in range(2):
            for j in range(reach(c, d)):
                rcopy(c, d, j).wait_send()
    if halves == 2:
        pair().wait_send()
    for dx in range(1, nx):
        xcopy(dx).wait_send()


VM = pl.BlockSpec(memory_space=pltpu.VMEM)
ANY = pl.BlockSpec(memory_space=pl.ANY)
LIMIT = 48 * 1024 * 1024


def per_device(sp, tp, hidden, value_weight, key_vecs, queries, decay_pre, decay_rate, cotangent):
    length, features = hidden.shape
    heads = decay_rate.shape[0]
    state = key_vecs.shape[2]
    columns = value_weight.shape[1]
    ny = inner_size(sp)
    nz = sp // ny
    tiles = columns // LANES
    nr = state // nz
    rows = features // sp
    own = length // tp
    halves = 2 if tp % 2 == 0 else 1
    nx = tp // halves
    far = nz // 2
    steps = 4
    vm = pltpu.VMEM
    dma = pltpu.SemaphoreType.DMA
    gk, gq, gd, gh, gw = pl.pallas_call(
        functools.partial(mixer_kernel, ny, nz, tp),
        out_shape=(
            jax.ShapeDtypeStruct((length, state), BF16),
            jax.ShapeDtypeStruct((length, state), BF16),
            jax.ShapeDtypeStruct((length, heads), F32),
            jax.ShapeDtypeStruct((own, features), BF16),
            jax.ShapeDtypeStruct((rows, columns), F32),
        ),
        in_specs=[ANY, ANY, ANY, ANY, ANY, VM, ANY],
        out_specs=(VM,) * 5,
        scratch_shapes=[
            vm((length, features), BF16),
            vm((features, columns), BF16),
            vm((length, state), BF16),
            vm((length, state), BF16),
            vm((length, heads), F32),
            vm((length, columns), BF16),
            vm((length, columns), F32),
            vm((length, columns), F32),
            vm((length, columns), F32),
            vm((heads, length, length), F32),
            vm((tiles, length, LANES), F32),
            vm((length, columns), BF16),
            vm((length, columns), F32),
            vm((heads, length), F32),
            vm((length, heads), F32),
            vm((length, state), F32),
            vm((length, state), F32),
            vm((2, ny, state, LANES), F32),
            vm((ny, SUB, LANES), F32),
            vm((2, ny, state, LANES), F32),
            vm((ny, SUB, LANES), F32),
            vm((2, nz, nr + SUB, LANES), F32),
            vm((2, nz, nr + SUB, LANES), F32),
            vm((2, nz, nr, LANES), F32),
            vm((2, nz, nr, LANES), F32),
            vm((2, ny, state, LANES), F32),
            vm((2, ny, state, LANES), F32),
            vm((ny, nz, rows, length), F32),
            vm((ny, nz, rows, length), F32),
            vm((nz, rows, ny * length), BF16),
            vm((ny, tiles, length, LANES), F32),
            vm((tiles, nz, rows, LANES), F32),
            vm((2, tiles, far, rows, LANES), F32),
            vm((halves, nx, own, features), F32),
            vm((nx, own, features), F32),
            vm((nx, own, features), F32),
            vm((nx, own, features), F32),
            dma((4 + steps,)),
            dma((ny,)), dma((ny,)),
            dma((2, ny)), dma((2, ny)),
            dma((2, nz)), dma((2, nz)),
            dma((2, nz)), dma((2, nz)),
            dma((2, ny)), dma((2, ny)),
            dma((ny,)), dma((ny,)),
            dma((ny,)), dma((ny,)),
            dma((ny, tiles)), dma((ny, tiles)),
            dma((2, tiles, far)), dma((2, tiles, far)),
            dma, dma,
            dma((nx,)), dma((nx,)),
        ],
        compiler_params=pltpu.CompilerParams(collective_id=0, has_side_effects=True, vmem_limit_bytes=LIMIT),
        name="mixer_backward",
    )(
        hidden, value_weight, key_vecs.reshape(length, state), queries.reshape(length, state), decay_pre,
        decay_rate.reshape(1, heads), cotangent.reshape(length, columns),
    )
    return gk.reshape(key_vecs.shape), gq.reshape(key_vecs.shape), gd, gh, gw


def solution(mesh):
    return jax.shard_map(
        functools.partial(per_device, mesh.shape["sp"], mesh.shape["tp"]),
        mesh=mesh,
        in_specs=(
            P("sp", None),
            P(None, "tp"),
            P("sp", "tp", None),
            P("sp", "tp", None),
            P("sp", "tp"),
            P("tp"),
            P("sp", "tp", None),
        ),
        out_specs=(
            P("sp", "tp", None),
            P("sp", "tp", None),
            P("sp", "tp"),
            P(("sp", "tp"), None),
            P("sp", "tp"),
        ),
        check_vma=False,
    )
```

```python
import functools

import jax
import jax.numpy as jnp
from jax import lax
from jax.experimental import pallas as pl
from jax.experimental.pallas import tpu as pltpu
from jax.sharding import PartitionSpec as P

MESH = pl.DeviceIdType.MESH
F32 = jnp.float32
BF16 = jnp.bfloat16
HIGH = lax.Precision.HIGHEST
LANES = 128
SUB = 8


def inner_size(count):
    size = 1
    while size * size * 4 <= count:
        size *= 2
    while count % size:
        size -= 1
    return size


def remote(src, dst, send, recv, axis, index):
    return pltpu.make_async_remote_copy(
        src_ref=src, dst_ref=dst, send_sem=send, recv_sem=recv, device_id={axis: index}, device_id_type=MESH
    )


def nn(a, b, precision=None):
    return jnp.dot(a, b, preferred_element_type=F32, precision=precision)


def nt(a, b, precision=None):
    return lax.dot_general(a, b, (((1,), (1,)), ((), ())), preferred_element_type=F32, precision=precision)


def split(x):
    hi = x.astype(BF16)
    return hi, (x - hi.astype(F32)).astype(BF16)


def mixer_kernel(ny, nz, ntp, hid_hbm, w_hbm, key_hbm, qry_hbm, pre_hbm, rate_hbm, cot_hbm,
                 gk_out, gq_out, gd_out, gh_out, gw_out,
                 gk_ref, gq_ref, gd_ref, gh_ref, gw_ref, hid, wt, key, qry, pre, rate_ref, cott, cot,
                 ecot, tend, xval, damp, gvloc, gvb, kgs, rows8, cols8, gkl, gql,
                 sbuf, decb, ybuf, ydec, tz, zbuf, cz, zcar, ob, scr, ht, hg, hcol,
                 gath, part, ring, ghp, pland, red, xland,
                 insem, dsend, drecv, ysend, yrecv, tsend, trecv, csend, crecv, osend, orecv,
                 hsend, hrecv, fsend, frecv, gsend, grecv, rsend, rrecv, psend, precv, xsend, xrecv, outsem):
    me = lax.axis_index("sp")
    mine = lax.axis_index("tp")
    z, y = me // ny, me % ny
    length, features = hid.shape
    heads = pre.shape[0]
    columns = cot.shape[1]
    width = columns // heads
    tiles = columns // LANES
    per = LANES // width
    state = key.shape[1]
    nr = state // nz
    rows = gw_ref.shape[0]
    own = gh_ref.shape[0]
    halves = 2 if ntp % 2 == 0 else 1
    core, x, nx = mine % halves, mine // halves, ntp // halves
    partner = mine + 1 - 2 * core
    hz = nz // ntp
    steps = insem.shape[0] - 5
    depth = features // steps
    ydev = [z * ny + (y + dy) % ny for dy in range(ny)]
    zdev = [((z + dz) % nz) * ny + y for dz in range(nz)]

    small = [
        pltpu.make_async_copy(pre_hbm, pre, insem.at[0]),
        pltpu.make_async_copy(rate_hbm, rate_ref, insem.at[4 + steps]),
        pltpu.make_async_copy(qry_hbm, qry, insem.at[1]),
        pltpu.make_async_copy(cot_hbm, cott, insem.at[2]),
        pltpu.make_async_copy(key_hbm, key, insem.at[3]),
    ]
    for copy in small:
        copy.start()
    wcopies = []
    for k in range(steps):
        at = pl.ds(k * depth, depth)
        wcopies.append(pltpu.make_async_copy(w_hbm.at[at, :], wt.at[at, :], insem.at[4 + k]))
    hload = pltpu.make_async_copy(hid_hbm, hid, hsend.at[y])
    hload.start()
    for copy in wcopies:
        copy.start()

    outs = [
        pltpu.make_async_copy(gk_ref, gk_out, outsem.at[0]),
        pltpu.make_async_copy(gq_ref, gq_out, outsem.at[1]),
        pltpu.make_async_copy(gd_ref, gd_out, outsem.at[2]),
        pltpu.make_async_copy(gh_ref, gh_out, outsem.at[3]),
    ]
    for c in range(tiles):
        at = pl.ds(c * LANES, LANES)
        outs.append(pltpu.make_async_copy(gw_ref.at[:, at], gw_out.at[:, at], outsem.at[4 + c]))

    barrier = pltpu.get_barrier_semaphore()
    for dev in ydev[1:] + zdev[1:]:
        pl.semaphore_signal(barrier, inc=1, device_id={"sp": dev}, device_id_type=MESH)
    for dt in range(1, ntp):
        pl.semaphore_signal(barrier, inc=1, device_id={"tp": (mine + dt) % ntp}, device_id_type=MESH)

    def dcopy(dy, arrive=False):
        there = (y + dy) % ny
        slot = there if arrive else y
        return remote(decb.at[there], ydec.at[slot], dsend.at[there], drecv.at[slot], "sp", ydev[dy])

    def ycopy(m, dy, arrive=False):
        there = (y + dy) % ny
        slot = there if arrive else y
        return remote(sbuf.at[m, there], ybuf.at[m, slot], ysend.at[m, there], yrecv.at[m, slot], "sp", ydev[dy])

    def tcopy(m, dz, arrive=False):
        there = (z + dz) % nz
        slot = there if arrive else z
        return remote(tz.at[m, there], zbuf.at[m, slot], tsend.at[m, there], trecv.at[m, slot], "sp", zdev[dz])

    def ccopy(m, dz, arrive=False):
        there = (z + dz) % nz
        slot = there if arrive else z
        return remote(cz.at[m, there], zcar.at[m, slot], csend.at[m, there], crecv.at[m, slot], "sp", zdev[dz])

    def ocopy(m, dy, arrive=False):
        there = (y + dy) % ny
        slot = there if arrive else y
        return remote(ob.at[m, there], scr.at[m, slot], osend.at[m, there], orecv.at[m, slot], "sp", ydev[dy])

    def section(k):
        return pl.ds(pl.multiple_of(k * hz, hz), hz)

    def hcopy(dy, arrive=False):
        there = (y + dy) % ny
        slot = there if arrive else y
        return remote(
            ht.at[there, section(mine)], hg.at[slot, section(mine)], hsend.at[there], hrecv.at[slot], "sp", ydev[dy]
        )

    def share(dy, dt, arrive=False):
        there = (y + dy) % ny
        peer = (mine + dt) % ntp
        which = peer if arrive else mine
        block = hg.at[there, section(which)]
        return remote(block, block, fsend.at[there, peer], frecv.at[there, which], "tp", peer)

    def gcopy(c, dy, arrive=False):
        there = (y + dy) % ny
        slot = there if arrive else y
        return remote(gath.at[slot, c], gath.at[slot, c], gsend.at[there, c], grecv.at[slot, c], "sp", ydev[dy])

    relayed = ny == 4

    def near(c):
        return ny - 1 if c % 2 == 0 else 1

    def fcopy(c):
        to = ny - near(c)
        block = gath.at[(y + near(c)) % ny, c]
        return remote(block, block, gsend.at[(y + 2) % ny, c], grecv.at[(y + near(c)) % ny, c], "sp", ydev[to])

    def pair():
        return remote(ghp.at[1 - core], pland, psend, precv, "tp", partner)

    def xcopy(dx, arrive=False):
        there = (x + dx) % nx
        slot = there if arrive else x
        return remote(red.at[there], xland.at[slot], xsend.at[there], xrecv.at[slot], "tp", there * halves + core)

    def reach(c, d):
        far = nz // 2
        return far if (c + d) % 2 == 0 else nz - 1 - far

    def fast(c):
        return nz == 8 and c >= tiles - 2

    def ahead(k, d):
        return (z + k) % nz if d == 0 else (z + nz - k) % nz

    def rcopy(c, d, j):
        src = part.at[c, ahead(reach(c, d), d)] if j == 0 else ring.at[d, c, j - 1]
        return remote(
            src, ring.at[d, c, j], rsend.at[d, c, j], rrecv.at[d, c, j], "sp", zdev[1] if d == 0 else zdev[nz - 1]
        )

    def scopy(c, d, j):
        if j == 0:
            src, hops = part.at[c, ahead(4, d)], 2
        elif j == 1:
            src, hops = part.at[c, ahead(3, d)], 2
        elif j == 2:
            src, hops = (ring.at[d, c, 0] if reach(c, d) == 4 else part.at[c, ahead(2, d)]), 2
        else:
            src, hops = ring.at[d, c, 1], 1
        return remote(
            src, ring.at[d, c, j], rsend.at[d, c, j], rrecv.at[d, c, j], "sp", zdev[hops if d == 0 else nz - hops]
        )

    def slots(c, d):
        if fast(c):
            return (0, 1, 2, 3) if reach(c, d) == 4 else (1, 2, 3)
        return tuple(range(reach(c, d)))

    def sent(c, d, j):
        return scopy(c, d, j) if fast(c) else rcopy(c, d, j)

    row_at = lax.broadcasted_iota(jnp.int32, (length, length), 0)
    col_at = lax.broadcasted_iota(jnp.int32, (length, length), 1)
    eye = (row_at == col_at).astype(BF16)
    seg = (
        lax.broadcasted_iota(jnp.int32, (heads, columns), 1) // width
        == lax.broadcasted_iota(jnp.int32, (heads, columns), 0)
    ).astype(F32)
    lane = lax.broadcasted_iota(jnp.int32, (length, LANES), 1) // width

    def tile(q):
        return slice(q * LANES, (q + 1) * LANES)

    same = (
        lax.broadcasted_iota(jnp.int32, (heads, heads), 0) == lax.broadcasted_iota(jnp.int32, (heads, heads), 1)
    ).astype(F32)
    small[0].wait()
    small[1].wait()
    p = pre[...]
    rate = nt(same, jnp.broadcast_to(rate_ref[...], (heads, heads)), HIGH)[:, :1]
    log_decay = -rate * (jnp.maximum(p, 0.0) + jnp.log1p(jnp.exp(-jnp.abs(p))))
    lower = (row_at >= col_at).astype(F32)
    cum = nt(lower, log_decay, HIGH)
    cumt = nt(log_decay, lower, HIGH)
    cumx = nn(cum, seg, HIGH)
    totx = cumx[length - 1:length]
    decx = jnp.exp(totx)
    small[2].wait()
    small[3].wait()
    for q in range(tiles):
        cot[:, tile(q)] = nt(eye, cott[tile(q), :]).astype(BF16)
    ec = jnp.exp(cumx) * cot[...].astype(F32)
    ecot[...] = ec
    qryt = nt(eye, qry[...]).astype(BF16)
    hi, lo = split(ec)
    pull = nn(qryt, hi) + nn(qryt, lo)
    for q in range(tiles):
        sbuf[0, q] = pull[:, tile(q)]
        decb[q] = jnp.broadcast_to(decx[:, tile(q)], (SUB, LANES))

    with jax.named_scope("barrier"):
        pl.semaphore_wait(barrier, ny - 1 + nz - 1 + ntp - 1)
    for dy in range(1, ny):
        dcopy(dy).start()
        ycopy(0, dy).start()
    ydec[y] = decb[y]
    ybuf[0, y] = sbuf[0, y]

    tend[...] = jnp.exp(totx - cumx)
    small[4].wait()
    hload.wait()
    values = jnp.zeros((length, columns), F32)
    for k in range(steps):
        wcopies[k].wait()
        values = values + nn(hid[:, k * depth:(k + 1) * depth], wt[k * depth:(k + 1) * depth, :])
    vals = values.astype(BF16)
    xv = tend[...] * vals.astype(F32)
    xval[...] = xv
    keyt = nt(eye, key[...]).astype(BF16)
    hi, lo = split(xv)
    push = nn(keyt, hi) + nn(keyt, lo)
    for q in range(tiles):
        sbuf[1, q] = push[:, tile(q)]
    with jax.named_scope("send_y1"):
        for dy in range(1, ny):
            ycopy(1, dy).start()
    ybuf[1, y] = sbuf[1, y]

    for b in range(features // LANES):
        block = nt(eye, hid[:, tile(b)])
        for i in range(LANES // rows):
            owner = b * LANES // rows + i
            ht[owner % ny, owner // ny] = block[i * rows:(i + 1) * rows]
    with jax.named_scope("send_h"):
        for dy in range(1, ny):
            hcopy(dy).start()
    hcol[:, :, pl.ds(pl.multiple_of(y * length, LANES), length)] = ht[y].astype(BF16)

    def stage_y(m):
        if m == 0:
            for dy in range(1, ny):
                dcopy(dy, True).wait_recv()
        for dy in range(1, ny):
            ycopy(m, dy, True).wait_recv()
        order = list(range(ny)) if m == 1 else list(reversed(range(ny)))
        run = ybuf[m, order[0]]
        for yy in order[1:]:
            run = ydec[yy][:1] * run + ybuf[m, yy]
        prod = ydec[0]
        for yy in range(1, ny):
            prod = prod * ydec[yy]
        for k in range(nz):
            tz[m, k, :nr] = run[k * nr:(k + 1) * nr]
            tz[m, k, nr:] = prod
        for dz in range(1, nz):
            tcopy(m, dz).start()
        zbuf[m, z] = tz[m, z]

    def stage_z(m):
        for dz in range(1, nz):
            tcopy(m, dz, True).wait_recv()
        run = jnp.zeros((nr, LANES), F32)
        for zz in (list(range(nz)) if m == 1 else list(reversed(range(nz)))):
            cz[m, zz] = run
            run = zbuf[m, zz, nr:nr + 1] * run + zbuf[m, zz, :nr]
        for dz in range(1, nz):
            ccopy(m, dz).start()
        zcar[m, z] = cz[m, z]

    def stage_c(m):
        for dz in range(1, nz):
            ccopy(m, dz, True).wait_recv()
        now = zcar[m].reshape(state, LANES)
        for yy in (list(range(ny)) if m == 1 else list(reversed(range(ny)))):
            ob[m, yy] = now
            now = ydec[yy][:1] * now + ybuf[m, yy]
        for dy in range(1, ny):
            ocopy(m, dy).start()
        scr[m, y] = ob[m, y]

    with jax.named_scope("stage_y0"):
        stage_y(0)

    causal = row_at <= col_at
    scores = nt(key[...], qry[...])
    for q in range(tiles):
        lefts, rights = [], []
        ct = cot[:, tile(q)]
        for i in range(per):
            h = q * per + i
            across = cumt[h:h + 1, :] - cum[:, h:h + 1]
            dm = jnp.where(causal, jnp.exp(jnp.where(causal, across, 0.0)), 0.0)
            damp[h] = dm
            lefts.extend(split(scores * dm))
            masked = jnp.where(lane == i, ct, jnp.zeros_like(ct))
            rights.extend([masked, masked])
        gvloc[q] = nn(jnp.concatenate(lefts, axis=1), jnp.concatenate(rights, axis=0))

    with jax.named_scope("stage_z0"):
        stage_z(0)

    with jax.named_scope("stage_y1"):
        stage_y(1)

    dsum = jnp.zeros((length, length), F32)
    for q in range(tiles):
        vt = vals[:, tile(q)]
        both = nt(
            jnp.concatenate([jnp.where(lane == i, vt, jnp.zeros_like(vt)) for i in range(per)], axis=0),
            cot[:, tile(q)],
        )
        for i in range(per):
            h = q * per + i
            ds = both[i * length:(i + 1) * length] * damp[h]
            flux = ds * scores
            dsum = dsum + ds
            rows8[h:h + 1, :] = jnp.sum(flux, axis=0, keepdims=True)
            cols8[:, h:h + 1] = jnp.sum(flux, axis=1, keepdims=True)

    with jax.named_scope("hid_y"):
        for dy in range(1, ny):
            hcopy(dy, True).wait_recv()
            for dt in range(1, ntp):
                share(dy, dt).start()

    with jax.named_scope("stage_c0"):
        stage_c(0)

    hi, lo = split(dsum)
    gkl[...] = nn(hi, qry[...]) + nn(lo, qry[...])
    hi, lo = split(dsum.T)
    gql[...] = nn(hi, key[...]) + nn(lo, key[...])
    with jax.named_scope("stage_z1"):
        stage_z(1)

    with jax.named_scope("stage_c1"):
        stage_c(1)

    with jax.named_scope("wait_o0"):
        for dy in range(1, ny):
            ocopy(0, dy, True).wait_recv()
    for q in range(tiles):
        hi, lo = split(scr[0, q])
        kg = nn(key[...], hi) + nn(key[...], lo)
        kgs[:, tile(q)] = kg
        gb = (gvloc[q] + tend[:, tile(q)] * kg).astype(BF16)
        gvb[:, tile(q)] = gb
        gath[y, q] = gb.astype(F32)
        for dy in range(1, ny):
            if not (relayed and dy == 2):
                gcopy(q, dy).start()

    def columns_in():
        for dy in range(1, ny):
            there = (y + dy) % ny
            for dt in range(1, ntp):
                share(dy, dt, True).wait_recv()
            hcol[:, :, pl.ds(pl.multiple_of(there * length, LANES), length)] = hg[there].astype(BF16)

    def relay(c):
        gcopy(c, near(c), True).wait_recv()
        fcopy(c).start()

    def multiply(c):
        for dy in range(1, ny):
            if not (relayed and dy == near(c)):
                gcopy(c, dy, True).wait_recv()
        block = gath[:, c].reshape(ny * length, LANES).astype(BF16)
        part[c] = nn(hcol[...].reshape(nz * rows, ny * length), block).reshape(nz, rows, LANES)
        for d in range(2):
            if fast(c):
                for j in slots(c, d):
                    if j < 2 or (j == 2 and reach(c, d) == 3):
                        scopy(c, d, j).start()
            elif reach(c, d) > 0:
                rcopy(c, d, 0).start()

    def hop(c, d, j):
        rcopy(c, d, j).wait_recv()
        left = reach(c, d) - 1 - j
        if left > 0:
            ring[d, c, j] = ring[d, c, j] + part[c, ahead(left, d)]
            rcopy(c, d, j + 1).start()

    def step(c, d, j):
        scopy(c, d, j).wait_recv()
        if j < 2:
            ring[d, c, j] = ring[d, c, j] + part[c, ahead(2 - j, d)]
            scopy(c, d, j + 2).start()

    def total_weight(c):
        total = part[c, z]
        for d in range(2):
            if fast(c):
                total = total + (ring[d, c, 2] + ring[d, c, 3])
            elif reach(c, d) > 0:
                total = total + ring[d, c, reach(c, d) - 1]
        gw_ref[:, tile(c)] = total
        outs[4 + c].start()

    def project():
        block = nt(gvb[...], wt[...])
        for t in range(ntp):
            ghp[t % halves, t // halves] = block[t * own:(t + 1) * own]
        if halves == 2:
            pair().start()

    def pairs():
        if halves == 2:
            pair().wait_recv()
            red[...] = ghp[core] + pland[...]
        else:
            red[...] = ghp[0]
        for dx in range(1, nx):
            xcopy(dx).start()

    def state_grads():
        with jax.named_scope("wait_o1"):
            for dy in range(1, ny):
                ocopy(1, dy, True).wait_recv()
        gq = gql[...]
        gk = gkl[...]
        into, pulled, through = [], [], []
        for q in range(tiles):
            si, sg = scr[1, q], scr[0, q]
            sih, sil = split(si)
            sgh, sgl = split(sg)
            eq, xq = ecot[:, tile(q)], xval[:, tile(q)]
            eh, el = split(eq)
            xh, xl = split(xq)
            gq = gq + (nt(eh, sih) + nt(el, sih) + nt(eh, sil))
            gk = gk + (nt(xh, sgh) + nt(xl, sgh) + nt(xh, sgl))
            into.append(eq * (nn(qry[...], sih) + nn(qry[...], sil)))
            pulled.append(xq * kgs[:, tile(q)])
            through.append(jnp.sum(si * sg, axis=0, keepdims=True))
        gq_ref[...] = gq.astype(BF16)
        gk_ref[...] = gk.astype(BF16)
        suffix_in = nt(seg, jnp.concatenate(into, axis=1), HIGH) - nt(same, cols8[...], HIGH) + rows8[...]
        prefix_in = nt(seg, jnp.concatenate(pulled, axis=1), HIGH)
        crossing = nt(seg, jnp.broadcast_to(decx * jnp.concatenate(through, axis=1), (SUB, columns)), HIGH)[:, :1]
        total = (
            nn(suffix_in, lower, HIGH) + nn(prefix_in, (row_at < col_at).astype(F32), HIGH) + crossing
        )
        gd_ref[...] = total * -rate * (1.0 / (1.0 + jnp.exp(-p)))
        for copy in outs[:3]:
            copy.start()

    def total_hidden():
        total = red[x]
        for dx in range(1, nx):
            xcopy(dx, True).wait_recv()
            total = total + xland[(x + dx) % nx]
        gh_ref[...] = total.astype(gh_ref.dtype)
        outs[3].start()

    tasks = [
        (0.0, "project", project), (1.0, "columns_in", columns_in), (9.0, "pairs", pairs),
        (3.0, "state_grads", state_grads), (18.0, "total_hidden", total_hidden),
    ]
    for c in range(tiles):
        ready = 5.0 + 2.2 * c
        if relayed:
            tasks.append((ready - 2.0, f"relay{c}", functools.partial(relay, c)))
        tasks.append((ready, f"multiply{c}", functools.partial(multiply, c)))
        last = ready
        for d in range(2):
            for j in slots(c, d):
                if fast(c):
                    at = ready + (3.6 if j < 2 else 7.2) + 0.2 * (j % 2)
                    tasks.append((at, f"step{c}{d}{j}", functools.partial(step, c, d, j)))
                else:
                    at = ready + 2.7 * (j + 1)
                    tasks.append((at, f"hop{c}{d}{j}", functools.partial(hop, c, d, j)))
                last = max(last, at)
        tasks.append((last + 0.01, f"total{c}", functools.partial(total_weight, c)))
    for _, name, task in sorted(tasks, key=lambda item: item[0]):
        with jax.named_scope(name):
            task()

    for dy in range(1, ny):
        dcopy(dy).wait_send()
        hcopy(dy).wait_send()
        for dt in range(1, ntp):
            share(dy, dt).wait_send()
        for m in range(2):
            ycopy(m, dy).wait_send()
            ocopy(m, dy).wait_send()
        for c in range(tiles):
            (fcopy(c) if relayed and dy == 2 else gcopy(c, dy)).wait_send()
    for dz in range(1, nz):
        for m in range(2):
            tcopy(m, dz).wait_send()
            ccopy(m, dz).wait_send()
    for c in range(tiles):
        for d in range(2):
            for j in slots(c, d):
                sent(c, d, j).wait_send()
    if halves == 2:
        pair().wait_send()
    for dx in range(1, nx):
        xcopy(dx).wait_send()
    for copy in outs:
        copy.wait()


def finish_kernel(*refs):
    count = (len(refs) - 1) // 3
    ins, outs, held, sems = refs[:count], refs[count:2 * count], refs[2 * count:3 * count], refs[-1]
    loads = [pltpu.make_async_copy(ins[k], held[k], sems.at[0, k]) for k in range(count)]
    stores = [pltpu.make_async_copy(held[k], outs[k], sems.at[1, k]) for k in range(count)]
    for load in loads:
        load.start()
    for load, store in zip(loads, stores):
        load.wait()
        store.start()
    for store in stores:
        store.wait()


HBM = pl.BlockSpec(memory_space=pltpu.HBM)
LIMIT = 60 * 1024 * 1024


def per_device(sp, tp, hidden, value_weight, key_vecs, queries, decay_pre, decay_rate, cotangent):
    length, features = hidden.shape
    heads = decay_rate.shape[0]
    state = key_vecs.shape[2]
    columns = value_weight.shape[1]
    ny = inner_size(sp)
    nz = sp // ny
    tiles = columns // LANES
    nr = state // nz
    rows = features // sp
    own = length // tp
    halves = 2 if tp % 2 == 0 else 1
    nx = tp // halves
    far = nz // 2
    steps = 4
    vm = pltpu.VMEM
    dma = pltpu.SemaphoreType.DMA
    outs = pl.pallas_call(
        functools.partial(mixer_kernel, ny, nz, tp),
        out_shape=(
            jax.ShapeDtypeStruct((length, state), BF16),
            jax.ShapeDtypeStruct((length, state), BF16),
            jax.ShapeDtypeStruct((heads, length), F32),
            jax.ShapeDtypeStruct((own, features), BF16),
            jax.ShapeDtypeStruct((rows, columns), F32),
        ),
        in_specs=[HBM] * 7,
        out_specs=(HBM,) * 5,
        scratch_shapes=[
            vm((length, state), BF16),
            vm((length, state), BF16),
            vm((heads, length), F32),
            vm((own, features), BF16),
            vm((rows, columns), F32),
            vm((length, features), BF16),
            vm((features, columns), BF16),
            vm((length, state), BF16),
            vm((length, state), BF16),
            vm((heads, length), F32),
            vm((1, heads), F32),
            vm((columns, length), BF16),
            vm((length, columns), BF16),
            vm((length, columns), F32),
            vm((length, columns), F32),
            vm((length, columns), F32),
            vm((heads, length, length), F32),
            vm((tiles, length, LANES), F32),
            vm((length, columns), BF16),
            vm((length, columns), F32),
            vm((heads, length), F32),
            vm((length, heads), F32),
            vm((length, state), F32),
            vm((length, state), F32),
            vm((2, ny, state, LANES), F32),
            vm((ny, SUB, LANES), F32),
            vm((2, ny, state, LANES), F32),
            vm((ny, SUB, LANES), F32),
            vm((2, nz, nr + SUB, LANES), F32),
            vm((2, nz, nr + SUB, LANES), F32),
            vm((2, nz, nr, LANES), F32),
            vm((2, nz, nr, LANES), F32),
            vm((2, ny, state, LANES), F32),
            vm((2, ny, state, LANES), F32),
            vm((ny, nz, rows, length), F32),
            vm((ny, nz, rows, length), F32),
            vm((nz, rows, ny * length), BF16),
            vm((ny, tiles, length, LANES), F32),
            vm((tiles, nz, rows, LANES), F32),
            vm((2, tiles, far, rows, LANES), F32),
            vm((halves, nx, own, features), F32),
            vm((nx, own, features), F32),
            vm((nx, own, features), F32),
            vm((nx, own, features), F32),
            dma((5 + steps,)),
            dma((ny,)), dma((ny,)),
            dma((2, ny)), dma((2, ny)),
            dma((2, nz)), dma((2, nz)),
            dma((2, nz)), dma((2, nz)),
            dma((2, ny)), dma((2, ny)),
            dma((ny,)), dma((ny,)),
            dma((ny, tp)), dma((ny, tp)),
            dma((ny, tiles)), dma((ny, tiles)),
            dma((2, tiles, far)), dma((2, tiles, far)),
            dma, dma,
            dma((nx,)), dma((nx,)),
            dma((4 + tiles,)),
        ],
        compiler_params=pltpu.CompilerParams(collective_id=0, has_side_effects=True, vmem_limit_bytes=LIMIT),
        name="mixer_backward",
    )(
        hidden, value_weight, key_vecs.reshape(length, state), queries.reshape(length, state), decay_pre.T,
        decay_rate.reshape(1, heads), cotangent.reshape(length, columns).T,
    )
    gk, gq, gd, gh, gw = pl.pallas_call(
        finish_kernel,
        out_shape=tuple(jax.ShapeDtypeStruct(o.shape, o.dtype) for o in outs),
        in_specs=[HBM] * 5,
        out_specs=(HBM,) * 5,
        scratch_shapes=[vm(o.shape, o.dtype) for o in outs] + [dma((2, 5))],
        compiler_params=pltpu.CompilerParams(vmem_limit_bytes=LIMIT),
        name="write_out",
    )(*outs)
    return gk.reshape(key_vecs.shape), gq.reshape(key_vecs.shape), gd.T, gh, gw


def solution(mesh):
    return jax.shard_map(
        functools.partial(per_device, mesh.shape["sp"], mesh.shape["tp"]),
        mesh=mesh,
        in_specs=(
            P("sp", None),
            P(None, "tp"),
            P("sp", "tp", None),
            P("sp", "tp", None),
            P("sp", "tp"),
            P("tp"),
            P("sp", "tp", None),
        ),
        out_specs=(
            P("sp", "tp", None),
            P("sp", "tp", None),
            P("sp", "tp"),
            P(("sp", "tp"), None),
            P("sp", "tp"),
        ),
        check_vma=False,
    )
```

```python
import functools

import jax
import jax.numpy as jnp
from jax import lax
from jax.experimental import pallas as pl
from jax.experimental.pallas import tpu as pltpu
from jax.sharding import PartitionSpec as P

MESH = pl.DeviceIdType.MESH
F32 = jnp.float32
BF16 = jnp.bfloat16
HIGH = lax.Precision.HIGHEST
LANES = 128
SUB = 8


def inner_size(count):
    size = 1
    while size * size * 4 <= count:
        size *= 2
    while count % size:
        size -= 1
    return size


def remote(src, dst, send, recv, axis, index):
    return pltpu.make_async_remote_copy(
        src_ref=src, dst_ref=dst, send_sem=send, recv_sem=recv, device_id={axis: index}, device_id_type=MESH
    )


def nn(a, b, precision=None):
    return jnp.dot(a, b, preferred_element_type=F32, precision=precision)


def nt(a, b, precision=None):
    return lax.dot_general(a, b, (((1,), (1,)), ((), ())), preferred_element_type=F32, precision=precision)


def split(x):
    hi = x.astype(BF16)
    return hi, (x - hi.astype(F32)).astype(BF16)


def mixer_kernel(ny, nz, ntp, hid_hbm, w_hbm, key_hbm, qry_hbm, pre_hbm, rate_hbm, cot_hbm,
                 gk_out, gq_out, gd_out, gh_out, gw_out,
                 gk_ref, gq_ref, gd_ref, gh_ref, gw_ref, hid, wt, key, qry, pre, rate_ref, cott, cot,
                 ecot, tend, xval, damp, gvloc, gvb, kgs, rows8, cols8, gkl, gql,
                 sbuf, decb, ybuf, ydec, tz, zbuf, cz, zcar, ob, scr, ht, hg, hcol,
                 gath, part, ring, ghp, pland, red, xland,
                 insem, wsem, dsend, drecv, ysend, yrecv, tsend, trecv, csend, crecv, osend, orecv,
                 hsend, hrecv, fsend, frecv, gsend, grecv, rsend, rrecv, psend, precv, xsend, xrecv, outsem):
    me = lax.axis_index("sp")
    mine = lax.axis_index("tp")
    z, y = me // ny, me % ny
    length, features = hid.shape
    heads = pre.shape[0]
    columns = cot.shape[1]
    width = columns // heads
    tiles = columns // LANES
    per = LANES // width
    state = key.shape[1]
    nr = state // nz
    rows = gw_ref.shape[0]
    own = gh_ref.shape[0]
    halves = 2 if ntp % 2 == 0 else 1
    core, x, nx = mine % halves, mine // halves, ntp // halves
    partner = mine + 1 - 2 * core
    hz = nz // ntp
    steps = wsem.shape[0]
    depth = features // steps
    ydev = [z * ny + (y + dy) % ny for dy in range(ny)]
    zdev = [((z + dz) % nz) * ny + y for dz in range(nz)]

    small = [
        pltpu.make_async_copy(pre_hbm, pre, insem.at[0]),
        pltpu.make_async_copy(rate_hbm, rate_ref, insem.at[4]),
        pltpu.make_async_copy(qry_hbm, qry, insem.at[1]),
        pltpu.make_async_copy(cot_hbm, cott, insem.at[2]),
        pltpu.make_async_copy(key_hbm, key, insem.at[3]),
    ]
    for copy in small:
        copy.start()
    wcopies = []
    for k in range(steps):
        at = pl.ds(k * depth, depth)
        wcopies.append(pltpu.make_async_copy(w_hbm.at[at, :], wt.at[at, :], wsem.at[k]))
    hload = pltpu.make_async_copy(hid_hbm, hid, insem.at[5])
    hload.start()
    for copy in wcopies:
        copy.start()

    outs = [
        pltpu.make_async_copy(gk_ref, gk_out, outsem.at[0]),
        pltpu.make_async_copy(gq_ref, gq_out, outsem.at[1]),
        pltpu.make_async_copy(gd_ref, gd_out, outsem.at[2]),
        pltpu.make_async_copy(gh_ref, gh_out, outsem.at[3]),
    ]
    for c in range(tiles):
        at = pl.ds(c * LANES, LANES)
        outs.append(pltpu.make_async_copy(gw_ref.at[:, at], gw_out.at[:, at], outsem.at[4]))

    barrier = pltpu.get_barrier_semaphore()
    for dev in ydev[1:] + zdev[1:]:
        pl.semaphore_signal(barrier, inc=1, device_id={"sp": dev}, device_id_type=MESH)
    for dt in range(1, ntp):
        pl.semaphore_signal(barrier, inc=1, device_id={"tp": (mine + dt) % ntp}, device_id_type=MESH)

    def dcopy(dy, arrive=False):
        there = (y + dy) % ny
        slot = there if arrive else y
        return remote(decb.at[there], ydec.at[slot], dsend, drecv, "sp", ydev[dy])

    def ycopy(m, dy, arrive=False):
        there = (y + dy) % ny
        slot = there if arrive else y
        return remote(sbuf.at[m, there], ybuf.at[m, slot], ysend.at[m], yrecv.at[m], "sp", ydev[dy])

    def tcopy(m, dz, arrive=False):
        there = (z + dz) % nz
        slot = there if arrive else z
        return remote(tz.at[m, there], zbuf.at[m, slot], tsend.at[m], trecv.at[m], "sp", zdev[dz])

    def ccopy(m, dz, arrive=False):
        there = (z + dz) % nz
        slot = there if arrive else z
        return remote(cz.at[m, there], zcar.at[m, slot], csend.at[m], crecv.at[m], "sp", zdev[dz])

    def ocopy(m, dy, arrive=False):
        there = (y + dy) % ny
        slot = there if arrive else y
        return remote(ob.at[m, there], scr.at[m, slot], osend.at[m], orecv.at[m], "sp", ydev[dy])

    def section(k):
        return pl.ds(pl.multiple_of(k * hz, hz), hz)

    def hcopy(dy, arrive=False):
        there = (y + dy) % ny
        slot = there if arrive else y
        return remote(
            ht.at[there, section(mine)], hg.at[slot, section(mine)], hsend, hrecv, "sp", ydev[dy]
        )

    def share(dy, dt, arrive=False):
        there = (y + dy) % ny
        peer = (mine + dt) % ntp
        which = peer if arrive else mine
        block = hg.at[there, section(which)]
        return remote(block, block, fsend, frecv, "tp", peer)

    def gcopy(c, dy, arrive=False):
        there = (y + dy) % ny
        slot = there if arrive else y
        return remote(gath.at[slot, c], gath.at[slot, c], gsend, grecv.at[c], "sp", ydev[dy])

    def pair():
        return remote(ghp.at[1 - core], pland, psend, precv, "tp", partner)

    def xcopy(dx, arrive=False):
        there = (x + dx) % nx
        slot = there if arrive else x
        return remote(red.at[there], xland.at[slot], xsend, xrecv, "tp", there * halves + core)

    def reach(c, d):
        far = nz // 2
        return far if (c + d) % 2 == 0 else nz - 1 - far

    def fast(c):
        return nz == 8 and c >= tiles - 2

    def ahead(k, d):
        return (z + k) % nz if d == 0 else (z + nz - k) % nz

    def rcopy(c, d, j):
        src = part.at[c, ahead(reach(c, d), d)] if j == 0 else ring.at[d, c, j - 1]
        return remote(
            src, ring.at[d, c, j], rsend, rrecv.at[slot_at(c, d, j)], "sp", zdev[1] if d == 0 else zdev[nz - 1]
        )

    def scopy(c, d, j):
        if j == 0:
            src, hops = part.at[c, ahead(4, d)], 2
        elif j == 1:
            src, hops = part.at[c, ahead(3, d)], 2
        elif j == 2:
            src, hops = (ring.at[d, c, 0] if reach(c, d) == 4 else part.at[c, ahead(2, d)]), 2
        else:
            src, hops = ring.at[d, c, 1], 1
        return remote(
            src, ring.at[d, c, j], rsend, rrecv.at[slot_at(c, d, j)], "sp", zdev[hops if d == 0 else nz - hops]
        )

    def slots(c, d):
        if fast(c):
            return (0, 1, 2, 3) if reach(c, d) == 4 else (1, 2, 3)
        return tuple(range(reach(c, d)))

    ring_slots = sorted({(c, d, min(j, 2) if fast(c) else j) for c in range(tiles) for d in range(2) for j in slots(c, d)})

    def slot_at(c, d, j):
        return ring_slots.index((c, d, min(j, 2) if fast(c) else j))

    def bulk(ref, send, recv):
        return remote(ref, ref, send, recv, "sp", ydev[1])

    row_at = lax.broadcasted_iota(jnp.int32, (length, length), 0)
    col_at = lax.broadcasted_iota(jnp.int32, (length, length), 1)
    eye = (row_at == col_at).astype(BF16)
    seg = (
        lax.broadcasted_iota(jnp.int32, (heads, columns), 1) // width
        == lax.broadcasted_iota(jnp.int32, (heads, columns), 0)
    ).astype(F32)
    lane = lax.broadcasted_iota(jnp.int32, (length, LANES), 1) // width

    def tile(q):
        return slice(q * LANES, (q + 1) * LANES)

    same = (
        lax.broadcasted_iota(jnp.int32, (heads, heads), 0) == lax.broadcasted_iota(jnp.int32, (heads, heads), 1)
    ).astype(F32)
    small[0].wait()
    small[1].wait()
    p = pre[...]
    rate = nt(same, jnp.broadcast_to(rate_ref[...], (heads, heads)), HIGH)[:, :1]
    log_decay = -rate * (jnp.maximum(p, 0.0) + jnp.log1p(jnp.exp(-jnp.abs(p))))
    lower = (row_at >= col_at).astype(F32)
    cum = nt(lower, log_decay, HIGH)
    cumt = nt(log_decay, lower, HIGH)
    cumx = nn(cum, seg, HIGH)
    totx = cumx[length - 1:length]
    decx = jnp.exp(totx)
    small[2].wait()
    small[3].wait()
    for q in range(tiles):
        cot[:, tile(q)] = nt(eye, cott[tile(q), :]).astype(BF16)
    ec = jnp.exp(cumx) * cot[...].astype(F32)
    ecot[...] = ec
    qryt = nt(eye, qry[...]).astype(BF16)
    hi, lo = split(ec)
    pull = nn(qryt, hi) + nn(qryt, lo)
    for q in range(tiles):
        sbuf[0, q] = pull[:, tile(q)]
        decb[q] = jnp.broadcast_to(decx[:, tile(q)], (SUB, LANES))

    with jax.named_scope("barrier"):
        pl.semaphore_wait(barrier, ny - 1 + nz - 1 + ntp - 1)
    for dy in range(1, ny):
        dcopy(dy).start()
        ycopy(0, dy).start()
    ydec[y] = decb[y]
    ybuf[0, y] = sbuf[0, y]

    hload.wait()
    for b in range(features // LANES):
        block = nt(eye, hid[:, tile(b)])
        for i in range(LANES // rows):
            owner = b * LANES // rows + i
            ht[owner % ny, owner // ny] = block[i * rows:(i + 1) * rows]
    with jax.named_scope("send_h"):
        for dy in range(1, ny):
            hcopy(dy).start()
    tend[...] = jnp.exp(totx - cumx)
    small[4].wait()
    values = jnp.zeros((length, columns), F32)
    for k in range(steps):
        wcopies[k].wait()
        values = values + nn(hid[:, k * depth:(k + 1) * depth], wt[k * depth:(k + 1) * depth, :])
    vals = values.astype(BF16)
    xv = tend[...] * vals.astype(F32)
    xval[...] = xv
    keyt = nt(eye, key[...]).astype(BF16)
    hi, lo = split(xv)
    push = nn(keyt, hi) + nn(keyt, lo)
    for q in range(tiles):
        sbuf[1, q] = push[:, tile(q)]
    with jax.named_scope("send_y1"):
        for dy in range(1, ny):
            ycopy(1, dy).start()
    ybuf[1, y] = sbuf[1, y]

    hcol[:, :, pl.ds(pl.multiple_of(y * length, LANES), length)] = ht[y].astype(BF16)

    def stage_y(m):
        if m == 0:
            bulk(ydec.at[:ny - 1], dsend, drecv).wait_recv()
        bulk(ybuf.at[m, :ny - 1], ysend.at[m], yrecv.at[m]).wait_recv()
        order = list(range(ny)) if m == 1 else list(reversed(range(ny)))
        run = ybuf[m, order[0]]
        for yy in order[1:]:
            run = ydec[yy][:1] * run + ybuf[m, yy]
        prod = ydec[0]
        for yy in range(1, ny):
            prod = prod * ydec[yy]
        for k in range(nz):
            tz[m, k, :nr] = run[k * nr:(k + 1) * nr]
            tz[m, k, nr:] = prod
        for dz in range(1, nz):
            tcopy(m, dz).start()
        zbuf[m, z] = tz[m, z]

    def stage_z(m):
        bulk(zbuf.at[m, :nz - 1], tsend.at[m], trecv.at[m]).wait_recv()
        run = jnp.zeros((nr, LANES), F32)
        for zz in (list(range(nz)) if m == 1 else list(reversed(range(nz)))):
            cz[m, zz] = run
            run = zbuf[m, zz, nr:nr + 1] * run + zbuf[m, zz, :nr]
        for dz in range(1, nz):
            ccopy(m, dz).start()
        zcar[m, z] = cz[m, z]

    def stage_c(m):
        bulk(zcar.at[m, :nz - 1], csend.at[m], crecv.at[m]).wait_recv()
        now = zcar[m].reshape(state, LANES)
        for yy in (list(range(ny)) if m == 1 else list(reversed(range(ny)))):
            ob[m, yy] = now
            now = ydec[yy][:1] * now + ybuf[m, yy]
        for dy in range(1, ny):
            ocopy(m, dy).start()
        scr[m, y] = ob[m, y]

    with jax.named_scope("stage_y0"):
        stage_y(0)

    causal = row_at <= col_at
    scores = nt(key[...], qry[...])
    for q in range(tiles):
        lefts, rights = [], []
        ct = cot[:, tile(q)]
        for i in range(per):
            h = q * per + i
            across = cumt[h:h + 1, :] - cum[:, h:h + 1]
            dm = jnp.where(causal, jnp.exp(jnp.where(causal, across, 0.0)), 0.0)
            damp[h] = dm
            lefts.extend(split(scores * dm))
            masked = jnp.where(lane == i, ct, jnp.zeros_like(ct))
            rights.extend([masked, masked])
        gvloc[q] = nn(jnp.concatenate(lefts, axis=1), jnp.concatenate(rights, axis=0))

    with jax.named_scope("hid_y"):
        bulk(hg.at[:ny - 1, :hz], hsend, hrecv).wait_recv()
        for dt in range(1, ntp):
            for dy in range(1, ny):
                share(dy, dt).start()

    with jax.named_scope("stage_z0"):
        stage_z(0)

    with jax.named_scope("stage_y1"):
        stage_y(1)

    dsum = jnp.zeros((length, length), F32)
    for q in range(tiles):
        vt = vals[:, tile(q)]
        both = nt(
            jnp.concatenate([jnp.where(lane == i, vt, jnp.zeros_like(vt)) for i in range(per)], axis=0),
            cot[:, tile(q)],
        )
        for i in range(per):
            h = q * per + i
            ds = both[i * length:(i + 1) * length] * damp[h]
            flux = ds * scores
            dsum = dsum + ds
            rows8[h:h + 1, :] = jnp.sum(flux, axis=0, keepdims=True)
            cols8[:, h:h + 1] = jnp.sum(flux, axis=1, keepdims=True)

    with jax.named_scope("stage_c0"):
        stage_c(0)

    hi, lo = split(dsum)
    gkl[...] = nn(hi, qry[...]) + nn(lo, qry[...])
    hi, lo = split(dsum.T)
    gql[...] = nn(hi, key[...]) + nn(lo, key[...])
    with jax.named_scope("stage_z1"):
        stage_z(1)

    with jax.named_scope("wait_o0"):
        bulk(scr.at[0, :ny - 1], osend.at[0], orecv.at[0]).wait_recv()
    for q in range(tiles):
        hi, lo = split(scr[0, q])
        kg = nn(key[...], hi) + nn(key[...], lo)
        kgs[:, tile(q)] = kg
        gb = (gvloc[q] + tend[:, tile(q)] * kg).astype(BF16)
        gvb[:, tile(q)] = gb
        gath[y, q] = gb.astype(F32)
        for dy in sorted(range(1, ny), key=lambda dy: -min(dy, ny - dy)):
            gcopy(q, dy).start()

    def columns_in():
        if ntp > 1:
            bulk(hg.at[:ny - 1, :nz - hz], fsend, frecv).wait_recv()
        for dy in range(1, ny):
            there = (y + dy) % ny
            hcol[:, :, pl.ds(pl.multiple_of(there * length, LANES), length)] = hg[there].astype(BF16)

    def multiply(c):
        bulk(gath.at[:ny - 1, c], gsend, grecv.at[c]).wait_recv()
        block = gath[:, c].reshape(ny * length, LANES).astype(BF16)
        part[c] = nn(hcol[...].reshape(nz * rows, ny * length), block).reshape(nz, rows, LANES)
        for d in range(2):
            if fast(c):
                for j in slots(c, d):
                    if j < 2 or (j == 2 and reach(c, d) == 3):
                        scopy(c, d, j).start()
            elif reach(c, d) > 0:
                rcopy(c, d, 0).start()

    def hop(c, d, j):
        rcopy(c, d, j).wait_recv()
        left = reach(c, d) - 1 - j
        if left > 0:
            ring[d, c, j] = ring[d, c, j] + part[c, ahead(left, d)]
            rcopy(c, d, j + 1).start()

    def step(c, d, j):
        if j == 2:
            bulk(ring.at[d, c, 2:4], rsend, rrecv.at[slot_at(c, d, 2)]).wait_recv()
        else:
            scopy(c, d, j).wait_recv()
            ring[d, c, j] = ring[d, c, j] + part[c, ahead(2 - j, d)]
            scopy(c, d, j + 2).start()

    def total_weight(c):
        total = part[c, z]
        for d in range(2):
            if fast(c):
                total = total + (ring[d, c, 2] + ring[d, c, 3])
            elif reach(c, d) > 0:
                total = total + ring[d, c, reach(c, d) - 1]
        gw_ref[:, tile(c)] = total
        outs[4 + c].start()

    def project():
        block = nt(gvb[...], wt[...])
        for t in range(ntp):
            ghp[t % halves, t // halves] = block[t * own:(t + 1) * own]
        if halves == 2:
            pair().start()

    def pairs():
        if halves == 2:
            pair().wait_recv()
            red[...] = ghp[core] + pland[...]
        else:
            red[...] = ghp[0]
        for dx in range(1, nx):
            xcopy(dx).start()

    def state_grads():
        with jax.named_scope("wait_o1"):
            bulk(scr.at[1, :ny - 1], osend.at[1], orecv.at[1]).wait_recv()
        gq = gql[...]
        gk = gkl[...]
        into, pulled, through = [], [], []
        for q in range(tiles):
            si, sg = scr[1, q], scr[0, q]
            sih, sil = split(si)
            sgh, sgl = split(sg)
            eq, xq = ecot[:, tile(q)], xval[:, tile(q)]
            eh, el = split(eq)
            xh, xl = split(xq)
            gq = gq + (nt(eh, sih) + nt(el, sih) + nt(eh, sil))
            gk = gk + (nt(xh, sgh) + nt(xl, sgh) + nt(xh, sgl))
            into.append(eq * (nn(qry[...], sih) + nn(qry[...], sil)))
            pulled.append(xq * kgs[:, tile(q)])
            through.append(jnp.sum(si * sg, axis=0, keepdims=True))
        gq_ref[...] = gq.astype(BF16)
        gk_ref[...] = gk.astype(BF16)
        suffix_in = nt(seg, jnp.concatenate(into, axis=1), HIGH) - nt(same, cols8[...], HIGH) + rows8[...]
        prefix_in = nt(seg, jnp.concatenate(pulled, axis=1), HIGH)
        crossing = nt(seg, jnp.broadcast_to(decx * jnp.concatenate(through, axis=1), (SUB, columns)), HIGH)[:, :1]
        total = (
            nn(suffix_in, lower, HIGH) + nn(prefix_in, (row_at < col_at).astype(F32), HIGH) + crossing
        )
        gd_ref[...] = total * -rate * (1.0 / (1.0 + jnp.exp(-p)))
        for copy in outs[:3]:
            copy.start()

    def total_hidden():
        total = red[x]
        if nx > 1:
            bulk(xland.at[:nx - 1], xsend, xrecv).wait_recv()
        for dx in range(1, nx):
            total = total + xland[(x + dx) % nx]
        gh_ref[...] = total.astype(gh_ref.dtype)
        outs[3].start()

    def drain():
        bulk(decb.at[:ny - 1], dsend, drecv).wait_send()
        bulk(ht.at[:ny - 1, :hz], hsend, hrecv).wait_send()
        if ntp > 1:
            bulk(hg.at[:ny - 1, :nz - hz], fsend, frecv).wait_send()
        for m in range(2):
            bulk(sbuf.at[m, :ny - 1], ysend.at[m], yrecv.at[m]).wait_send()
            bulk(tz.at[m, :nz - 1], tsend.at[m], trecv.at[m]).wait_send()
            bulk(cz.at[m, :nz - 1], csend.at[m], crecv.at[m]).wait_send()
            bulk(ob.at[m, :ny - 1], osend.at[m], orecv.at[m]).wait_send()
        bulk(gath.at[:ny - 1], gsend, grecv.at[0]).wait_send()
        if halves == 2:
            pair().wait_send()

    tasks = [
        (0.0, "project", project), (0.9, "columns_in", columns_in), (1.0, "stage_c1", functools.partial(stage_c, 1)),
        (7.2, "pairs", pairs), (13.0, "state_grads", state_grads), (15.0, "drain", drain),
        (18.2, "total_hidden", total_hidden),
    ]
    arrive = (6.5, 8.0, 10.5, 12.0)
    for c in range(tiles):
        ready = arrive[c % 4] + 7.0 * (c // 4)
        tasks.append((ready, f"multiply{c}", functools.partial(multiply, c)))
        last = ready
        for d in range(2):
            for j in slots(c, d):
                if fast(c) and j == 3:
                    continue
                if fast(c):
                    at = ready + (3.6 if j < 2 else 7.2) + 0.2 * (j % 2)
                    tasks.append((at, f"step{c}{d}{j}", functools.partial(step, c, d, j)))
                else:
                    at = ready + 2.7 * (j + 1)
                    tasks.append((at, f"hop{c}{d}{j}", functools.partial(hop, c, d, j)))
                last = max(last, at)
        tasks.append((last + 0.01, f"total{c}", functools.partial(total_weight, c)))
    for _, name, task in sorted(tasks, key=lambda item: item[0]):
        with jax.named_scope(name):
            task()

    with jax.named_scope("drain_ring"):
        bulk(part.at[:, :nz - 1], rsend, rrecv.at[0]).wait_send()
        if nx > 1:
            bulk(red.at[:nx - 1], xsend, xrecv).wait_send()
    with jax.named_scope("outs"):
        for copy in outs[:4]:
            copy.wait()
        pltpu.make_async_copy(gw_ref, gw_out, outsem.at[4]).wait()


def finish_kernel(*refs):
    count = (len(refs) - 1) // 3
    ins, outs, held, sems = refs[:count], refs[count:2 * count], refs[2 * count:3 * count], refs[-1]
    loads = [pltpu.make_async_copy(ins[k], held[k], sems.at[0, k]) for k in range(count)]
    stores = [pltpu.make_async_copy(held[k], outs[k], sems.at[1, k]) for k in range(count)]
    for load in loads:
        load.start()
    for load, store in zip(loads, stores):
        load.wait()
        store.start()
    for store in stores:
        store.wait()


HBM = pl.BlockSpec(memory_space=pltpu.HBM)
LIMIT = 60 * 1024 * 1024


def per_device(sp, tp, hidden, value_weight, key_vecs, queries, decay_pre, decay_rate, cotangent):
    length, features = hidden.shape
    heads = decay_rate.shape[0]
    state = key_vecs.shape[2]
    columns = value_weight.shape[1]
    ny = inner_size(sp)
    nz = sp // ny
    tiles = columns // LANES
    nr = state // nz
    rows = features // sp
    own = length // tp
    halves = 2 if tp % 2 == 0 else 1
    nx = tp // halves
    far = nz // 2
    steps = 2
    vm = pltpu.VMEM
    dma = pltpu.SemaphoreType.DMA
    outs = pl.pallas_call(
        functools.partial(mixer_kernel, ny, nz, tp),
        out_shape=(
            jax.ShapeDtypeStruct((length, state), BF16),
            jax.ShapeDtypeStruct((length, state), BF16),
            jax.ShapeDtypeStruct((heads, length), F32),
            jax.ShapeDtypeStruct((own, features), BF16),
            jax.ShapeDtypeStruct((rows, columns), F32),
        ),
        in_specs=[HBM] * 7,
        out_specs=(HBM,) * 5,
        scratch_shapes=[
            vm((length, state), BF16),
            vm((length, state), BF16),
            vm((heads, length), F32),
            vm((own, features), BF16),
            vm((rows, columns), F32),
            vm((length, features), BF16),
            vm((features, columns), BF16),
            vm((length, state), BF16),
            vm((length, state), BF16),
            vm((heads, length), F32),
            vm((1, heads), F32),
            vm((columns, length), BF16),
            vm((length, columns), BF16),
            vm((length, columns), F32),
            vm((length, columns), F32),
            vm((length, columns), F32),
            vm((heads, length, length), F32),
            vm((tiles, length, LANES), F32),
            vm((length, columns), BF16),
            vm((length, columns), F32),
            vm((heads, length), F32),
            vm((length, heads), F32),
            vm((length, state), F32),
            vm((length, state), F32),
            vm((2, ny, state, LANES), F32),
            vm((ny, SUB, LANES), F32),
            vm((2, ny, state, LANES), F32),
            vm((ny, SUB, LANES), F32),
            vm((2, nz, nr + SUB, LANES), F32),
            vm((2, nz, nr + SUB, LANES), F32),
            vm((2, nz, nr, LANES), F32),
            vm((2, nz, nr, LANES), F32),
            vm((2, ny, state, LANES), F32),
            vm((2, ny, state, LANES), F32),
            vm((ny, nz, rows, length), F32),
            vm((ny, nz, rows, length), F32),
            vm((nz, rows, ny * length), BF16),
            vm((ny, tiles, length, LANES), F32),
            vm((tiles, nz, rows, LANES), F32),
            vm((2, tiles, far, rows, LANES), F32),
            vm((halves, nx, own, features), F32),
            vm((nx, own, features), F32),
            vm((nx, own, features), F32),
            vm((nx, own, features), F32),
            dma((6,)), dma((steps,)),
            dma, dma,
            dma((2,)), dma((2,)),
            dma((2,)), dma((2,)),
            dma((2,)), dma((2,)),
            dma((2,)), dma((2,)),
            dma, dma,
            dma, dma,
            dma, dma((tiles,)),
            dma, dma((tiles * (nz - 1) - (4 if nz == 8 else 0),)),
            dma, dma,
            dma, dma,
            dma((5,)),
        ],
        compiler_params=pltpu.CompilerParams(collective_id=0, has_side_effects=True, vmem_limit_bytes=LIMIT),
        name="mixer_backward",
    )(
        hidden, value_weight, key_vecs.reshape(length, state), queries.reshape(length, state), decay_pre.T,
        decay_rate.reshape(1, heads), cotangent.reshape(length, columns).T,
    )
    gk, gq, gd, gh, gw = pl.pallas_call(
        finish_kernel,
        out_shape=tuple(jax.ShapeDtypeStruct(o.shape, o.dtype) for o in outs),
        in_specs=[HBM] * 5,
        out_specs=(HBM,) * 5,
        scratch_shapes=[vm(o.shape, o.dtype) for o in outs] + [dma((2, 5))],
        compiler_params=pltpu.CompilerParams(vmem_limit_bytes=LIMIT),
        name="write_out",
    )(*outs)
    return gk.reshape(key_vecs.shape), gq.reshape(key_vecs.shape), gd.T, gh, gw


def solution(mesh):
    return jax.shard_map(
        functools.partial(per_device, mesh.shape["sp"], mesh.shape["tp"]),
        mesh=mesh,
        in_specs=(
            P("sp", None),
            P(None, "tp"),
            P("sp", "tp", None),
            P("sp", "tp", None),
            P("sp", "tp"),
            P("tp"),
            P("sp", "tp", None),
        ),
        out_specs=(
            P("sp", "tp", None),
            P("sp", "tp", None),
            P("sp", "tp"),
            P(("sp", "tp"), None),
            P("sp", "tp"),
        ),
        check_vma=False,
    )
```

```python
import functools

import jax
import jax.numpy as jnp
from jax import lax
from jax.experimental import pallas as pl
from jax.experimental.pallas import tpu as pltpu
from jax.sharding import PartitionSpec as P

MESH = pl.DeviceIdType.MESH
F32 = jnp.float32
BF16 = jnp.bfloat16
HIGH = lax.Precision.HIGHEST
LANES = 128
SUB = 8


def inner_size(count):
    size = 1
    while size * size * 4 <= count:
        size *= 2
    while count % size:
        size -= 1
    return size


def remote(src, dst, send, recv, axis, index):
    return pltpu.make_async_remote_copy(
        src_ref=src, dst_ref=dst, send_sem=send, recv_sem=recv, device_id={axis: index}, device_id_type=MESH
    )


def nn(a, b, precision=None):
    return jnp.dot(a, b, preferred_element_type=F32, precision=precision)


def nt(a, b, precision=None):
    return lax.dot_general(a, b, (((1,), (1,)), ((), ())), preferred_element_type=F32, precision=precision)


def split(x):
    hi = x.astype(BF16)
    return hi, (x - hi.astype(F32)).astype(BF16)


def mixer_kernel(ny, nz, ntp, hid_hbm, w_hbm, key_hbm, qry_hbm, pre_hbm, rate_hbm, cot_hbm,
                 gk_out, gq_out, gd_out, gh_out, gw_out,
                 gk_ref, gq_ref, gd_ref, gh_ref, gw_ref, hid, wt, key, qry, pre, rate_ref, cott, cot,
                 ecot, tend, xval, damp, gvloc, gvb, kgs, rows8, cols8, gkl, gql,
                 sbuf, decb, ybuf, ydec, tz, zbuf, cz, zcar, ob, scr, ht, hg, hcol,
                 gath, part, ring, ghp, pland, red, xland,
                 insem, wsem, dsend, drecv, ysend, yrecv, tsend, trecv, csend, crecv, osend, orecv,
                 hsend, hrecv, fsend, frecv, gsend, grecv, rsend, rrecv, psend, precv, xsend, xrecv, outsem):
    me = lax.axis_index("sp")
    mine = lax.axis_index("tp")
    z, y = me // ny, me % ny
    length, features = hid.shape
    heads = pre.shape[0]
    columns = cot.shape[1]
    width = columns // heads
    tiles = columns // LANES
    per = LANES // width
    state = key.shape[1]
    groups = sbuf.shape[1]
    pack = tiles // groups
    rw = state // ny
    pr = pack * rw // nz
    rows = gw_ref.shape[0]
    own = gh_ref.shape[0]
    halves = 2 if ntp % 2 == 0 else 1
    core, x, nx = mine % halves, mine // halves, ntp // halves
    partner = mine + 1 - 2 * core
    hz = nz // ntp
    steps = wsem.shape[0]
    depth = features // steps
    ydev = [z * ny + (y + dy) % ny for dy in range(ny)]
    zdev = [((z + dz) % nz) * ny + y for dz in range(nz)]

    small = [
        pltpu.make_async_copy(pre_hbm, pre, insem.at[0]),
        pltpu.make_async_copy(rate_hbm, rate_ref, insem.at[4]),
        pltpu.make_async_copy(qry_hbm, qry, insem.at[1]),
        pltpu.make_async_copy(cot_hbm, cott, insem.at[2]),
        pltpu.make_async_copy(key_hbm, key, insem.at[3]),
    ]
    for copy in small:
        copy.start()
    wcopies = []
    for k in range(steps):
        at = pl.ds(k * depth, depth)
        wcopies.append(pltpu.make_async_copy(w_hbm.at[at, :], wt.at[at, :], wsem.at[k]))
    hload = pltpu.make_async_copy(hid_hbm, hid, insem.at[5])
    hload.start()
    for copy in wcopies:
        copy.start()

    outs = [
        pltpu.make_async_copy(gk_ref, gk_out, outsem.at[0]),
        pltpu.make_async_copy(gq_ref, gq_out, outsem.at[1]),
        pltpu.make_async_copy(gd_ref, gd_out, outsem.at[2]),
        pltpu.make_async_copy(gh_ref, gh_out, outsem.at[3]),
    ]
    for c in range(tiles):
        at = pl.ds(c * LANES, LANES)
        outs.append(pltpu.make_async_copy(gw_ref.at[:, at], gw_out.at[:, at], outsem.at[4]))

    barrier = pltpu.get_barrier_semaphore()
    for dev in ydev[1:] + zdev[1:]:
        pl.semaphore_signal(barrier, inc=1, device_id={"sp": dev}, device_id_type=MESH)
    for dt in range(1, ntp):
        pl.semaphore_signal(barrier, inc=1, device_id={"tp": (mine + dt) % ntp}, device_id_type=MESH)

    def dcopy(dy, arrive=False):
        slot = (y + dy) % ny if arrive else y
        return remote(decb, ydec.at[slot], dsend, drecv, "sp", ydev[dy])

    def ycopy(m, g, dy):
        there = (y + dy) % ny
        return remote(sbuf.at[m, g, there], ybuf.at[m, g, y], ysend, yrecv.at[m, g], "sp", ydev[dy])

    def tcopy(m, g, dz):
        there = (z + dz) % nz
        return remote(tz.at[m, g, there], zbuf.at[m, g, z], tsend, trecv.at[m, g], "sp", zdev[dz])

    def ccopy(m, g, dz):
        there = (z + dz) % nz
        return remote(cz.at[m, g, there], zcar.at[m, g, z], csend, crecv.at[m, g], "sp", zdev[dz])

    def ocopy(m, g, dy):
        there = (y + dy) % ny
        return remote(ob.at[m, g, there], scr.at[m, g, y], osend, orecv.at[m, g], "sp", ydev[dy])

    def section(k):
        return pl.ds(pl.multiple_of(k * hz, hz), hz)

    def hcopy(dy, arrive=False):
        there = (y + dy) % ny
        slot = there if arrive else y
        return remote(
            ht.at[there, section(mine)], hg.at[slot, section(mine)], hsend, hrecv, "sp", ydev[dy]
        )

    def share(dy, dt, arrive=False):
        there = (y + dy) % ny
        peer = (mine + dt) % ntp
        which = peer if arrive else mine
        block = hg.at[there, section(which)]
        return remote(block, block, fsend, frecv, "tp", peer)

    def gcopy(c, dy, arrive=False):
        there = (y + dy) % ny
        slot = there if arrive else y
        return remote(gath.at[slot, c], gath.at[slot, c], gsend, grecv.at[c], "sp", ydev[dy])

    def pair():
        return remote(ghp.at[1 - core], pland, psend, precv, "tp", partner)

    def xcopy(dx, arrive=False):
        there = (x + dx) % nx
        slot = there if arrive else x
        return remote(red.at[there], xland.at[slot], xsend, xrecv, "tp", there * halves + core)

    def reach(c, d):
        far = nz // 2
        return far if (c + d) % 2 == 0 else nz - 1 - far

    def fast(c):
        return nz == 8 and c >= tiles - 2

    def ahead(k, d):
        return (z + k) % nz if d == 0 else (z + nz - k) % nz

    def rcopy(c, d, j):
        src = part.at[c, ahead(reach(c, d), d)] if j == 0 else ring.at[d, c, j - 1]
        return remote(
            src, ring.at[d, c, j], rsend, rrecv.at[slot_at(c, d, j)], "sp", zdev[1] if d == 0 else zdev[nz - 1]
        )

    def scopy(c, d, j):
        if j == 0:
            src, hops = part.at[c, ahead(4, d)], 2
        elif j == 1:
            src, hops = part.at[c, ahead(3, d)], 2
        elif j == 2:
            src, hops = (ring.at[d, c, 0] if reach(c, d) == 4 else part.at[c, ahead(2, d)]), 2
        else:
            src, hops = ring.at[d, c, 1], 1
        return remote(
            src, ring.at[d, c, j], rsend, rrecv.at[slot_at(c, d, j)], "sp", zdev[hops if d == 0 else nz - hops]
        )

    def slots(c, d):
        if fast(c):
            return (0, 1, 2, 3) if reach(c, d) == 4 else (1, 2, 3)
        return tuple(range(reach(c, d)))

    ring_slots = sorted({(c, d, min(j, 2) if fast(c) else j) for c in range(tiles) for d in range(2) for j in slots(c, d)})

    def slot_at(c, d, j):
        return ring_slots.index((c, d, min(j, 2) if fast(c) else j))

    def bulk(ref, send, recv):
        return remote(ref, ref, send, recv, "sp", ydev[1])

    row_at = lax.broadcasted_iota(jnp.int32, (length, length), 0)
    col_at = lax.broadcasted_iota(jnp.int32, (length, length), 1)
    eye = (row_at == col_at).astype(BF16)
    seg = (
        lax.broadcasted_iota(jnp.int32, (heads, columns), 1) // width
        == lax.broadcasted_iota(jnp.int32, (heads, columns), 0)
    ).astype(F32)
    lane = lax.broadcasted_iota(jnp.int32, (length, LANES), 1) // width

    def tile(q):
        return slice(q * LANES, (q + 1) * LANES)

    same = (
        lax.broadcasted_iota(jnp.int32, (heads, heads), 0) == lax.broadcasted_iota(jnp.int32, (heads, heads), 1)
    ).astype(F32)
    small[0].wait()
    small[1].wait()
    p = pre[...]
    rate = nt(same, jnp.broadcast_to(rate_ref[...], (heads, heads)), HIGH)[:, :1]
    log_decay = -rate * (jnp.maximum(p, 0.0) + jnp.log1p(jnp.exp(-jnp.abs(p))))
    lower = (row_at >= col_at).astype(F32)
    cum = nt(lower, log_decay, HIGH)
    cumt = nt(log_decay, lower, HIGH)
    cumx = nn(cum, seg, HIGH)
    totx = cumx[length - 1:length]
    decx = jnp.exp(totx)
    small[2].wait()
    small[3].wait()
    for q in range(tiles):
        cot[:, tile(q)] = nt(eye, cott[tile(q), :]).astype(BF16)
    ec = jnp.exp(cumx) * cot[...].astype(F32)
    ecot[...] = ec
    qryt = nt(eye, qry[...]).astype(BF16)
    hi, lo = split(ec)
    pull = nn(qryt, hi) + nn(qryt, lo)
    def spread(m, whole):
        for g in range(groups):
            for yy in range(ny):
                for i in range(pack):
                    sbuf[m, g, yy, i * rw:(i + 1) * rw] = whole[yy * rw:(yy + 1) * rw, tile(g * pack + i)]

    spread(0, pull)
    for q in range(tiles):
        decb[q:q + 1, :] = decx[:, tile(q)]

    with jax.named_scope("barrier"):
        pl.semaphore_wait(barrier, ny - 1 + nz - 1 + ntp - 1)
    for dy in range(1, ny):
        dcopy(dy).start()
    for g in range(groups):
        for dy in range(1, ny):
            ycopy(0, g, dy).start()
    ydec[y] = decb[...]
    ybuf[0, :, y] = sbuf[0, :, y]

    hload.wait()
    for b in range(features // LANES):
        block = nt(eye, hid[:, tile(b)])
        for i in range(LANES // rows):
            owner = b * LANES // rows + i
            ht[owner % ny, owner // ny] = block[i * rows:(i + 1) * rows]
    with jax.named_scope("send_h"):
        for dy in range(1, ny):
            hcopy(dy).start()
    tend[...] = jnp.exp(totx - cumx)
    small[4].wait()
    values = jnp.zeros((length, columns), F32)
    for k in range(steps):
        wcopies[k].wait()
        values = values + nn(hid[:, k * depth:(k + 1) * depth], wt[k * depth:(k + 1) * depth, :])
    vals = values.astype(BF16)
    xv = tend[...] * vals.astype(F32)
    xval[...] = xv
    keyt = nt(eye, key[...]).astype(BF16)
    hi, lo = split(xv)
    push = nn(keyt, hi) + nn(keyt, lo)
    spread(1, push)
    with jax.named_scope("send_y1"):
        for g in range(groups):
            for dy in range(1, ny):
                ycopy(1, g, dy).start()
    ybuf[1, :, y] = sbuf[1, :, y]

    hcol[:, :, pl.ds(pl.multiple_of(y * length, LANES), length)] = ht[y].astype(BF16)

    def scan_order(m, count):
        return list(range(count)) if m == 1 else list(reversed(range(count)))

    def stage_y(m, g):
        if m == 0 and g == 0:
            bulk(ydec.at[:ny - 1], dsend, drecv).wait_recv()
        bulk(ybuf.at[m, g, :ny - 1], ysend, yrecv.at[m, g]).wait_recv()
        order = scan_order(m, ny)
        for i in range(pack):
            q, at = g * pack + i, slice(i * rw, (i + 1) * rw)
            run = ybuf[m, g, order[0], at]
            for yy in order[1:]:
                run = ydec[yy, q:q + 1] * run + ybuf[m, g, yy, at]
            prod = ydec[0, q:q + 1]
            for yy in range(1, ny):
                prod = prod * ydec[yy, q:q + 1]
            prod = jnp.broadcast_to(prod, (SUB, LANES))
            for k in range(rw // pr):
                tz[m, g, i * (rw // pr) + k, :pr] = run[k * pr:(k + 1) * pr]
                tz[m, g, i * (rw // pr) + k, pr:] = prod
        for dz in sorted(range(1, nz), key=lambda dz: -min(dz, nz - dz)):
            tcopy(m, g, dz).start()
        zbuf[m, g, z] = tz[m, g, z]

    def stage_z(m, g):
        bulk(zbuf.at[m, g, :nz - 1], tsend, trecv.at[m, g]).wait_recv()
        run = jnp.zeros((pr, LANES), F32)
        for zz in scan_order(m, nz):
            cz[m, g, zz] = run
            run = zbuf[m, g, zz, pr:pr + 1] * run + zbuf[m, g, zz, :pr]
        for dz in sorted(range(1, nz), key=lambda dz: -min(dz, nz - dz)):
            ccopy(m, g, dz).start()
        zcar[m, g, z] = cz[m, g, z]

    def stage_c(m, g):
        bulk(zcar.at[m, g, :nz - 1], csend, crecv.at[m, g]).wait_recv()
        carry = zcar[m, g].reshape(pack * rw, LANES)
        for i in range(pack):
            q, at = g * pack + i, slice(i * rw, (i + 1) * rw)
            now = carry[at]
            for yy in scan_order(m, ny):
                ob[m, g, yy, at] = now
                now = ydec[yy, q:q + 1] * now + ybuf[m, g, yy, at]
        for dy in sorted(range(1, ny), key=lambda dy: -min(dy, ny - dy)):
            ocopy(m, g, dy).start()
        scr[m, g, y] = ob[m, g, y]

    def stage(name, work, m):
        for g in range(groups):
            with jax.named_scope(f"{name}{m}{g}"):
                work(m, g)

    def state_tile(m, q):
        g, i = q // pack, q % pack
        return scr[m, g, :, i * rw:(i + 1) * rw].reshape(state, LANES)

    stage("stage_y", stage_y, 0)

    causal = row_at <= col_at
    scores = nt(key[...], qry[...])
    for q in range(tiles):
        lefts, rights = [], []
        ct = cot[:, tile(q)]
        for i in range(per):
            h = q * per + i
            across = cumt[h:h + 1, :] - cum[:, h:h + 1]
            dm = jnp.where(causal, jnp.exp(jnp.where(causal, across, 0.0)), 0.0)
            damp[h] = dm
            lefts.extend(split(scores * dm))
            masked = jnp.where(lane == i, ct, jnp.zeros_like(ct))
            rights.extend([masked, masked])
        gvloc[q] = nn(jnp.concatenate(lefts, axis=1), jnp.concatenate(rights, axis=0))

    with jax.named_scope("hid_y"):
        bulk(hg.at[:ny - 1, :hz], hsend, hrecv).wait_recv()
        for dt in range(1, ntp):
            for dy in range(1, ny):
                share(dy, dt).start()

    stage("stage_z", stage_z, 0)

    stage("stage_y", stage_y, 1)

    dsum = jnp.zeros((length, length), F32)
    for q in range(tiles):
        vt = vals[:, tile(q)]
        both = nt(
            jnp.concatenate([jnp.where(lane == i, vt, jnp.zeros_like(vt)) for i in range(per)], axis=0),
            cot[:, tile(q)],
        )
        for i in range(per):
            h = q * per + i
            ds = both[i * length:(i + 1) * length] * damp[h]
            flux = ds * scores
            dsum = dsum + ds
            rows8[h:h + 1, :] = jnp.sum(flux, axis=0, keepdims=True)
            cols8[:, h:h + 1] = jnp.sum(flux, axis=1, keepdims=True)

    stage("stage_c", stage_c, 0)

    hi, lo = split(dsum)
    gkl[...] = nn(hi, qry[...]) + nn(lo, qry[...])
    hi, lo = split(dsum.T)
    gql[...] = nn(hi, key[...]) + nn(lo, key[...])
    stage("stage_z", stage_z, 1)

    for g in range(groups):
        with jax.named_scope(f"wait_o0{g}"):
            bulk(scr.at[0, g, :ny - 1], osend, orecv.at[0, g]).wait_recv()
        for q in range(g * pack, (g + 1) * pack):
            hi, lo = split(state_tile(0, q))
            kg = nn(key[...], hi) + nn(key[...], lo)
            kgs[:, tile(q)] = kg
            gb = (gvloc[q] + tend[:, tile(q)] * kg).astype(BF16)
            gvb[:, tile(q)] = gb
            gath[y, q] = gb.astype(F32)
            for dy in sorted(range(1, ny), key=lambda dy: -min(dy, ny - dy)):
                gcopy(q, dy).start()

    def columns_in():
        if ntp > 1:
            bulk(hg.at[:ny - 1, :nz - hz], fsend, frecv).wait_recv()
        for dy in range(1, ny):
            there = (y + dy) % ny
            hcol[:, :, pl.ds(pl.multiple_of(there * length, LANES), length)] = hg[there].astype(BF16)

    def multiply(c):
        bulk(gath.at[:ny - 1, c], gsend, grecv.at[c]).wait_recv()
        block = gath[:, c].reshape(ny * length, LANES).astype(BF16)
        part[c] = nn(hcol[...].reshape(nz * rows, ny * length), block).reshape(nz, rows, LANES)
        for d in range(2):
            if fast(c):
                for j in slots(c, d):
                    if j < 2 or (j == 2 and reach(c, d) == 3):
                        scopy(c, d, j).start()
            elif reach(c, d) > 0:
                rcopy(c, d, 0).start()

    def hop(c, d, j):
        rcopy(c, d, j).wait_recv()
        left = reach(c, d) - 1 - j
        if left > 0:
            ring[d, c, j] = ring[d, c, j] + part[c, ahead(left, d)]
            rcopy(c, d, j + 1).start()

    def step(c, d, j):
        if j == 2:
            bulk(ring.at[d, c, 2:4], rsend, rrecv.at[slot_at(c, d, 2)]).wait_recv()
        else:
            scopy(c, d, j).wait_recv()
            ring[d, c, j] = ring[d, c, j] + part[c, ahead(2 - j, d)]
            scopy(c, d, j + 2).start()

    def total_weight(c):
        total = part[c, z]
        for d in range(2):
            if fast(c):
                total = total + (ring[d, c, 2] + ring[d, c, 3])
            elif reach(c, d) > 0:
                total = total + ring[d, c, reach(c, d) - 1]
        gw_ref[:, tile(c)] = total
        outs[4 + c].start()

    def project():
        block = nt(gvb[...], wt[...])
        for t in range(ntp):
            ghp[t % halves, t // halves] = block[t * own:(t + 1) * own]
        if halves == 2:
            pair().start()

    def pairs():
        if halves == 2:
            pair().wait_recv()
            red[...] = ghp[core] + pland[...]
        else:
            red[...] = ghp[0]
        for dx in range(1, nx):
            xcopy(dx).start()

    def key_grads():
        gk = gkl[...]
        pulled = []
        for q in range(tiles):
            sgh, sgl = split(state_tile(0, q))
            xq = xval[:, tile(q)]
            xh, xl = split(xq)
            gk = gk + (nt(xh, sgh) + nt(xl, sgh) + nt(xh, sgl))
            pulled.append(xq * kgs[:, tile(q)])
        gk_ref[...] = gk.astype(BF16)
        outs[0].start()
        prefix_in = nt(seg, jnp.concatenate(pulled, axis=1), HIGH)
        gd_ref[...] = nn(prefix_in, (row_at < col_at).astype(F32), HIGH)

    def query_grads():
        with jax.named_scope("wait_o1"):
            for g in range(groups):
                bulk(scr.at[1, g, :ny - 1], osend, orecv.at[1, g]).wait_recv()
        gq = gql[...]
        into, through = [], []
        for q in range(tiles):
            si, sg = state_tile(1, q), state_tile(0, q)
            sih, sil = split(si)
            eq = ecot[:, tile(q)]
            eh, el = split(eq)
            gq = gq + (nt(eh, sih) + nt(el, sih) + nt(eh, sil))
            into.append(eq * (nn(qry[...], sih) + nn(qry[...], sil)))
            through.append(jnp.sum(si * sg, axis=0, keepdims=True))
        gq_ref[...] = gq.astype(BF16)
        outs[1].start()
        suffix_in = nt(seg, jnp.concatenate(into, axis=1), HIGH) - nt(same, cols8[...], HIGH) + rows8[...]
        crossing = nt(seg, jnp.broadcast_to(decx * jnp.concatenate(through, axis=1), (SUB, columns)), HIGH)[:, :1]
        total = nn(suffix_in, lower, HIGH) + gd_ref[...] + crossing
        gd_ref[...] = total * -rate * (1.0 / (1.0 + jnp.exp(-p)))
        outs[2].start()

    def total_hidden():
        total = red[x]
        if nx > 1:
            bulk(xland.at[:nx - 1], xsend, xrecv).wait_recv()
        for dx in range(1, nx):
            total = total + xland[(x + dx) % nx]
        gh_ref[...] = total.astype(gh_ref.dtype)
        outs[3].start()

    def drain():
        bulk(ydec.at[:ny - 1], dsend, drecv).wait_send()
        bulk(ht.at[:ny - 1, :hz], hsend, hrecv).wait_send()
        if ntp > 1:
            bulk(hg.at[:ny - 1, :nz - hz], fsend, frecv).wait_send()
        bulk(sbuf.at[:, :, :ny - 1], ysend, yrecv.at[0, 0]).wait_send()
        bulk(tz.at[:, :, :nz - 1], tsend, trecv.at[0, 0]).wait_send()
        bulk(cz.at[:, :, :nz - 1], csend, crecv.at[0, 0]).wait_send()
        bulk(ob.at[:, :, :ny - 1], osend, orecv.at[0, 0]).wait_send()
        bulk(gath.at[:ny - 1], gsend, grecv.at[0]).wait_send()
        if halves == 2:
            pair().wait_send()

    tasks = [
        (1.0, "project", project), (1.9, "columns_in", columns_in),
        (2.0, "stage_c1", functools.partial(stage, "stage_c", stage_c, 1)), (3.0, "key_grads", key_grads),
        (9.6, "pairs", pairs), (15.2, "query_grads", query_grads), (15.1, "drain", drain),
        (18.2, "total_hidden", total_hidden),
    ]
    arrive = (4.5, 6.0, 8.5, 11.0)
    for c in range(tiles):
        ready = arrive[c % 4] + 7.0 * (c // 4)
        tasks.append((ready, f"multiply{c}", functools.partial(multiply, c)))
        last = ready
        for d in range(2):
            for j in slots(c, d):
                if fast(c) and j == 3:
                    continue
                if fast(c):
                    at = ready + (4.0 if j < 2 else 8.0) + 0.2 * (j % 2)
                    tasks.append((at, f"step{c}{d}{j}", functools.partial(step, c, d, j)))
                else:
                    at = ready + 3.5 * (j + 1)
                    tasks.append((at, f"hop{c}{d}{j}", functools.partial(hop, c, d, j)))
                last = max(last, at)
        tasks.append((last + 0.01, f"total{c}", functools.partial(total_weight, c)))
    for _, name, task in sorted(tasks, key=lambda item: item[0]):
        with jax.named_scope(name):
            task()

    with jax.named_scope("drain_ring"):
        bulk(part.at[:, :nz - 1], rsend, rrecv.at[0]).wait_send()
        if nx > 1:
            bulk(red.at[:nx - 1], xsend, xrecv).wait_send()
    with jax.named_scope("outs"):
        for copy in outs[:4]:
            copy.wait()
        pltpu.make_async_copy(gw_ref, gw_out, outsem.at[4]).wait()


def finish_kernel(*refs):
    count = (len(refs) - 1) // 3
    ins, outs, held, sems = refs[:count], refs[count:2 * count], refs[2 * count:3 * count], refs[-1]
    loads = [pltpu.make_async_copy(ins[k], held[k], sems.at[0, k]) for k in range(count)]
    stores = [pltpu.make_async_copy(held[k], outs[k], sems.at[1, k]) for k in range(count)]
    for load in loads:
        load.start()
    for load, store in zip(loads, stores):
        load.wait()
        store.start()
    for store in stores:
        store.wait()


HBM = pl.BlockSpec(memory_space=pltpu.HBM)
LIMIT = 60 * 1024 * 1024


def per_device(sp, tp, hidden, value_weight, key_vecs, queries, decay_pre, decay_rate, cotangent):
    length, features = hidden.shape
    heads = decay_rate.shape[0]
    state = key_vecs.shape[2]
    columns = value_weight.shape[1]
    ny = inner_size(sp)
    nz = sp // ny
    tiles = columns // LANES
    groups = 2
    pack = tiles // groups
    rw = state // ny
    pr = pack * rw // nz
    rows = features // sp
    own = length // tp
    halves = 2 if tp % 2 == 0 else 1
    nx = tp // halves
    far = nz // 2
    steps = 2
    vm = pltpu.VMEM
    dma = pltpu.SemaphoreType.DMA
    outs = pl.pallas_call(
        functools.partial(mixer_kernel, ny, nz, tp),
        out_shape=(
            jax.ShapeDtypeStruct((length, state), BF16),
            jax.ShapeDtypeStruct((length, state), BF16),
            jax.ShapeDtypeStruct((heads, length), F32),
            jax.ShapeDtypeStruct((own, features), BF16),
            jax.ShapeDtypeStruct((rows, columns), F32),
        ),
        in_specs=[HBM] * 7,
        out_specs=(HBM,) * 5,
        scratch_shapes=[
            vm((length, state), BF16),
            vm((length, state), BF16),
            vm((heads, length), F32),
            vm((own, features), BF16),
            vm((rows, columns), F32),
            vm((length, features), BF16),
            vm((features, columns), BF16),
            vm((length, state), BF16),
            vm((length, state), BF16),
            vm((heads, length), F32),
            vm((1, heads), F32),
            vm((columns, length), BF16),
            vm((length, columns), BF16),
            vm((length, columns), F32),
            vm((length, columns), F32),
            vm((length, columns), F32),
            vm((heads, length, length), F32),
            vm((tiles, length, LANES), F32),
            vm((length, columns), BF16),
            vm((length, columns), F32),
            vm((heads, length), F32),
            vm((length, heads), F32),
            vm((length, state), F32),
            vm((length, state), F32),
            vm((2, groups, ny, pack * rw, LANES), F32),
            vm((SUB, LANES), F32),
            vm((2, groups, ny, pack * rw, LANES), F32),
            vm((ny, SUB, LANES), F32),
            vm((2, groups, nz, pr + SUB, LANES), F32),
            vm((2, groups, nz, pr + SUB, LANES), F32),
            vm((2, groups, nz, pr, LANES), F32),
            vm((2, groups, nz, pr, LANES), F32),
            vm((2, groups, ny, pack * rw, LANES), F32),
            vm((2, groups, ny, pack * rw, LANES), F32),
            vm((ny, nz, rows, length), F32),
            vm((ny, nz, rows, length), F32),
            vm((nz, rows, ny * length), BF16),
            vm((ny, tiles, length, LANES), F32),
            vm((tiles, nz, rows, LANES), F32),
            vm((2, tiles, far, rows, LANES), F32),
            vm((halves, nx, own, features), F32),
            vm((nx, own, features), F32),
            vm((nx, own, features), F32),
            vm((nx, own, features), F32),
            dma((6,)), dma((steps,)),
            dma, dma,
            dma, dma((2, groups)),
            dma, dma((2, groups)),
            dma, dma((2, groups)),
            dma, dma((2, groups)),
            dma, dma,
            dma, dma,
            dma, dma((tiles,)),
            dma, dma((tiles * (nz - 1) - (2 * 2 if nz == 8 else 0),)),
            dma, dma,
            dma, dma,
            dma((5,)),
        ],
        compiler_params=pltpu.CompilerParams(collective_id=0, has_side_effects=True, vmem_limit_bytes=LIMIT),
        name="mixer_backward",
    )(
        hidden, value_weight, key_vecs.reshape(length, state), queries.reshape(length, state), decay_pre.T,
        decay_rate.reshape(1, heads), cotangent.reshape(length, columns).T,
    )
    gk, gq, gd, gh, gw = pl.pallas_call(
        finish_kernel,
        out_shape=tuple(jax.ShapeDtypeStruct(o.shape, o.dtype) for o in outs),
        in_specs=[HBM] * 5,
        out_specs=(HBM,) * 5,
        scratch_shapes=[vm(o.shape, o.dtype) for o in outs] + [dma((2, 5))],
        compiler_params=pltpu.CompilerParams(vmem_limit_bytes=LIMIT),
        name="write_out",
    )(*outs)
    return gk.reshape(key_vecs.shape), gq.reshape(key_vecs.shape), gd.T, gh, gw


def solution(mesh):
    return jax.shard_map(
        functools.partial(per_device, mesh.shape["sp"], mesh.shape["tp"]),
        mesh=mesh,
        in_specs=(
            P("sp", None),
            P(None, "tp"),
            P("sp", "tp", None),
            P("sp", "tp", None),
            P("sp", "tp"),
            P("tp"),
            P("sp", "tp", None),
        ),
        out_specs=(
            P("sp", "tp", None),
            P("sp", "tp", None),
            P("sp", "tp"),
            P(("sp", "tp"), None),
            P("sp", "tp"),
        ),
        check_vma=False,
    )
```

```python
import functools

import jax
import jax.numpy as jnp
from jax import lax
from jax.experimental import pallas as pl
from jax.experimental.pallas import tpu as pltpu
from jax.sharding import PartitionSpec as P

MESH = pl.DeviceIdType.MESH
F32 = jnp.float32
BF16 = jnp.bfloat16
HIGH = lax.Precision.HIGHEST
LANES = 128
SUB = 8


def inner_size(count):
    size = 1
    while size * size * 4 <= count:
        size *= 2
    while count % size:
        size -= 1
    return size


def remote(src, dst, send, recv, axis, index):
    return pltpu.make_async_remote_copy(
        src_ref=src, dst_ref=dst, send_sem=send, recv_sem=recv, device_id={axis: index}, device_id_type=MESH
    )


def nn(a, b, precision=None):
    return jnp.dot(a, b, preferred_element_type=F32, precision=precision)


def nt(a, b, precision=None):
    return lax.dot_general(a, b, (((1,), (1,)), ((), ())), preferred_element_type=F32, precision=precision)


def split(x):
    hi = x.astype(BF16)
    return hi, (x - hi.astype(F32)).astype(BF16)


def mixer_kernel(ny, nz, ntp, hid_hbm, w_hbm, key_hbm, qry_hbm, pre_hbm, rate_hbm, cot_hbm,
                 gk_out, gq_out, gd_out, gh_out, gw_out,
                 gk_ref, gq_ref, gd_ref, gh_ref, gw_ref, hid, wt, key, qry, pre, rate_ref, cott, cot,
                 ecot, tend, xval, damp, gvloc, gvb, kgs, rows8, cols8, gkl, gql,
                 sbuf, decb, ybuf, ydec, tz, zbuf, cz, zcar, crow, ob, scr, ht, hg, hcol,
                 gath, part, ring, ghp, pland, red, xland,
                 insem, wsem, dsend, drecv, ysend, yrecv, tsend, trecv, csend, crecv, osend, orecv,
                 hsend, hrecv, fsend, frecv, gsend, grecv, rsend, rrecv, psend, precv, xsend, xrecv, outsem):
    me = lax.axis_index("sp")
    mine = lax.axis_index("tp")
    z, y = me // ny, me % ny
    length, features = hid.shape
    heads = pre.shape[0]
    columns = cot.shape[1]
    width = columns // heads
    tiles = columns // LANES
    per = LANES // width
    state = key.shape[1]
    groups = sbuf.shape[1]
    pack = tiles // groups
    rw = state // ny
    pr = pack * rw // nz
    rows = gw_ref.shape[0]
    own = gh_ref.shape[0]
    halves = 2 if ntp % 2 == 0 else 1
    core, x, nx = mine % halves, mine // halves, ntp // halves
    partner = mine + 1 - 2 * core
    hz = nz // ntp
    steps = wsem.shape[0]
    depth = features // steps
    ydev = [z * ny + (y + dy) % ny for dy in range(ny)]
    zdev = [((z + dz) % nz) * ny + y for dz in range(nz)]

    small = [
        pltpu.make_async_copy(pre_hbm, pre, insem.at[0]),
        pltpu.make_async_copy(rate_hbm, rate_ref, insem.at[4]),
        pltpu.make_async_copy(qry_hbm, qry, insem.at[1]),
        pltpu.make_async_copy(cot_hbm, cott, insem.at[2]),
        pltpu.make_async_copy(key_hbm, key, insem.at[3]),
    ]
    for copy in small:
        copy.start()
    wcopies = []
    for k in range(steps):
        at = pl.ds(k * depth, depth)
        wcopies.append(pltpu.make_async_copy(w_hbm.at[at, :], wt.at[at, :], wsem.at[k]))
    hload = pltpu.make_async_copy(hid_hbm, hid, insem.at[5])
    hload.start()
    for copy in wcopies:
        copy.start()

    outs = [
        pltpu.make_async_copy(gk_ref, gk_out, outsem.at[0]),
        pltpu.make_async_copy(gq_ref, gq_out, outsem.at[1]),
        pltpu.make_async_copy(gd_ref, gd_out, outsem.at[2]),
        pltpu.make_async_copy(gh_ref, gh_out, outsem.at[3]),
    ]
    for c in range(tiles):
        at = pl.ds(c * LANES, LANES)
        outs.append(pltpu.make_async_copy(gw_ref.at[:, at], gw_out.at[:, at], outsem.at[4]))

    barrier = pltpu.get_barrier_semaphore()
    for dev in ydev[1:] + zdev[1:]:
        pl.semaphore_signal(barrier, inc=1, device_id={"sp": dev}, device_id_type=MESH)
    for dt in range(1, ntp):
        pl.semaphore_signal(barrier, inc=1, device_id={"tp": (mine + dt) % ntp}, device_id_type=MESH)

    def dcopy(dy, arrive=False):
        slot = (y + dy) % ny if arrive else y
        return remote(decb, ydec.at[slot], dsend, drecv, "sp", ydev[dy])

    def ycopy(m, g, dy):
        there = (y + dy) % ny
        return remote(sbuf.at[m, g, there], ybuf.at[m, g, y], ysend, yrecv.at[m, g], "sp", ydev[dy])

    def tcopy(m, g, dz):
        there = (z + dz) % nz
        return remote(tz.at[m, g, there], zbuf.at[m, g, z], tsend, trecv.at[m, g], "sp", zdev[dz])

    def ccopy(m, g, dz):
        there = (z + dz) % nz
        return remote(cz.at[m, g, there], zcar.at[m, g, z], csend, crecv.at[m, g], "sp", zdev[dz])

    def ocopy(m, g, dy):
        there = (y + dy) % ny
        return remote(ob.at[m, g, there], scr.at[m, g, y], osend, orecv.at[m, g], "sp", ydev[dy])

    def section(k):
        return pl.ds(pl.multiple_of(k * hz, hz), hz)

    def hcopy(dy, arrive=False):
        there = (y + dy) % ny
        slot = there if arrive else y
        return remote(
            ht.at[there, section(mine)], hg.at[slot, section(mine)], hsend, hrecv, "sp", ydev[dy]
        )

    def share(dy, dt, arrive=False):
        there = (y + dy) % ny
        peer = (mine + dt) % ntp
        which = peer if arrive else mine
        block = hg.at[there, section(which)]
        return remote(block, block, fsend, frecv, "tp", peer)

    def gcopy(c, dy, arrive=False):
        there = (y + dy) % ny
        slot = there if arrive else y
        return remote(gath.at[slot, c], gath.at[slot, c], gsend, grecv.at[c], "sp", ydev[dy])

    def pair():
        return remote(ghp.at[1 - core], pland, psend, precv, "tp", partner)

    def xcopy(dx, arrive=False):
        there = (x + dx) % nx
        slot = there if arrive else x
        return remote(red.at[there], xland.at[slot], xsend, xrecv, "tp", there * halves + core)

    def reach(c, d):
        far = nz // 2
        return far if (c + d) % 2 == 0 else nz - 1 - far

    def fast(c):
        return nz == 8 and c >= tiles - 2

    def ahead(k, d):
        return (z + k) % nz if d == 0 else (z + nz - k) % nz

    def rcopy(c, d, j):
        src = part.at[c, ahead(reach(c, d), d)] if j == 0 else ring.at[d, c, j - 1]
        return remote(
            src, ring.at[d, c, j], rsend, rrecv.at[slot_at(c, d, j)], "sp", zdev[1] if d == 0 else zdev[nz - 1]
        )

    def scopy(c, d, j):
        if j == 0:
            src, hops = part.at[c, ahead(4, d)], 2
        elif j == 1:
            src, hops = part.at[c, ahead(3, d)], 2
        elif j == 2:
            src, hops = (ring.at[d, c, 0] if reach(c, d) == 4 else part.at[c, ahead(2, d)]), 2
        else:
            src, hops = ring.at[d, c, 1], 1
        return remote(
            src, ring.at[d, c, j], rsend, rrecv.at[slot_at(c, d, j)], "sp", zdev[hops if d == 0 else nz - hops]
        )

    def slots(c, d):
        if fast(c):
            return (0, 1, 2, 3) if reach(c, d) == 4 else (1, 2, 3)
        return tuple(range(reach(c, d)))

    ring_slots = sorted({(c, d, min(j, 2) if fast(c) else j) for c in range(tiles) for d in range(2) for j in slots(c, d)})

    def slot_at(c, d, j):
        return ring_slots.index((c, d, min(j, 2) if fast(c) else j))

    def bulk(ref, send, recv):
        return remote(ref, ref, send, recv, "sp", ydev[1])

    row_at = lax.broadcasted_iota(jnp.int32, (length, length), 0)
    col_at = lax.broadcasted_iota(jnp.int32, (length, length), 1)
    eye = (row_at == col_at).astype(BF16)
    seg = (
        lax.broadcasted_iota(jnp.int32, (heads, columns), 1) // width
        == lax.broadcasted_iota(jnp.int32, (heads, columns), 0)
    ).astype(F32)
    lane = lax.broadcasted_iota(jnp.int32, (length, LANES), 1) // width

    def tile(q):
        return slice(q * LANES, (q + 1) * LANES)

    same = (
        lax.broadcasted_iota(jnp.int32, (heads, heads), 0) == lax.broadcasted_iota(jnp.int32, (heads, heads), 1)
    ).astype(F32)
    small[0].wait()
    small[1].wait()
    p = pre[...]
    rate = nt(same, jnp.broadcast_to(rate_ref[...], (heads, heads)), HIGH)[:, :1]
    log_decay = -rate * (jnp.maximum(p, 0.0) + jnp.log1p(jnp.exp(-jnp.abs(p))))
    lower = (row_at >= col_at).astype(F32)
    cum = nt(lower, log_decay, HIGH)
    cumt = nt(log_decay, lower, HIGH)
    cumx = nn(cum, seg, HIGH)
    totx = cumx[length - 1:length]
    decx = jnp.exp(totx)
    small[2].wait()
    small[3].wait()
    for q in range(tiles):
        cot[:, tile(q)] = nt(eye, cott[tile(q), :]).astype(BF16)
    ec = jnp.exp(cumx) * cot[...].astype(F32)
    ecot[...] = ec
    qryt = nt(eye, qry[...]).astype(BF16)
    hi, lo = split(ec)
    pull = nn(qryt, hi) + nn(qryt, lo)
    def spread(m, whole):
        for g in range(groups):
            for yy in range(ny):
                for i in range(pack):
                    sbuf[m, g, yy, i * rw:(i + 1) * rw] = whole[yy * rw:(yy + 1) * rw, tile(g * pack + i)]

    spread(0, pull)
    for q in range(tiles):
        decb[q:q + 1, :] = decx[:, tile(q)]

    with jax.named_scope("barrier"):
        pl.semaphore_wait(barrier, ny - 1 + nz - 1 + ntp - 1)
    for dy in range(1, ny):
        dcopy(dy).start()
    for g in range(groups):
        for dy in range(1, ny):
            ycopy(0, g, dy).start()
    ydec[y] = decb[...]
    ybuf[0, :, y] = sbuf[0, :, y]

    hload.wait()
    for b in range(features // LANES):
        block = nt(eye, hid[:, tile(b)])
        for i in range(LANES // rows):
            owner = b * LANES // rows + i
            ht[owner % ny, owner // ny] = block[i * rows:(i + 1) * rows]
    with jax.named_scope("send_h"):
        for dy in range(1, ny):
            hcopy(dy).start()
    tend[...] = jnp.exp(totx - cumx)
    small[4].wait()
    values = jnp.zeros((length, columns), F32)
    for k in range(steps):
        wcopies[k].wait()
        values = values + nn(hid[:, k * depth:(k + 1) * depth], wt[k * depth:(k + 1) * depth, :])
    vals = values.astype(BF16)
    xv = tend[...] * vals.astype(F32)
    xval[...] = xv
    keyt = nt(eye, key[...]).astype(BF16)
    hi, lo = split(xv)
    push = nn(keyt, hi) + nn(keyt, lo)
    spread(1, push)
    with jax.named_scope("send_y1"):
        for g in range(groups):
            for dy in range(1, ny):
                ycopy(1, g, dy).start()
    ybuf[1, :, y] = sbuf[1, :, y]

    hcol[:, :, pl.ds(pl.multiple_of(y * length, LANES), length)] = ht[y].astype(BF16)

    def scan_order(m, count):
        return list(range(count)) if m == 1 else list(reversed(range(count)))

    def stage_y(m, g):
        if m == 0 and g == 0:
            bulk(ydec.at[:ny - 1], dsend, drecv).wait_recv()
        bulk(ybuf.at[m, g, :ny - 1], ysend, yrecv.at[m, g]).wait_recv()
        order = scan_order(m, ny)
        for i in range(pack):
            q, at = g * pack + i, slice(i * rw, (i + 1) * rw)
            run = ybuf[m, g, order[0], at]
            for yy in order[1:]:
                run = ydec[yy, q:q + 1] * run + ybuf[m, g, yy, at]
            prod = ydec[0, q:q + 1]
            for yy in range(1, ny):
                prod = prod * ydec[yy, q:q + 1]
            for k in range(rw // pr):
                tz[m, g, i * (rw // pr) + k, :pr] = run[k * pr:(k + 1) * pr]
                tz[m, g, i * (rw // pr) + k, pr:pr + 1] = prod
        for dz in sorted(range(1, nz), key=lambda dz: -min(dz, nz - dz)):
            tcopy(m, g, dz).start()
        zbuf[m, g, z] = tz[m, g, z]

    def stage_z(m, g):
        bulk(zbuf.at[m, g, :nz - 1], tsend, trecv.at[m, g]).wait_recv()
        run = jnp.zeros((pr, LANES), F32)
        for zz in scan_order(m, nz):
            cz[m, g, zz] = run
            run = zbuf[m, g, zz, pr:pr + 1] * run + zbuf[m, g, zz, :pr]
        for dz in sorted(range(1, nz), key=lambda dz: -min(dz, nz - dz)):
            ccopy(m, g, dz).start()
        zcar[m, g, z] = cz[m, g, z]

    def stage_c(m, g):
        bulk(zcar.at[m, g, :nz - 1], csend, crecv.at[m, g]).wait_recv()
        for k in range(nz):
            crow[m, g, k * pr:(k + 1) * pr] = zcar[m, g, k]
        carry = crow[m, g]
        for i in range(pack):
            q, at = g * pack + i, slice(i * rw, (i + 1) * rw)
            now = carry[at]
            for yy in scan_order(m, ny):
                ob[m, g, yy, at] = now
                now = ydec[yy, q:q + 1] * now + ybuf[m, g, yy, at]
        for dy in sorted(range(1, ny), key=lambda dy: -min(dy, ny - dy)):
            ocopy(m, g, dy).start()
        scr[m, g, y] = ob[m, g, y]

    def stage(name, work, m):
        for g in range(groups):
            with jax.named_scope(f"{name}{m}{g}"):
                work(m, g)

    def state_tile(m, q):
        g, i = q // pack, q % pack
        return scr[m, g, :, i * rw:(i + 1) * rw].reshape(state, LANES)

    stage("stage_y", stage_y, 0)

    causal = row_at <= col_at
    scores = nt(key[...], qry[...])
    for q in range(tiles):
        lefts, rights = [], []
        ct = cot[:, tile(q)]
        for i in range(per):
            h = q * per + i
            across = cumt[h:h + 1, :] - cum[:, h:h + 1]
            dm = jnp.where(causal, jnp.exp(jnp.where(causal, across, 0.0)), 0.0)
            damp[h] = dm
            lefts.extend(split(scores * dm))
            masked = jnp.where(lane == i, ct, jnp.zeros_like(ct))
            rights.extend([masked, masked])
        gvloc[q] = nn(jnp.concatenate(lefts, axis=1), jnp.concatenate(rights, axis=0))

    with jax.named_scope("hid_y"):
        bulk(hg.at[:ny - 1, :hz], hsend, hrecv).wait_recv()
        for dt in range(1, ntp):
            for dy in range(1, ny):
                share(dy, dt).start()

    stage("stage_z", stage_z, 0)

    stage("stage_y", stage_y, 1)

    dsum = jnp.zeros((length, length), F32)
    for q in range(tiles):
        vt = vals[:, tile(q)]
        both = nt(
            jnp.concatenate([jnp.where(lane == i, vt, jnp.zeros_like(vt)) for i in range(per)], axis=0),
            cot[:, tile(q)],
        )
        for i in range(per):
            h = q * per + i
            ds = both[i * length:(i + 1) * length] * damp[h]
            flux = ds * scores
            dsum = dsum + ds
            rows8[h:h + 1, :] = jnp.sum(flux, axis=0, keepdims=True)
            cols8[:, h:h + 1] = jnp.sum(flux, axis=1, keepdims=True)

    stage("stage_c", stage_c, 0)

    hi, lo = split(dsum)
    gkl[...] = nn(hi, qry[...]) + nn(lo, qry[...])
    hi, lo = split(dsum.T)
    gql[...] = nn(hi, key[...]) + nn(lo, key[...])
    stage("stage_z", stage_z, 1)

    for g in range(groups):
        with jax.named_scope(f"wait_o0{g}"):
            bulk(scr.at[0, g, :ny - 1], osend, orecv.at[0, g]).wait_recv()
        for q in range(g * pack, (g + 1) * pack):
            hi, lo = split(state_tile(0, q))
            kg = nn(key[...], hi) + nn(key[...], lo)
            kgs[:, tile(q)] = kg
            gb = (gvloc[q] + tend[:, tile(q)] * kg).astype(BF16)
            gvb[:, tile(q)] = gb
            gath[y, q] = gb.astype(F32)
            for dy in sorted(range(1, ny), key=lambda dy: -min(dy, ny - dy)):
                gcopy(q, dy).start()

    def columns_in():
        if ntp > 1:
            bulk(hg.at[:ny - 1, :nz - hz], fsend, frecv).wait_recv()
        for dy in range(1, ny):
            there = (y + dy) % ny
            hcol[:, :, pl.ds(pl.multiple_of(there * length, LANES), length)] = hg[there].astype(BF16)

    def multiply(c):
        bulk(gath.at[:ny - 1, c], gsend, grecv.at[c]).wait_recv()
        block = gath[:, c].reshape(ny * length, LANES).astype(BF16)
        part[c] = nn(hcol[...].reshape(nz * rows, ny * length), block).reshape(nz, rows, LANES)
        for d in range(2):
            if fast(c):
                for j in slots(c, d):
                    if j < 2 or (j == 2 and reach(c, d) == 3):
                        scopy(c, d, j).start()
            elif reach(c, d) > 0:
                rcopy(c, d, 0).start()

    def hop(c, d, j):
        rcopy(c, d, j).wait_recv()
        left = reach(c, d) - 1 - j
        if left > 0:
            ring[d, c, j] = ring[d, c, j] + part[c, ahead(left, d)]
            rcopy(c, d, j + 1).start()

    def step(c, d, j):
        if j == 2:
            bulk(ring.at[d, c, 2:4], rsend, rrecv.at[slot_at(c, d, 2)]).wait_recv()
        else:
            scopy(c, d, j).wait_recv()
            ring[d, c, j] = ring[d, c, j] + part[c, ahead(2 - j, d)]
            scopy(c, d, j + 2).start()

    def total_weight(c):
        total = part[c, z]
        for d in range(2):
            if fast(c):
                total = total + (ring[d, c, 2] + ring[d, c, 3])
            elif reach(c, d) > 0:
                total = total + ring[d, c, reach(c, d) - 1]
        gw_ref[:, tile(c)] = total
        outs[4 + c].start()

    def project():
        block = nt(gvb[...], wt[...])
        for t in range(ntp):
            ghp[t % halves, t // halves] = block[t * own:(t + 1) * own]
        if halves == 2:
            pair().start()

    def pairs():
        if halves == 2:
            pair().wait_recv()
            red[...] = ghp[core] + pland[...]
        else:
            red[...] = ghp[0]
        for dx in range(1, nx):
            xcopy(dx).start()

    def key_grads():
        gk = gkl[...]
        pulled = []
        for q in range(tiles):
            sgh, sgl = split(state_tile(0, q))
            xq = xval[:, tile(q)]
            xh, xl = split(xq)
            gk = gk + (nt(xh, sgh) + nt(xl, sgh) + nt(xh, sgl))
            pulled.append(xq * kgs[:, tile(q)])
        gk_ref[...] = gk.astype(BF16)
        outs[0].start()
        prefix_in = nt(seg, jnp.concatenate(pulled, axis=1), HIGH)
        gd_ref[...] = nn(prefix_in, (row_at < col_at).astype(F32), HIGH)

    def query_grads():
        with jax.named_scope("wait_o1"):
            for g in range(groups):
                bulk(scr.at[1, g, :ny - 1], osend, orecv.at[1, g]).wait_recv()
        gq = gql[...]
        into, through = [], []
        for q in range(tiles):
            si, sg = state_tile(1, q), state_tile(0, q)
            sih, sil = split(si)
            eq = ecot[:, tile(q)]
            eh, el = split(eq)
            gq = gq + (nt(eh, sih) + nt(el, sih) + nt(eh, sil))
            into.append(eq * (nn(qry[...], sih) + nn(qry[...], sil)))
            through.append(jnp.sum(si * sg, axis=0, keepdims=True))
        gq_ref[...] = gq.astype(BF16)
        outs[1].start()
        suffix_in = nt(seg, jnp.concatenate(into, axis=1), HIGH) - nt(same, cols8[...], HIGH) + rows8[...]
        crossing = nt(seg, jnp.broadcast_to(decx * jnp.concatenate(through, axis=1), (SUB, columns)), HIGH)[:, :1]
        total = nn(suffix_in, lower, HIGH) + gd_ref[...] + crossing
        gd_ref[...] = total * -rate * (1.0 / (1.0 + jnp.exp(-p)))
        outs[2].start()

    def total_hidden():
        total = red[x]
        if nx > 1:
            bulk(xland.at[:nx - 1], xsend, xrecv).wait_recv()
        for dx in range(1, nx):
            total = total + xland[(x + dx) % nx]
        gh_ref[...] = total.astype(gh_ref.dtype)
        outs[3].start()

    def drain():
        bulk(ydec.at[:ny - 1], dsend, drecv).wait_send()
        bulk(ht.at[:ny - 1, :hz], hsend, hrecv).wait_send()
        if ntp > 1:
            bulk(hg.at[:ny - 1, :nz - hz], fsend, frecv).wait_send()
        bulk(sbuf.at[:, :, :ny - 1], ysend, yrecv.at[0, 0]).wait_send()
        bulk(tz.at[:, :, :nz - 1], tsend, trecv.at[0, 0]).wait_send()
        bulk(cz.at[:, :, :nz - 1], csend, crecv.at[0, 0]).wait_send()
        bulk(ob.at[:, :, :ny - 1], osend, orecv.at[0, 0]).wait_send()
        bulk(gath.at[:ny - 1], gsend, grecv.at[0]).wait_send()
        if halves == 2:
            pair().wait_send()

    tasks = [
        (1.0, "project", project), (1.9, "columns_in", columns_in),
        (2.0, "stage_c1", functools.partial(stage, "stage_c", stage_c, 1)), (3.0, "key_grads", key_grads),
        (9.6, "pairs", pairs), (15.2, "query_grads", query_grads), (15.1, "drain", drain),
        (18.2, "total_hidden", total_hidden),
    ]
    arrive = (4.5, 6.0, 8.5, 11.0)
    for c in range(tiles):
        ready = arrive[c % 4] + 7.0 * (c // 4)
        tasks.append((ready, f"multiply{c}", functools.partial(multiply, c)))
        last = ready
        for d in range(2):
            for j in slots(c, d):
                if fast(c) and j == 3:
                    continue
                if fast(c):
                    at = ready + (4.0 if j < 2 else 8.0) + 0.2 * (j % 2)
                    tasks.append((at, f"step{c}{d}{j}", functools.partial(step, c, d, j)))
                else:
                    at = ready + 3.5 * (j + 1)
                    tasks.append((at, f"hop{c}{d}{j}", functools.partial(hop, c, d, j)))
                last = max(last, at)
        tasks.append((last + 0.01, f"total{c}", functools.partial(total_weight, c)))
    for _, name, task in sorted(tasks, key=lambda item: item[0]):
        with jax.named_scope(name):
            task()

    with jax.named_scope("drain_ring"):
        bulk(part.at[:, :nz - 1], rsend, rrecv.at[0]).wait_send()
        if nx > 1:
            bulk(red.at[:nx - 1], xsend, xrecv).wait_send()
    with jax.named_scope("outs"):
        for copy in outs[:4]:
            copy.wait()
        pltpu.make_async_copy(gw_ref, gw_out, outsem.at[4]).wait()


def finish_kernel(*refs):
    count = (len(refs) - 1) // 3
    ins, outs, held, sems = refs[:count], refs[count:2 * count], refs[2 * count:3 * count], refs[-1]
    loads = [pltpu.make_async_copy(ins[k], held[k], sems.at[0, k]) for k in range(count)]
    stores = [pltpu.make_async_copy(held[k], outs[k], sems.at[1, k]) for k in range(count)]
    for load in loads:
        load.start()
    for load, store in zip(loads, stores):
        load.wait()
        store.start()
    for store in stores:
        store.wait()


HBM = pl.BlockSpec(memory_space=pltpu.HBM)
LIMIT = 60 * 1024 * 1024


def per_device(sp, tp, hidden, value_weight, key_vecs, queries, decay_pre, decay_rate, cotangent):
    length, features = hidden.shape
    heads = decay_rate.shape[0]
    state = key_vecs.shape[2]
    columns = value_weight.shape[1]
    ny = inner_size(sp)
    nz = sp // ny
    tiles = columns // LANES
    groups = tiles
    pack = tiles // groups
    rw = state // ny
    pr = pack * rw // nz
    rows = features // sp
    own = length // tp
    halves = 2 if tp % 2 == 0 else 1
    nx = tp // halves
    far = nz // 2
    steps = 2
    vm = pltpu.VMEM
    dma = pltpu.SemaphoreType.DMA
    outs = pl.pallas_call(
        functools.partial(mixer_kernel, ny, nz, tp),
        out_shape=(
            jax.ShapeDtypeStruct((length, state), BF16),
            jax.ShapeDtypeStruct((length, state), BF16),
            jax.ShapeDtypeStruct((heads, length), F32),
            jax.ShapeDtypeStruct((own, features), BF16),
            jax.ShapeDtypeStruct((rows, columns), F32),
        ),
        in_specs=[HBM] * 7,
        out_specs=(HBM,) * 5,
        scratch_shapes=[
            vm((length, state), BF16),
            vm((length, state), BF16),
            vm((heads, length), F32),
            vm((own, features), BF16),
            vm((rows, columns), F32),
            vm((length, features), BF16),
            vm((features, columns), BF16),
            vm((length, state), BF16),
            vm((length, state), BF16),
            vm((heads, length), F32),
            vm((1, heads), F32),
            vm((columns, length), BF16),
            vm((length, columns), BF16),
            vm((length, columns), F32),
            vm((length, columns), F32),
            vm((length, columns), F32),
            vm((heads, length, length), F32),
            vm((tiles, length, LANES), F32),
            vm((length, columns), BF16),
            vm((length, columns), F32),
            vm((heads, length), F32),
            vm((length, heads), F32),
            vm((length, state), F32),
            vm((length, state), F32),
            vm((2, groups, ny, pack * rw, LANES), F32),
            vm((SUB, LANES), F32),
            vm((2, groups, ny, pack * rw, LANES), F32),
            vm((ny, SUB, LANES), F32),
            vm((2, groups, nz, -(-(pr + 1) // SUB) * SUB, LANES), F32),
            vm((2, groups, nz, -(-(pr + 1) // SUB) * SUB, LANES), F32),
            vm((2, groups, nz, pr, LANES), F32),
            vm((2, groups, nz, pr, LANES), F32),
            vm((2, groups, pack * rw, LANES), F32),
            vm((2, groups, ny, pack * rw, LANES), F32),
            vm((2, groups, ny, pack * rw, LANES), F32),
            vm((ny, nz, rows, length), F32),
            vm((ny, nz, rows, length), F32),
            vm((nz, rows, ny * length), BF16),
            vm((ny, tiles, length, LANES), F32),
            vm((tiles, nz, rows, LANES), F32),
            vm((2, tiles, far, rows, LANES), F32),
            vm((halves, nx, own, features), F32),
            vm((nx, own, features), F32),
            vm((nx, own, features), F32),
            vm((nx, own, features), F32),
            dma((6,)), dma((steps,)),
            dma, dma,
            dma, dma((2, groups)),
            dma, dma((2, groups)),
            dma, dma((2, groups)),
            dma, dma((2, groups)),
            dma, dma,
            dma, dma,
            dma, dma((tiles,)),
            dma, dma((tiles * (nz - 1) - (2 * 2 if nz == 8 else 0),)),
            dma, dma,
            dma, dma,
            dma((5,)),
        ],
        compiler_params=pltpu.CompilerParams(collective_id=0, has_side_effects=True, vmem_limit_bytes=LIMIT),
        name="mixer_backward",
    )(
        hidden, value_weight, key_vecs.reshape(length, state), queries.reshape(length, state), decay_pre.T,
        decay_rate.reshape(1, heads), cotangent.reshape(length, columns).T,
    )
    gk, gq, gd, gh, gw = pl.pallas_call(
        finish_kernel,
        out_shape=tuple(jax.ShapeDtypeStruct(o.shape, o.dtype) for o in outs),
        in_specs=[HBM] * 5,
        out_specs=(HBM,) * 5,
        scratch_shapes=[vm(o.shape, o.dtype) for o in outs] + [dma((2, 5))],
        compiler_params=pltpu.CompilerParams(vmem_limit_bytes=LIMIT),
        name="write_out",
    )(*outs)
    return gk.reshape(key_vecs.shape), gq.reshape(key_vecs.shape), gd.T, gh, gw


def solution(mesh):
    return jax.shard_map(
        functools.partial(per_device, mesh.shape["sp"], mesh.shape["tp"]),
        mesh=mesh,
        in_specs=(
            P("sp", None),
            P(None, "tp"),
            P("sp", "tp", None),
            P("sp", "tp", None),
            P("sp", "tp"),
            P("tp"),
            P("sp", "tp", None),
        ),
        out_specs=(
            P("sp", "tp", None),
            P("sp", "tp", None),
            P("sp", "tp"),
            P(("sp", "tp"), None),
            P("sp", "tp"),
        ),
        check_vma=False,
    )
```

```python
import functools

import jax
import jax.numpy as jnp
from jax import lax
from jax.experimental import pallas as pl
from jax.experimental.pallas import tpu as pltpu
from jax.sharding import PartitionSpec as P

MESH = pl.DeviceIdType.MESH
F32 = jnp.float32
BF16 = jnp.bfloat16
HIGH = lax.Precision.HIGHEST
LANES = 128
SUB = 8


def inner_size(count):
    size = 1
    while size * size * 4 <= count:
        size *= 2
    while count % size:
        size -= 1
    return size


def remote(src, dst, send, recv, axis, index):
    return pltpu.make_async_remote_copy(
        src_ref=src, dst_ref=dst, send_sem=send, recv_sem=recv, device_id={axis: index}, device_id_type=MESH
    )


def nn(a, b, precision=None):
    return jnp.dot(a, b, preferred_element_type=F32, precision=precision)


def nt(a, b, precision=None):
    return lax.dot_general(a, b, (((1,), (1,)), ((), ())), preferred_element_type=F32, precision=precision)


def split(x):
    hi = x.astype(BF16)
    return hi, (x - hi.astype(F32)).astype(BF16)


def mixer_kernel(ny, nz, ntp, hid_hbm, w_hbm, key_hbm, qry_hbm, pre_hbm, rate_hbm, cot_hbm,
                 gk_out, gq_out, gd_out, gh_out, gw_out,
                 gk_ref, gq_ref, gd_ref, gh_ref, gw_ref, hid, wt, key, qry, pre, rate_ref, cott, cot,
                 ecot, tend, xval, damp, gvloc, gvb, kgs, rows8, cols8, gkl, gql,
                 sbuf, decb, ybuf, ydec, tz, zbuf, cz, zcar, crow, ob, scr, ht, hg, hcol,
                 gath, part, ring, ghp, pland, red, xland,
                 insem, wsem, dsend, drecv, ysend, yrecv, tsend, trecv, csend, crecv, osend, orecv,
                 hsend, hrecv, fsend, frecv, gsend, grecv, rsend, rrecv, psend, precv, xsend, xrecv, outsem):
    me = lax.axis_index("sp")
    mine = lax.axis_index("tp")
    z, y = me // ny, me % ny
    length, features = hid.shape
    heads = pre.shape[0]
    columns = cot.shape[1]
    width = columns // heads
    tiles = columns // LANES
    per = LANES // width
    state = key.shape[1]
    groups = sbuf.shape[1]
    pack = tiles // groups
    rw = state // ny
    pr = pack * rw // nz
    rows = gw_ref.shape[0]
    own = gh_ref.shape[0]
    halves = 2 if ntp % 2 == 0 else 1
    core, x, nx = mine % halves, mine // halves, ntp // halves
    partner = mine + 1 - 2 * core
    hz = nz // ntp
    steps = wsem.shape[0]
    depth = features // steps
    ydev = [z * ny + (y + dy) % ny for dy in range(ny)]
    zdev = [((z + dz) % nz) * ny + y for dz in range(nz)]

    barrier = pltpu.get_barrier_semaphore()
    for dev in [zdev[dz] for dz in sorted(range(1, nz), key=lambda dz: -min(dz, nz - dz))] + ydev[1:]:
        pl.semaphore_signal(barrier, inc=1, device_id={"sp": dev}, device_id_type=MESH)
    for dt in range(1, ntp):
        pl.semaphore_signal(barrier, inc=1, device_id={"tp": (mine + dt) % ntp}, device_id_type=MESH)

    small = [
        pltpu.make_async_copy(pre_hbm, pre, insem.at[0]),
        pltpu.make_async_copy(rate_hbm, rate_ref, insem.at[4]),
        pltpu.make_async_copy(qry_hbm, qry, insem.at[1]),
        pltpu.make_async_copy(cot_hbm, cott, insem.at[2]),
        pltpu.make_async_copy(key_hbm, key, insem.at[3]),
    ]
    for copy in small:
        copy.start()
    wcopies = []
    for k in range(steps):
        at = pl.ds(k * depth, depth)
        wcopies.append(pltpu.make_async_copy(w_hbm.at[at, :], wt.at[at, :], wsem.at[k]))
    hload = pltpu.make_async_copy(hid_hbm, hid, insem.at[5])
    hload.start()
    for copy in wcopies:
        copy.start()

    outs = [
        pltpu.make_async_copy(gk_ref, gk_out, outsem.at[0]),
        pltpu.make_async_copy(gq_ref, gq_out, outsem.at[1]),
        pltpu.make_async_copy(gd_ref, gd_out, outsem.at[2]),
        pltpu.make_async_copy(gh_ref, gh_out, outsem.at[3]),
    ]
    for c in range(tiles):
        at = pl.ds(c * LANES, LANES)
        outs.append(pltpu.make_async_copy(gw_ref.at[:, at], gw_out.at[:, at], outsem.at[4]))

    def dcopy(dy, arrive=False):
        slot = (y + dy) % ny if arrive else y
        return remote(decb, ydec.at[slot], dsend, drecv, "sp", ydev[dy])

    def ycopy(m, g, dy):
        there = (y + dy) % ny
        return remote(sbuf.at[m, g, there], ybuf.at[m, g, y], ysend, yrecv.at[m, g], "sp", ydev[dy])

    def tcopy(m, g, dz):
        there = (z + dz) % nz
        return remote(tz.at[m, g, there], zbuf.at[m, g, z], tsend, trecv.at[m, g], "sp", zdev[dz])

    def ccopy(m, g, dz):
        there = (z + dz) % nz
        return remote(cz.at[m, g, there], zcar.at[m, g, z], csend, crecv.at[m, g], "sp", zdev[dz])

    def ocopy(m, g, dy):
        there = (y + dy) % ny
        return remote(ob.at[m, g, there], scr.at[m, g, y], osend, orecv.at[m, g], "sp", ydev[dy])

    def section(k):
        return pl.ds(pl.multiple_of(k * hz, hz), hz)

    def hcopy(dy, arrive=False):
        there = (y + dy) % ny
        slot = there if arrive else y
        return remote(
            ht.at[there, section(mine)], hg.at[slot, section(mine)], hsend, hrecv, "sp", ydev[dy]
        )

    def share(dy, dt, arrive=False):
        there = (y + dy) % ny
        peer = (mine + dt) % ntp
        which = peer if arrive else mine
        block = hg.at[there, section(which)]
        return remote(block, block, fsend, frecv, "tp", peer)

    def gcopy(c, dy, arrive=False):
        there = (y + dy) % ny
        slot = there if arrive else y
        return remote(gath.at[slot, c], gath.at[slot, c], gsend, grecv.at[c], "sp", ydev[dy])

    def pair():
        return remote(ghp.at[1 - core], pland, psend, precv, "tp", partner)

    def xcopy(dx, arrive=False):
        there = (x + dx) % nx
        slot = there if arrive else x
        return remote(red.at[there], xland.at[slot], xsend, xrecv, "tp", there * halves + core)

    def reach(c, d):
        far = nz // 2
        return far if (c + d) % 2 == 0 else nz - 1 - far

    def fast(c):
        return nz == 8 and c >= tiles - 2

    def ahead(k, d):
        return (z + k) % nz if d == 0 else (z + nz - k) % nz

    def rcopy(c, d, j):
        src = part.at[c, ahead(reach(c, d), d)] if j == 0 else ring.at[d, c, j - 1]
        return remote(
            src, ring.at[d, c, j], rsend, rrecv.at[slot_at(c, d, j)], "sp", zdev[1] if d == 0 else zdev[nz - 1]
        )

    def scopy(c, d, j):
        src, hops = (part.at[c, ahead(j + 2, d)], j + 1) if j < 3 else (ring.at[d, c, 0], 1)
        return remote(
            src, ring.at[d, c, j], rsend, rrecv.at[slot_at(c, d, j)], "sp", zdev[hops if d == 0 else nz - hops]
        )

    def slots(c, d):
        if fast(c):
            return tuple(range(reach(c, d) - 1)) + (3,)
        return tuple(range(reach(c, d)))

    def step_of(c, j):
        return j // 3 if fast(c) else j

    ring_slots = sorted({(c, d, step_of(c, j)) for c in range(tiles) for d in range(2) for j in slots(c, d)})

    def slot_at(c, d, j):
        return ring_slots.index((c, d, step_of(c, j)))

    def bulk(ref, send, recv):
        return remote(ref, ref, send, recv, "sp", ydev[1])

    row_at = lax.broadcasted_iota(jnp.int32, (length, length), 0)
    col_at = lax.broadcasted_iota(jnp.int32, (length, length), 1)
    eye = (row_at == col_at).astype(BF16)
    seg = (
        lax.broadcasted_iota(jnp.int32, (heads, columns), 1) // width
        == lax.broadcasted_iota(jnp.int32, (heads, columns), 0)
    ).astype(F32)
    lane = lax.broadcasted_iota(jnp.int32, (length, LANES), 1) // width

    def tile(q):
        return slice(q * LANES, (q + 1) * LANES)

    same = (
        lax.broadcasted_iota(jnp.int32, (heads, heads), 0) == lax.broadcasted_iota(jnp.int32, (heads, heads), 1)
    ).astype(F32)
    small[0].wait()
    small[1].wait()
    p = pre[...]
    rate = nt(same, jnp.broadcast_to(rate_ref[...], (heads, heads)), HIGH)[:, :1]
    log_decay = -rate * (jnp.maximum(p, 0.0) + jnp.log1p(jnp.exp(-jnp.abs(p))))
    lower = (row_at >= col_at).astype(F32)
    cum = nt(lower, log_decay, HIGH)
    cumt = nt(log_decay, lower, HIGH)
    cumx = nn(cum, seg, HIGH)
    totx = cumx[length - 1:length]
    decx = jnp.exp(totx)
    small[2].wait()
    small[3].wait()
    for q in range(tiles):
        cot[:, tile(q)] = nt(eye, cott[tile(q), :]).astype(BF16)
    ec = jnp.exp(cumx) * cot[...].astype(F32)
    ecot[...] = ec
    qryt = nt(eye, qry[...]).astype(BF16)
    hi, lo = split(ec)
    pull = nn(qryt, hi) + nn(qryt, lo)
    def spread(m, whole):
        for g in range(groups):
            for yy in range(ny):
                for i in range(pack):
                    sbuf[m, g, yy, i * rw:(i + 1) * rw] = whole[yy * rw:(yy + 1) * rw, tile(g * pack + i)]

    spread(0, pull)
    for q in range(tiles):
        decb[q:q + 1, :] = decx[:, tile(q)]

    with jax.named_scope("barrier"):
        pl.semaphore_wait(barrier, ny - 1 + nz - 1 + ntp - 1)
    for dy in range(1, ny):
        dcopy(dy).start()
    for g in range(groups):
        for dy in range(1, ny):
            ycopy(0, g, dy).start()
    ydec[y] = decb[...]
    ybuf[0, :, y] = sbuf[0, :, y]

    hload.wait()
    for b in range(features // LANES):
        block = nt(eye, hid[:, tile(b)])
        for i in range(LANES // rows):
            owner = b * LANES // rows + i
            ht[owner % ny, owner // ny] = block[i * rows:(i + 1) * rows]
    with jax.named_scope("send_h"):
        for dy in range(1, ny):
            hcopy(dy).start()
    tend[...] = jnp.exp(totx - cumx)
    small[4].wait()
    values = jnp.zeros((length, columns), F32)
    for k in range(steps):
        wcopies[k].wait()
        values = values + nn(hid[:, k * depth:(k + 1) * depth], wt[k * depth:(k + 1) * depth, :])
    vals = values.astype(BF16)
    xv = tend[...] * vals.astype(F32)
    xval[...] = xv
    keyt = nt(eye, key[...]).astype(BF16)
    hi, lo = split(xv)
    push = nn(keyt, hi) + nn(keyt, lo)
    spread(1, push)
    with jax.named_scope("send_y1"):
        for g in range(groups):
            for dy in range(1, ny):
                ycopy(1, g, dy).start()
    ybuf[1, :, y] = sbuf[1, :, y]

    hcol[:, :, pl.ds(pl.multiple_of(y * length, LANES), length)] = ht[y].astype(BF16)

    def scan_order(m, count):
        return list(range(count)) if m == 1 else list(reversed(range(count)))

    def stage_y(m, g):
        if m == 0 and g == 0:
            bulk(ydec.at[:ny - 1], dsend, drecv).wait_recv()
        bulk(ybuf.at[m, g, :ny - 1], ysend, yrecv.at[m, g]).wait_recv()
        order = scan_order(m, ny)
        for i in range(pack):
            q, at = g * pack + i, slice(i * rw, (i + 1) * rw)
            run = ybuf[m, g, order[0], at]
            for yy in order[1:]:
                run = ydec[yy, q:q + 1] * run + ybuf[m, g, yy, at]
            prod = ydec[0, q:q + 1]
            for yy in range(1, ny):
                prod = prod * ydec[yy, q:q + 1]
            for k in range(rw // pr):
                tz[m, g, i * (rw // pr) + k, :pr] = run[k * pr:(k + 1) * pr]
                tz[m, g, i * (rw // pr) + k, pr:pr + 1] = prod
        for dz in sorted(range(1, nz), key=lambda dz: -min(dz, nz - dz)):
            tcopy(m, g, dz).start()
        zbuf[m, g, z] = tz[m, g, z]

    def stage_z(m, g):
        bulk(zbuf.at[m, g, :nz - 1], tsend, trecv.at[m, g]).wait_recv()
        run = jnp.zeros((pr, LANES), F32)
        for zz in scan_order(m, nz):
            cz[m, g, zz] = run
            run = zbuf[m, g, zz, pr:pr + 1] * run + zbuf[m, g, zz, :pr]
        for dz in sorted(range(1, nz), key=lambda dz: -min(dz, nz - dz)):
            ccopy(m, g, dz).start()
        zcar[m, g, z] = cz[m, g, z]

    def stage_c(m, g):
        bulk(zcar.at[m, g, :nz - 1], csend, crecv.at[m, g]).wait_recv()
        for k in range(nz):
            crow[m, g, k * pr:(k + 1) * pr] = zcar[m, g, k]
        carry = crow[m, g]
        for i in range(pack):
            q, at = g * pack + i, slice(i * rw, (i + 1) * rw)
            now = carry[at]
            for yy in scan_order(m, ny):
                ob[m, g, yy, at] = now
                now = ydec[yy, q:q + 1] * now + ybuf[m, g, yy, at]
        for dy in sorted(range(1, ny), key=lambda dy: -min(dy, ny - dy)):
            ocopy(m, g, dy).start()
        scr[m, g, y] = ob[m, g, y]

    def stage(name, work, m):
        for g in range(groups):
            with jax.named_scope(f"{name}{m}{g}"):
                work(m, g)

    def state_tile(m, q):
        g, i = q // pack, q % pack
        return scr[m, g, :, i * rw:(i + 1) * rw].reshape(state, LANES)

    stage("stage_y", stage_y, 0)

    causal = row_at <= col_at
    scores = nt(key[...], qry[...])
    for q in range(tiles):
        lefts, rights = [], []
        ct = cot[:, tile(q)]
        for i in range(per):
            h = q * per + i
            across = cumt[h:h + 1, :] - cum[:, h:h + 1]
            dm = jnp.where(causal, jnp.exp(jnp.where(causal, across, 0.0)), 0.0)
            damp[h] = dm
            lefts.extend(split(scores * dm))
            masked = jnp.where(lane == i, ct, jnp.zeros_like(ct))
            rights.extend([masked, masked])
        gvloc[q] = nn(jnp.concatenate(lefts, axis=1), jnp.concatenate(rights, axis=0))

    with jax.named_scope("hid_y"):
        bulk(hg.at[:ny - 1, :hz], hsend, hrecv).wait_recv()
        for dt in range(1, ntp):
            for dy in range(1, ny):
                share(dy, dt).start()

    stage("stage_z", stage_z, 0)

    stage("stage_y", stage_y, 1)

    dsum = jnp.zeros((length, length), F32)
    for q in range(tiles):
        vt = vals[:, tile(q)]
        both = nt(
            jnp.concatenate([jnp.where(lane == i, vt, jnp.zeros_like(vt)) for i in range(per)], axis=0),
            cot[:, tile(q)],
        )
        for i in range(per):
            h = q * per + i
            ds = both[i * length:(i + 1) * length] * damp[h]
            flux = ds * scores
            dsum = dsum + ds
            rows8[h:h + 1, :] = jnp.sum(flux, axis=0, keepdims=True)
            cols8[:, h:h + 1] = jnp.sum(flux, axis=1, keepdims=True)

    stage("stage_c", stage_c, 0)

    hi, lo = split(dsum)
    gkl[...] = nn(hi, qry[...]) + nn(lo, qry[...])
    hi, lo = split(dsum.T)
    gql[...] = nn(hi, key[...]) + nn(lo, key[...])
    stage("stage_z", stage_z, 1)

    for g in range(groups):
        with jax.named_scope(f"wait_o0{g}"):
            bulk(scr.at[0, g, :ny - 1], osend, orecv.at[0, g]).wait_recv()
        for q in range(g * pack, (g + 1) * pack):
            hi, lo = split(state_tile(0, q))
            kg = nn(key[...], hi) + nn(key[...], lo)
            kgs[:, tile(q)] = kg
            gb = (gvloc[q] + tend[:, tile(q)] * kg).astype(BF16)
            gvb[:, tile(q)] = gb
            gath[y, q] = gb.astype(F32)
            for dy in sorted(range(1, ny), key=lambda dy: -min(dy, ny - dy)):
                gcopy(q, dy).start()

    def columns_in():
        if ntp > 1:
            bulk(hg.at[:ny - 1, :nz - hz], fsend, frecv).wait_recv()
        for dy in range(1, ny):
            there = (y + dy) % ny
            hcol[:, :, pl.ds(pl.multiple_of(there * length, LANES), length)] = hg[there].astype(BF16)

    def multiply(c):
        bulk(gath.at[:ny - 1, c], gsend, grecv.at[c]).wait_recv()
        block = gath[:, c].reshape(ny * length, LANES).astype(BF16)
        part[c] = nn(hcol[...].reshape(nz * rows, ny * length), block).reshape(nz, rows, LANES)
        for d in range(2):
            if fast(c):
                for j in reversed(range(reach(c, d) - 1)):
                    scopy(c, d, j).start()
            elif reach(c, d) > 0:
                rcopy(c, d, 0).start()

    def hop(c, d, j):
        rcopy(c, d, j).wait_recv()
        left = reach(c, d) - 1 - j
        if left > 0:
            ring[d, c, j] = ring[d, c, j] + part[c, ahead(left, d)]
            rcopy(c, d, j + 1).start()

    def step(c, d, j):
        if j == 3:
            scopy(c, d, 3).wait_recv()
        else:
            count = reach(c, d) - 1
            bulk(ring.at[d, c, :count], rsend, rrecv.at[slot_at(c, d, 0)]).wait_recv()
            total = part[c, ahead(1, d)]
            for k in range(count):
                total = total + ring[d, c, k]
            ring[d, c, 0] = total
            scopy(c, d, 3).start()

    def total_weight(c):
        total = part[c, z]
        for d in range(2):
            if fast(c):
                total = total + ring[d, c, 3]
            elif reach(c, d) > 0:
                total = total + ring[d, c, reach(c, d) - 1]
        gw_ref[:, tile(c)] = total
        outs[4 + c].start()

    def project():
        block = nt(gvb[...], wt[...])
        for t in range(ntp):
            ghp[t % halves, t // halves] = block[t * own:(t + 1) * own]
        if halves == 2:
            pair().start()

    def pairs():
        if halves == 2:
            pair().wait_recv()
            red[...] = ghp[core] + pland[...]
        else:
            red[...] = ghp[0]
        for dx in range(1, nx):
            xcopy(dx).start()

    def key_grads():
        gk = gkl[...]
        pulled = []
        for q in range(tiles):
            sgh, sgl = split(state_tile(0, q))
            xq = xval[:, tile(q)]
            xh, xl = split(xq)
            gk = gk + (nt(xh, sgh) + nt(xl, sgh) + nt(xh, sgl))
            pulled.append(xq * kgs[:, tile(q)])
        gk_ref[...] = gk.astype(BF16)
        outs[0].start()
        prefix_in = nt(seg, jnp.concatenate(pulled, axis=1), HIGH)
        gd_ref[...] = nn(prefix_in, (row_at < col_at).astype(F32), HIGH)

    def query_grads():
        with jax.named_scope("wait_o1"):
            for g in range(groups):
                bulk(scr.at[1, g, :ny - 1], osend, orecv.at[1, g]).wait_recv()
        gq = gql[...]
        into, through = [], []
        for q in range(tiles):
            si, sg = state_tile(1, q), state_tile(0, q)
            sih, sil = split(si)
            eq = ecot[:, tile(q)]
            eh, el = split(eq)
            gq = gq + (nt(eh, sih) + nt(el, sih) + nt(eh, sil))
            into.append(eq * (nn(qry[...], sih) + nn(qry[...], sil)))
            through.append(jnp.sum(si * sg, axis=0, keepdims=True))
        gq_ref[...] = gq.astype(BF16)
        outs[1].start()
        suffix_in = nt(seg, jnp.concatenate(into, axis=1), HIGH) - nt(same, cols8[...], HIGH) + rows8[...]
        crossing = nt(seg, jnp.broadcast_to(decx * jnp.concatenate(through, axis=1), (SUB, columns)), HIGH)[:, :1]
        total = nn(suffix_in, lower, HIGH) + gd_ref[...] + crossing
        gd_ref[...] = total * -rate * (1.0 / (1.0 + jnp.exp(-p)))
        outs[2].start()

    def total_hidden():
        total = red[x]
        if nx > 1:
            bulk(xland.at[:nx - 1], xsend, xrecv).wait_recv()
        for dx in range(1, nx):
            total = total + xland[(x + dx) % nx]
        gh_ref[...] = total.astype(gh_ref.dtype)
        outs[3].start()

    def drain():
        bulk(ydec.at[:ny - 1], dsend, drecv).wait_send()
        bulk(ht.at[:ny - 1, :hz], hsend, hrecv).wait_send()
        if ntp > 1:
            bulk(hg.at[:ny - 1, :nz - hz], fsend, frecv).wait_send()
        bulk(sbuf.at[:, :, :ny - 1], ysend, yrecv.at[0, 0]).wait_send()
        bulk(tz.at[:, :, :nz - 1], tsend, trecv.at[0, 0]).wait_send()
        bulk(cz.at[:, :, :nz - 1], csend, crecv.at[0, 0]).wait_send()
        bulk(ob.at[:, :, :ny - 1], osend, orecv.at[0, 0]).wait_send()
        bulk(gath.at[:ny - 1], gsend, grecv.at[0]).wait_send()
        if halves == 2:
            pair().wait_send()

    tasks = [
        (1.0, "project", project), (1.9, "columns_in", columns_in),
        (6.1, "stage_c1", functools.partial(stage, "stage_c", stage_c, 1)), (3.0, "key_grads", key_grads),
        (9.6, "pairs", pairs), (17.9, "query_grads", query_grads), (18.0, "drain", drain),
        (18.2, "total_hidden", total_hidden),
    ]
    arrive = (4.5, 6.0, 8.5, 11.0)
    for c in range(tiles):
        ready = arrive[c % 4] + 7.0 * (c // 4)
        tasks.append((ready, f"multiply{c}", functools.partial(multiply, c)))
        last = ready
        for d in range(2):
            for j in slots(c, d):
                if fast(c) and j not in (0, 3):
                    continue
                if fast(c):
                    at = ready + (4.0 if j < 3 else 8.0) + 0.1 * d
                    tasks.append((at, f"step{c}{d}{j}", functools.partial(step, c, d, j)))
                else:
                    at = ready + 3.5 * (j + 1)
                    tasks.append((at, f"hop{c}{d}{j}", functools.partial(hop, c, d, j)))
                last = max(last, at)
        tasks.append((last + 0.01, f"total{c}", functools.partial(total_weight, c)))
    for _, name, task in sorted(tasks, key=lambda item: item[0]):
        with jax.named_scope(name):
            task()

    with jax.named_scope("drain_ring"):
        bulk(part.at[:, :nz - 1], rsend, rrecv.at[0]).wait_send()
        if nx > 1:
            bulk(red.at[:nx - 1], xsend, xrecv).wait_send()
    with jax.named_scope("outs"):
        for copy in outs[:4]:
            copy.wait()
        pltpu.make_async_copy(gw_ref, gw_out, outsem.at[4]).wait()


def finish_kernel(*refs):
    count = (len(refs) - 1) // 3
    ins, outs, held, sems = refs[:count], refs[count:2 * count], refs[2 * count:3 * count], refs[-1]
    loads = [pltpu.make_async_copy(ins[k], held[k], sems.at[0, k]) for k in range(count)]
    stores = [pltpu.make_async_copy(held[k], outs[k], sems.at[1, k]) for k in range(count)]
    for load in loads:
        load.start()
    for load, store in zip(loads, stores):
        load.wait()
        store.start()
    for store in stores:
        store.wait()


HBM = pl.BlockSpec(memory_space=pltpu.HBM)
LIMIT = 60 * 1024 * 1024


def per_device(sp, tp, hidden, value_weight, key_vecs, queries, decay_pre, decay_rate, cotangent):
    length, features = hidden.shape
    heads = decay_rate.shape[0]
    state = key_vecs.shape[2]
    columns = value_weight.shape[1]
    ny = inner_size(sp)
    nz = sp // ny
    tiles = columns // LANES
    groups = tiles
    pack = tiles // groups
    rw = state // ny
    pr = pack * rw // nz
    rows = features // sp
    own = length // tp
    halves = 2 if tp % 2 == 0 else 1
    nx = tp // halves
    far = nz // 2
    steps = 2
    vm = pltpu.VMEM
    dma = pltpu.SemaphoreType.DMA
    outs = pl.pallas_call(
        functools.partial(mixer_kernel, ny, nz, tp),
        out_shape=(
            jax.ShapeDtypeStruct((length, state), BF16),
            jax.ShapeDtypeStruct((length, state), BF16),
            jax.ShapeDtypeStruct((heads, length), F32),
            jax.ShapeDtypeStruct((own, features), BF16),
            jax.ShapeDtypeStruct((rows, columns), F32),
        ),
        in_specs=[HBM] * 7,
        out_specs=(HBM,) * 5,
        scratch_shapes=[
            vm((length, state), BF16),
            vm((length, state), BF16),
            vm((heads, length), F32),
            vm((own, features), BF16),
            vm((rows, columns), F32),
            vm((length, features), BF16),
            vm((features, columns), BF16),
            vm((length, state), BF16),
            vm((length, state), BF16),
            vm((heads, length), F32),
            vm((1, heads), F32),
            vm((columns, length), BF16),
            vm((length, columns), BF16),
            vm((length, columns), F32),
            vm((length, columns), F32),
            vm((length, columns), F32),
            vm((heads, length, length), F32),
            vm((tiles, length, LANES), F32),
            vm((length, columns), BF16),
            vm((length, columns), F32),
            vm((heads, length), F32),
            vm((length, heads), F32),
            vm((length, state), F32),
            vm((length, state), F32),
            vm((2, groups, ny, pack * rw, LANES), F32),
            vm((SUB, LANES), F32),
            vm((2, groups, ny, pack * rw, LANES), F32),
            vm((ny, SUB, LANES), F32),
            vm((2, groups, nz, -(-(pr + 1) // SUB) * SUB, LANES), F32),
            vm((2, groups, nz, -(-(pr + 1) // SUB) * SUB, LANES), F32),
            vm((2, groups, nz, pr, LANES), F32),
            vm((2, groups, nz, pr, LANES), F32),
            vm((2, groups, pack * rw, LANES), F32),
            vm((2, groups, ny, pack * rw, LANES), F32),
            vm((2, groups, ny, pack * rw, LANES), F32),
            vm((ny, nz, rows, length), F32),
            vm((ny, nz, rows, length), F32),
            vm((nz, rows, ny * length), BF16),
            vm((ny, tiles, length, LANES), F32),
            vm((tiles, nz, rows, LANES), F32),
            vm((2, tiles, far, rows, LANES), F32),
            vm((halves, nx, own, features), F32),
            vm((nx, own, features), F32),
            vm((nx, own, features), F32),
            vm((nx, own, features), F32),
            dma((6,)), dma((steps,)),
            dma, dma,
            dma, dma((2, groups)),
            dma, dma((2, groups)),
            dma, dma((2, groups)),
            dma, dma((2, groups)),
            dma, dma,
            dma, dma,
            dma, dma((tiles,)),
            dma, dma((tiles * (nz - 1) - (3 * 2 if nz == 8 else 0),)),
            dma, dma,
            dma, dma,
            dma((5,)),
        ],
        compiler_params=pltpu.CompilerParams(collective_id=0, has_side_effects=True, vmem_limit_bytes=LIMIT),
        name="mixer_backward",
    )(
        hidden, value_weight, key_vecs.reshape(length, state), queries.reshape(length, state), decay_pre.T,
        decay_rate.reshape(1, heads), cotangent.reshape(length, columns).T,
    )
    gk, gq, gd, gh, gw = pl.pallas_call(
        finish_kernel,
        out_shape=tuple(jax.ShapeDtypeStruct(o.shape, o.dtype) for o in outs),
        in_specs=[HBM] * 5,
        out_specs=(HBM,) * 5,
        scratch_shapes=[vm(o.shape, o.dtype) for o in outs] + [dma((2, 5))],
        compiler_params=pltpu.CompilerParams(vmem_limit_bytes=LIMIT),
        name="write_out",
    )(*outs)
    return gk.reshape(key_vecs.shape), gq.reshape(key_vecs.shape), gd.T, gh, gw


def solution(mesh):
    return jax.shard_map(
        functools.partial(per_device, mesh.shape["sp"], mesh.shape["tp"]),
        mesh=mesh,
        in_specs=(
            P("sp", None),
            P(None, "tp"),
            P("sp", "tp", None),
            P("sp", "tp", None),
            P("sp", "tp"),
            P("tp"),
            P("sp", "tp", None),
        ),
        out_specs=(
            P("sp", "tp", None),
            P("sp", "tp", None),
            P("sp", "tp"),
            P(("sp", "tp"), None),
            P("sp", "tp"),
        ),
        check_vma=False,
    )
```

```python
import functools

import jax
import jax.numpy as jnp
from jax import lax
from jax.experimental import pallas as pl
from jax.experimental.pallas import tpu as pltpu
from jax.sharding import PartitionSpec as P

MESH = pl.DeviceIdType.MESH
F32 = jnp.float32
BF16 = jnp.bfloat16
HIGH = lax.Precision.HIGHEST
LANES = 128
SUB = 8


def inner_size(count):
    size = 1
    while size * size * 4 <= count:
        size *= 2
    while count % size:
        size -= 1
    return size


def remote(src, dst, send, recv, axis, index):
    return pltpu.make_async_remote_copy(
        src_ref=src, dst_ref=dst, send_sem=send, recv_sem=recv, device_id={axis: index}, device_id_type=MESH
    )


def nn(a, b, precision=None):
    return jnp.dot(a, b, preferred_element_type=F32, precision=precision)


def nt(a, b, precision=None):
    return lax.dot_general(a, b, (((1,), (1,)), ((), ())), preferred_element_type=F32, precision=precision)


def split(x):
    hi = x.astype(BF16)
    return hi, (x - hi.astype(F32)).astype(BF16)


def mixer_kernel(ny, nz, ntp, hid_hbm, w_hbm, key_hbm, qry_hbm, pre_hbm, rate_hbm, cot_hbm,
                 gk_out, gq_out, gd_out, gh_out, gw_out,
                 gk_ref, gq_ref, gd_ref, gh_ref, gw_ref, hid, wt, key, qry, pre, rate_ref, cott, cot,
                 ecot, tend, xval, damp, gvloc, gvb, kgs, rows8, cols8, gkl, gql,
                 sbuf, decb, ybuf, ydec, tz, zbuf, cz, zcar, crow, ob, scr, ht, hg, hcol,
                 gath, part, ring, ghp, pland, red, xland,
                 insem, wsem, dsend, drecv, ysend, yrecv, tsend, trecv, csend, crecv, osend, orecv,
                 hsend, hrecv, fsend, frecv, gsend, grecv, rsend, rrecv, psend, precv, xsend, xrecv, outsem):
    me = lax.axis_index("sp")
    mine = lax.axis_index("tp")
    z, y = me // ny, me % ny
    length, features = hid.shape
    heads = pre.shape[0]
    columns = cot.shape[1]
    width = columns // heads
    tiles = columns // LANES
    per = LANES // width
    state = key.shape[1]
    groups = sbuf.shape[1]
    pack = tiles // groups
    rw = state // ny
    pr = pack * rw // nz
    rows = gw_ref.shape[0]
    own = gh_ref.shape[0]
    halves = 2 if ntp % 2 == 0 else 1
    core, x, nx = mine % halves, mine // halves, ntp // halves
    partner = mine + 1 - 2 * core
    hz = nz // ntp
    steps = wsem.shape[0]
    depth = features // steps
    ydev = [z * ny + (y + dy) % ny for dy in range(ny)]
    zdev = [((z + dz) % nz) * ny + y for dz in range(nz)]

    barrier = pltpu.get_barrier_semaphore()
    for dev in [zdev[dz] for dz in sorted(range(1, nz), key=lambda dz: -min(dz, nz - dz))] + ydev[1:]:
        pl.semaphore_signal(barrier, inc=1, device_id={"sp": dev}, device_id_type=MESH)
    for dt in range(1, ntp):
        pl.semaphore_signal(barrier, inc=1, device_id={"tp": (mine + dt) % ntp}, device_id_type=MESH)

    small = [
        pltpu.make_async_copy(pre_hbm, pre, insem.at[0]),
        pltpu.make_async_copy(rate_hbm, rate_ref, insem.at[4]),
        pltpu.make_async_copy(qry_hbm, qry, insem.at[1]),
        pltpu.make_async_copy(cot_hbm, cott, insem.at[2]),
        pltpu.make_async_copy(key_hbm, key, insem.at[3]),
    ]
    for copy in small:
        copy.start()
    wcopies = []
    for k in range(steps):
        at = pl.ds(k * depth, depth)
        wcopies.append(pltpu.make_async_copy(w_hbm.at[at, :], wt.at[at, :], wsem.at[k]))
    hload = pltpu.make_async_copy(hid_hbm, hid, insem.at[5])
    hload.start()
    for copy in wcopies:
        copy.start()

    outs = [
        pltpu.make_async_copy(gk_ref, gk_out, outsem.at[0]),
        pltpu.make_async_copy(gq_ref, gq_out, outsem.at[1]),
        pltpu.make_async_copy(gd_ref, gd_out, outsem.at[2]),
        pltpu.make_async_copy(gh_ref, gh_out, outsem.at[3]),
    ]
    for c in range(tiles):
        at = pl.ds(c * LANES, LANES)
        outs.append(pltpu.make_async_copy(gw_ref.at[:, at], gw_out.at[:, at], outsem.at[4]))

    def dcopy(dy, arrive=False):
        slot = (y + dy) % ny if arrive else y
        return remote(decb, ydec.at[slot], dsend, drecv, "sp", ydev[dy])

    def ycopy(m, g, dy):
        there = (y + dy) % ny
        return remote(sbuf.at[m, g, there], ybuf.at[m, g, y], ysend, yrecv.at[m, g], "sp", ydev[dy])

    def tcopy(m, g, dz):
        there = (z + dz) % nz
        return remote(tz.at[m, g, there], zbuf.at[m, g, z], tsend, trecv.at[m, g], "sp", zdev[dz])

    def ccopy(m, g, dz):
        there = (z + dz) % nz
        return remote(cz.at[m, g, there], zcar.at[m, g, z], csend, crecv.at[m, g], "sp", zdev[dz])

    def ocopy(m, g, dy):
        there = (y + dy) % ny
        return remote(ob.at[m, g, there], scr.at[m, g, y], osend, orecv.at[m, g], "sp", ydev[dy])

    def section(k):
        return pl.ds(pl.multiple_of(k * hz, hz), hz)

    def hcopy(dy, arrive=False):
        there = (y + dy) % ny
        slot = there if arrive else y
        return remote(
            ht.at[there, section(mine)], hg.at[slot, section(mine)], hsend, hrecv, "sp", ydev[dy]
        )

    def share(dy, dt, arrive=False):
        there = (y + dy) % ny
        peer = (mine + dt) % ntp
        which = peer if arrive else mine
        block = hg.at[there, section(which)]
        return remote(block, block, fsend, frecv, "tp", peer)

    def gcopy(c, dy, arrive=False):
        there = (y + dy) % ny
        slot = there if arrive else y
        return remote(gath.at[slot, c], gath.at[slot, c], gsend, grecv.at[c], "sp", ydev[dy])

    def pair():
        return remote(ghp.at[1 - core], pland, psend, precv, "tp", partner)

    def xcopy(dx, arrive=False):
        there = (x + dx) % nx
        slot = there if arrive else x
        return remote(red.at[there], xland.at[slot], xsend, xrecv, "tp", there * halves + core)

    def reach(c, d):
        far = nz // 2
        return far if (c + d) % 2 == 0 else nz - 1 - far

    def fast(c):
        return nz == 8 and c >= tiles - 2

    def ahead(k, d):
        return (z + k) % nz if d == 0 else (z + nz - k) % nz

    def rcopy(c, d, j):
        src = part.at[c, ahead(reach(c, d), d)] if j == 0 else ring.at[d, c, j - 1]
        return remote(
            src, ring.at[d, c, j], rsend, rrecv.at[slot_at(c, d, j)], "sp", zdev[1] if d == 0 else zdev[nz - 1]
        )

    def scopy(c, d, j):
        src, hops = (part.at[c, ahead(j + 2, d)], j + 1) if j < 3 else (ring.at[d, c, 0], 1)
        return remote(
            src, ring.at[d, c, j], rsend, rrecv.at[slot_at(c, d, j)], "sp", zdev[hops if d == 0 else nz - hops]
        )

    def slots(c, d):
        if fast(c):
            return tuple(range(reach(c, d) - 1)) + (3,)
        return tuple(range(reach(c, d)))

    def step_of(c, j):
        return j // 3 if fast(c) else j

    ring_slots = sorted({(c, d, step_of(c, j)) for c in range(tiles) for d in range(2) for j in slots(c, d)})

    def slot_at(c, d, j):
        return ring_slots.index((c, d, step_of(c, j)))

    def bulk(ref, send, recv):
        return remote(ref, ref, send, recv, "sp", ydev[1])

    row_at = lax.broadcasted_iota(jnp.int32, (length, length), 0)
    col_at = lax.broadcasted_iota(jnp.int32, (length, length), 1)
    eye = (row_at == col_at).astype(BF16)
    seg = (
        lax.broadcasted_iota(jnp.int32, (heads, columns), 1) // width
        == lax.broadcasted_iota(jnp.int32, (heads, columns), 0)
    ).astype(F32)
    lane = lax.broadcasted_iota(jnp.int32, (length, LANES), 1) // width

    def tile(q):
        return slice(q * LANES, (q + 1) * LANES)

    same = (
        lax.broadcasted_iota(jnp.int32, (heads, heads), 0) == lax.broadcasted_iota(jnp.int32, (heads, heads), 1)
    ).astype(F32)
    small[0].wait()
    small[1].wait()
    p = pre[...]
    rate = nt(same, jnp.broadcast_to(rate_ref[...], (heads, heads)), HIGH)[:, :1]
    log_decay = -rate * (jnp.maximum(p, 0.0) + jnp.log1p(jnp.exp(-jnp.abs(p))))
    lower = (row_at >= col_at).astype(F32)
    cum = nt(lower, log_decay, HIGH)
    cumt = nt(log_decay, lower, HIGH)
    cumx = nn(cum, seg, HIGH)
    totx = cumx[length - 1:length]
    decx = jnp.exp(totx)
    small[2].wait()
    small[3].wait()
    for q in range(tiles):
        cot[:, tile(q)] = nt(eye, cott[tile(q), :]).astype(BF16)
    ec = jnp.exp(cumx) * cot[...].astype(F32)
    ecot[...] = ec
    qryt = nt(eye, qry[...]).astype(BF16)
    hi, lo = split(ec)
    pull = nn(qryt, hi) + nn(qryt, lo)
    def spread(m, whole):
        for g in range(groups):
            for yy in range(ny):
                for i in range(pack):
                    sbuf[m, g, yy, i * rw:(i + 1) * rw] = whole[yy * rw:(yy + 1) * rw, tile(g * pack + i)]

    spread(0, pull)
    for q in range(tiles):
        decb[q:q + 1, :] = decx[:, tile(q)]

    with jax.named_scope("barrier"):
        pl.semaphore_wait(barrier, ny - 1 + nz - 1 + ntp - 1)
    for dy in range(1, ny):
        dcopy(dy).start()
    for g in range(groups):
        for dy in range(1, ny):
            ycopy(0, g, dy).start()
    ydec[y] = decb[...]
    ybuf[0, :, y] = sbuf[0, :, y]

    hload.wait()
    for b in range(features // LANES):
        block = nt(eye, hid[:, tile(b)])
        for i in range(LANES // rows):
            owner = b * LANES // rows + i
            ht[owner % ny, owner // ny] = block[i * rows:(i + 1) * rows]
    with jax.named_scope("send_h"):
        for dy in range(1, ny):
            hcopy(dy).start()
    tend[...] = jnp.exp(totx - cumx)
    small[4].wait()
    values = jnp.zeros((length, columns), F32)
    for k in range(steps):
        wcopies[k].wait()
        values = values + nn(hid[:, k * depth:(k + 1) * depth], wt[k * depth:(k + 1) * depth, :])
    vals = values.astype(BF16)
    xv = tend[...] * vals.astype(F32)
    xval[...] = xv
    keyt = nt(eye, key[...]).astype(BF16)
    hi, lo = split(xv)
    push = nn(keyt, hi) + nn(keyt, lo)
    spread(1, push)
    with jax.named_scope("send_y1"):
        for g in range(groups):
            for dy in range(1, ny):
                ycopy(1, g, dy).start()
    ybuf[1, :, y] = sbuf[1, :, y]

    hcol[:, :, pl.ds(pl.multiple_of(y * length, LANES), length)] = ht[y].astype(BF16)

    def scan_order(m, count):
        return list(range(count)) if m == 1 else list(reversed(range(count)))

    def stage_y(m, g):
        if m == 0 and g == 0:
            bulk(ydec.at[:ny - 1], dsend, drecv).wait_recv()
        bulk(ybuf.at[m, g, :ny - 1], ysend, yrecv.at[m, g]).wait_recv()
        order = scan_order(m, ny)
        for i in range(pack):
            q, at = g * pack + i, slice(i * rw, (i + 1) * rw)
            run = ybuf[m, g, order[0], at]
            for yy in order[1:]:
                run = ydec[yy, q:q + 1] * run + ybuf[m, g, yy, at]
            prod = ydec[0, q:q + 1]
            for yy in range(1, ny):
                prod = prod * ydec[yy, q:q + 1]
            for k in range(rw // pr):
                tz[m, g, i * (rw // pr) + k, :pr] = run[k * pr:(k + 1) * pr]
                tz[m, g, i * (rw // pr) + k, pr:pr + 1] = prod
        for dz in sorted(range(1, nz), key=lambda dz: -min(dz, nz - dz)):
            tcopy(m, g, dz).start()
        zbuf[m, g, z] = tz[m, g, z]

    def stage_z(m, g):
        bulk(zbuf.at[m, g, :nz - 1], tsend, trecv.at[m, g]).wait_recv()
        run = jnp.zeros((pr, LANES), F32)
        for zz in scan_order(m, nz):
            cz[m, g, zz] = run
            run = zbuf[m, g, zz, pr:pr + 1] * run + zbuf[m, g, zz, :pr]
        for dz in sorted(range(1, nz), key=lambda dz: -min(dz, nz - dz)):
            ccopy(m, g, dz).start()
        zcar[m, g, z] = cz[m, g, z]

    def stage_c(m, g):
        bulk(zcar.at[m, g, :nz - 1], csend, crecv.at[m, g]).wait_recv()
        for k in range(nz):
            crow[m, g, k * pr:(k + 1) * pr] = zcar[m, g, k]
        carry = crow[m, g]
        for i in range(pack):
            q, at = g * pack + i, slice(i * rw, (i + 1) * rw)
            now = carry[at]
            for yy in scan_order(m, ny):
                ob[m, g, yy, at] = now
                now = ydec[yy, q:q + 1] * now + ybuf[m, g, yy, at]
        for dy in sorted(range(1, ny), key=lambda dy: -min(dy, ny - dy)):
            ocopy(m, g, dy).start()
        scr[m, g, y] = ob[m, g, y]

    def stage(name, work, m):
        for g in range(groups):
            with jax.named_scope(f"{name}{m}{g}"):
                work(m, g)

    def state_tile(m, q):
        g, i = q // pack, q % pack
        return scr[m, g, :, i * rw:(i + 1) * rw].reshape(state, LANES)

    stage("stage_y", stage_y, 0)

    causal = row_at <= col_at
    scores = nt(key[...], qry[...])
    for q in range(tiles):
        lefts, rights = [], []
        ct = cot[:, tile(q)]
        for i in range(per):
            h = q * per + i
            across = cumt[h:h + 1, :] - cum[:, h:h + 1]
            dm = jnp.where(causal, jnp.exp(jnp.where(causal, across, 0.0)), 0.0)
            damp[h] = dm
            lefts.extend(split(scores * dm))
            masked = jnp.where(lane == i, ct, jnp.zeros_like(ct))
            rights.extend([masked, masked])
        gvloc[q] = nn(jnp.concatenate(lefts, axis=1), jnp.concatenate(rights, axis=0))

    with jax.named_scope("hid_y"):
        bulk(hg.at[:ny - 1, :hz], hsend, hrecv).wait_recv()
        for dt in range(1, ntp):
            for dy in range(1, ny):
                share(dy, dt).start()

    stage("stage_z", stage_z, 0)

    dsum = jnp.zeros((length, length), F32)
    for q in range(tiles):
        vt = vals[:, tile(q)]
        both = nt(
            jnp.concatenate([jnp.where(lane == i, vt, jnp.zeros_like(vt)) for i in range(per)], axis=0),
            cot[:, tile(q)],
        )
        for i in range(per):
            h = q * per + i
            ds = both[i * length:(i + 1) * length] * damp[h]
            flux = ds * scores
            dsum = dsum + ds
            rows8[h:h + 1, :] = jnp.sum(flux, axis=0, keepdims=True)
            cols8[:, h:h + 1] = jnp.sum(flux, axis=1, keepdims=True)

    stage("stage_c", stage_c, 0)

    stage("stage_y", stage_y, 1)

    hi, lo = split(dsum)
    gkl[...] = nn(hi, qry[...]) + nn(lo, qry[...])
    hi, lo = split(dsum.T)
    gql[...] = nn(hi, key[...]) + nn(lo, key[...])
    for g in range(groups):
        with jax.named_scope(f"wait_o0{g}"):
            bulk(scr.at[0, g, :ny - 1], osend, orecv.at[0, g]).wait_recv()
        for q in range(g * pack, (g + 1) * pack):
            hi, lo = split(state_tile(0, q))
            kg = nn(key[...], hi) + nn(key[...], lo)
            kgs[:, tile(q)] = kg
            gb = (gvloc[q] + tend[:, tile(q)] * kg).astype(BF16)
            gvb[:, tile(q)] = gb
            gath[y, q] = gb.astype(F32)
            for dy in sorted(range(1, ny), key=lambda dy: -min(dy, ny - dy)):
                gcopy(q, dy).start()

    stage("stage_z", stage_z, 1)

    def columns_in():
        if ntp > 1:
            bulk(hg.at[:ny - 1, :nz - hz], fsend, frecv).wait_recv()
        for dy in range(1, ny):
            there = (y + dy) % ny
            hcol[:, :, pl.ds(pl.multiple_of(there * length, LANES), length)] = hg[there].astype(BF16)

    def multiply(c):
        bulk(gath.at[:ny - 1, c], gsend, grecv.at[c]).wait_recv()
        block = gath[:, c].reshape(ny * length, LANES).astype(BF16)
        part[c] = nn(hcol[...].reshape(nz * rows, ny * length), block).reshape(nz, rows, LANES)
        for d in range(2):
            if fast(c):
                for j in reversed(range(reach(c, d) - 1)):
                    scopy(c, d, j).start()
            elif reach(c, d) > 0:
                rcopy(c, d, 0).start()

    def hop(c, d, j):
        rcopy(c, d, j).wait_recv()
        left = reach(c, d) - 1 - j
        if left > 0:
            ring[d, c, j] = ring[d, c, j] + part[c, ahead(left, d)]
            rcopy(c, d, j + 1).start()

    def step(c, d, j):
        if j == 3:
            scopy(c, d, 3).wait_recv()
        else:
            count = reach(c, d) - 1
            bulk(ring.at[d, c, :count], rsend, rrecv.at[slot_at(c, d, 0)]).wait_recv()
            total = part[c, ahead(1, d)]
            for k in range(count):
                total = total + ring[d, c, k]
            ring[d, c, 0] = total
            scopy(c, d, 3).start()

    def total_weight(c):
        total = part[c, z]
        for d in range(2):
            if fast(c):
                total = total + ring[d, c, 3]
            elif reach(c, d) > 0:
                total = total + ring[d, c, reach(c, d) - 1]
        gw_ref[:, tile(c)] = total
        outs[4 + c].start()

    def project():
        block = nt(gvb[...], wt[...])
        for t in range(ntp):
            ghp[t % halves, t // halves] = block[t * own:(t + 1) * own]
        if halves == 2:
            pair().start()

    def pairs():
        if halves == 2:
            pair().wait_recv()
            red[...] = ghp[core] + pland[...]
        else:
            red[...] = ghp[0]
        for dx in range(1, nx):
            xcopy(dx).start()

    def key_grads():
        gk = gkl[...]
        pulled = []
        for q in range(tiles):
            sgh, sgl = split(state_tile(0, q))
            xq = xval[:, tile(q)]
            xh, xl = split(xq)
            gk = gk + (nt(xh, sgh) + nt(xl, sgh) + nt(xh, sgl))
            pulled.append(xq * kgs[:, tile(q)])
        gk_ref[...] = gk.astype(BF16)
        outs[0].start()
        prefix_in = nt(seg, jnp.concatenate(pulled, axis=1), HIGH)
        gd_ref[...] = nn(prefix_in, (row_at < col_at).astype(F32), HIGH)

    def query_grads():
        with jax.named_scope("wait_o1"):
            for g in range(groups):
                bulk(scr.at[1, g, :ny - 1], osend, orecv.at[1, g]).wait_recv()
        gq = gql[...]
        into, through = [], []
        for q in range(tiles):
            si, sg = state_tile(1, q), state_tile(0, q)
            sih, sil = split(si)
            eq = ecot[:, tile(q)]
            eh, el = split(eq)
            gq = gq + (nt(eh, sih) + nt(el, sih) + nt(eh, sil))
            into.append(eq * (nn(qry[...], sih) + nn(qry[...], sil)))
            through.append(jnp.sum(si * sg, axis=0, keepdims=True))
        gq_ref[...] = gq.astype(BF16)
        outs[1].start()
        suffix_in = nt(seg, jnp.concatenate(into, axis=1), HIGH) - nt(same, cols8[...], HIGH) + rows8[...]
        crossing = nt(seg, jnp.broadcast_to(decx * jnp.concatenate(through, axis=1), (SUB, columns)), HIGH)[:, :1]
        total = nn(suffix_in, lower, HIGH) + gd_ref[...] + crossing
        gd_ref[...] = total * -rate * (1.0 / (1.0 + jnp.exp(-p)))
        outs[2].start()

    def total_hidden():
        total = red[x]
        if nx > 1:
            bulk(xland.at[:nx - 1], xsend, xrecv).wait_recv()
        for dx in range(1, nx):
            total = total + xland[(x + dx) % nx]
        gh_ref[...] = total.astype(gh_ref.dtype)
        outs[3].start()

    def drain():
        bulk(ydec.at[:ny - 1], dsend, drecv).wait_send()
        bulk(ht.at[:ny - 1, :hz], hsend, hrecv).wait_send()
        if ntp > 1:
            bulk(hg.at[:ny - 1, :nz - hz], fsend, frecv).wait_send()
        bulk(sbuf.at[:, :, :ny - 1], ysend, yrecv.at[0, 0]).wait_send()
        bulk(tz.at[:, :, :nz - 1], tsend, trecv.at[0, 0]).wait_send()
        bulk(cz.at[:, :, :nz - 1], csend, crecv.at[0, 0]).wait_send()
        bulk(ob.at[:, :, :ny - 1], osend, orecv.at[0, 0]).wait_send()
        bulk(gath.at[:ny - 1], gsend, grecv.at[0]).wait_send()
        if halves == 2:
            pair().wait_send()

    tasks = [
        (1.0, "project", project), (1.9, "columns_in", columns_in),
        (6.1, "stage_c1", functools.partial(stage, "stage_c", stage_c, 1)), (3.0, "key_grads", key_grads),
        (9.6, "pairs", pairs), (17.9, "query_grads", query_grads), (18.0, "drain", drain),
        (18.2, "total_hidden", total_hidden),
    ]
    arrive = (4.5, 6.0, 8.5, 11.0)
    for c in range(tiles):
        ready = arrive[c % 4] + 7.0 * (c // 4)
        tasks.append((ready, f"multiply{c}", functools.partial(multiply, c)))
        last = ready
        for d in range(2):
            for j in slots(c, d):
                if fast(c) and j not in (0, 3):
                    continue
                if fast(c):
                    at = ready + (4.0 if j < 3 else 8.0) + 0.1 * d
                    tasks.append((at, f"step{c}{d}{j}", functools.partial(step, c, d, j)))
                else:
                    at = ready + 3.5 * (j + 1)
                    tasks.append((at, f"hop{c}{d}{j}", functools.partial(hop, c, d, j)))
                last = max(last, at)
        tasks.append((last + 0.01, f"total{c}", functools.partial(total_weight, c)))
    for _, name, task in sorted(tasks, key=lambda item: item[0]):
        with jax.named_scope(name):
            task()

    with jax.named_scope("drain_ring"):
        bulk(part.at[:, :nz - 1], rsend, rrecv.at[0]).wait_send()
        if nx > 1:
            bulk(red.at[:nx - 1], xsend, xrecv).wait_send()
    with jax.named_scope("outs"):
        for copy in outs[:4]:
            copy.wait()
        pltpu.make_async_copy(gw_ref, gw_out, outsem.at[4]).wait()


def finish_kernel(*refs):
    count = (len(refs) - 1) // 3
    ins, outs, held, sems = refs[:count], refs[count:2 * count], refs[2 * count:3 * count], refs[-1]
    loads = [pltpu.make_async_copy(ins[k], held[k], sems.at[0, k]) for k in range(count)]
    stores = [pltpu.make_async_copy(held[k], outs[k], sems.at[1, k]) for k in range(count)]
    for load in loads:
        load.start()
    for load, store in zip(loads, stores):
        load.wait()
        store.start()
    for store in stores:
        store.wait()


HBM = pl.BlockSpec(memory_space=pltpu.HBM)
LIMIT = 60 * 1024 * 1024


def per_device(sp, tp, hidden, value_weight, key_vecs, queries, decay_pre, decay_rate, cotangent):
    length, features = hidden.shape
    heads = decay_rate.shape[0]
    state = key_vecs.shape[2]
    columns = value_weight.shape[1]
    ny = inner_size(sp)
    nz = sp // ny
    tiles = columns // LANES
    groups = tiles
    pack = tiles // groups
    rw = state // ny
    pr = pack * rw // nz
    rows = features // sp
    own = length // tp
    halves = 2 if tp % 2 == 0 else 1
    nx = tp // halves
    far = nz // 2
    steps = 2
    vm = pltpu.VMEM
    dma = pltpu.SemaphoreType.DMA
    outs = pl.pallas_call(
        functools.partial(mixer_kernel, ny, nz, tp),
        out_shape=(
            jax.ShapeDtypeStruct((length, state), BF16),
            jax.ShapeDtypeStruct((length, state), BF16),
            jax.ShapeDtypeStruct((heads, length), F32),
            jax.ShapeDtypeStruct((own, features), BF16),
            jax.ShapeDtypeStruct((rows, columns), F32),
        ),
        in_specs=[HBM] * 7,
        out_specs=(HBM,) * 5,
        scratch_shapes=[
            vm((length, state), BF16),
            vm((length, state), BF16),
            vm((heads, length), F32),
            vm((own, features), BF16),
            vm((rows, columns), F32),
            vm((length, features), BF16),
            vm((features, columns), BF16),
            vm((length, state), BF16),
            vm((length, state), BF16),
            vm((heads, length), F32),
            vm((1, heads), F32),
            vm((columns, length), BF16),
            vm((length, columns), BF16),
            vm((length, columns), F32),
            vm((length, columns), F32),
            vm((length, columns), F32),
            vm((heads, length, length), F32),
            vm((tiles, length, LANES), F32),
            vm((length, columns), BF16),
            vm((length, columns), F32),
            vm((heads, length), F32),
            vm((length, heads), F32),
            vm((length, state), F32),
            vm((length, state), F32),
            vm((2, groups, ny, pack * rw, LANES), F32),
            vm((SUB, LANES), F32),
            vm((2, groups, ny, pack * rw, LANES), F32),
            vm((ny, SUB, LANES), F32),
            vm((2, groups, nz, -(-(pr + 1) // SUB) * SUB, LANES), F32),
            vm((2, groups, nz, -(-(pr + 1) // SUB) * SUB, LANES), F32),
            vm((2, groups, nz, pr, LANES), F32),
            vm((2, groups, nz, pr, LANES), F32),
            vm((2, groups, pack * rw, LANES), F32),
            vm((2, groups, ny, pack * rw, LANES), F32),
            vm((2, groups, ny, pack * rw, LANES), F32),
            vm((ny, nz, rows, length), F32),
            vm((ny, nz, rows, length), F32),
            vm((nz, rows, ny * length), BF16),
            vm((ny, tiles, length, LANES), F32),
            vm((tiles, nz, rows, LANES), F32),
            vm((2, tiles, far, rows, LANES), F32),
            vm((halves, nx, own, features), F32),
            vm((nx, own, features), F32),
            vm((nx, own, features), F32),
            vm((nx, own, features), F32),
            dma((6,)), dma((steps,)),
            dma, dma,
            dma, dma((2, groups)),
            dma, dma((2, groups)),
            dma, dma((2, groups)),
            dma, dma((2, groups)),
            dma, dma,
            dma, dma,
            dma, dma((tiles,)),
            dma, dma((tiles * (nz - 1) - (3 * 2 if nz == 8 else 0),)),
            dma, dma,
            dma, dma,
            dma((5,)),
        ],
        compiler_params=pltpu.CompilerParams(collective_id=0, has_side_effects=True, vmem_limit_bytes=LIMIT),
        name="mixer_backward",
    )(
        hidden, value_weight, key_vecs.reshape(length, state), queries.reshape(length, state), decay_pre.T,
        decay_rate.reshape(1, heads), cotangent.reshape(length, columns).T,
    )
    gk, gq, gd, gh, gw = pl.pallas_call(
        finish_kernel,
        out_shape=tuple(jax.ShapeDtypeStruct(o.shape, o.dtype) for o in outs),
        in_specs=[HBM] * 5,
        out_specs=(HBM,) * 5,
        scratch_shapes=[vm(o.shape, o.dtype) for o in outs] + [dma((2, 5))],
        compiler_params=pltpu.CompilerParams(vmem_limit_bytes=LIMIT),
        name="write_out",
    )(*outs)
    return gk.reshape(key_vecs.shape), gq.reshape(key_vecs.shape), gd.T, gh, gw


def solution(mesh):
    return jax.shard_map(
        functools.partial(per_device, mesh.shape["sp"], mesh.shape["tp"]),
        mesh=mesh,
        in_specs=(
            P("sp", None),
            P(None, "tp"),
            P("sp", "tp", None),
            P("sp", "tp", None),
            P("sp", "tp"),
            P("tp"),
            P("sp", "tp", None),
        ),
        out_specs=(
            P("sp", "tp", None),
            P("sp", "tp", None),
            P("sp", "tp"),
            P(("sp", "tp"), None),
            P("sp", "tp"),
        ),
        check_vma=False,
    )
```

```python
import functools

import jax
import jax.numpy as jnp
from jax import lax
from jax.experimental import pallas as pl
from jax.experimental.pallas import tpu as pltpu
from jax.sharding import PartitionSpec as P

MESH = pl.DeviceIdType.MESH
F32 = jnp.float32
BF16 = jnp.bfloat16
HIGH = lax.Precision.HIGHEST
LANES = 128
SUB = 8


def inner_size(count):
    size = 1
    while size * size * 4 <= count:
        size *= 2
    while count % size:
        size -= 1
    return size


def remote(src, dst, send, recv, axis, index):
    return pltpu.make_async_remote_copy(
        src_ref=src, dst_ref=dst, send_sem=send, recv_sem=recv, device_id={axis: index}, device_id_type=MESH
    )


def nn(a, b, precision=None):
    return jnp.dot(a, b, preferred_element_type=F32, precision=precision)


def nt(a, b, precision=None):
    return lax.dot_general(a, b, (((1,), (1,)), ((), ())), preferred_element_type=F32, precision=precision)


def split(x):
    hi = x.astype(BF16)
    return hi, (x - hi.astype(F32)).astype(BF16)


def mixer_kernel(ny, nz, ntp, hid_hbm, w_hbm, key_hbm, qry_hbm, pre_hbm, rate_hbm, cot_hbm,
                 gk_out, gq_out, gd_out, gh_out, gw_out,
                 gk_ref, gq_ref, gd_ref, gh_ref, gw_ref, hid, wt, key, qry, pre, rate_ref, cott, cot,
                 ecot, tend, xval, damp, gvloc, gvb, kgs, rows8, cols8, gkl, gql,
                 sbuf, decb, ybuf, ydec, tz, zbuf, cz, zcar, crow, ob, scr, ht, hg, hcol,
                 gath, part, ring, ghp, pland, red, xland,
                 insem, wsem, dsend, drecv, ysend, yrecv, tsend, trecv, csend, crecv, osend, orecv,
                 hsend, hrecv, fsend, frecv, gsend, grecv, rsend, rrecv, psend, precv, xsend, xrecv, outsem):
    me = lax.axis_index("sp")
    mine = lax.axis_index("tp")
    z, y = me // ny, me % ny
    length, features = hid.shape
    heads = pre.shape[0]
    columns = cot.shape[1]
    width = columns // heads
    tiles = columns // LANES
    per = LANES // width
    state = key.shape[1]
    groups = sbuf.shape[1]
    pack = tiles // groups
    rw = state // ny
    pr = pack * rw // nz
    rows = gw_ref.shape[0]
    own = gh_ref.shape[0]
    halves = 2 if ntp % 2 == 0 else 1
    core, x, nx = mine % halves, mine // halves, ntp // halves
    partner = mine + 1 - 2 * core
    hz = nz // ntp
    steps = wsem.shape[0]
    depth = features // steps
    ydev = [z * ny + (y + dy) % ny for dy in range(ny)]
    zdev = [((z + dz) % nz) * ny + y for dz in range(nz)]

    barrier = pltpu.get_barrier_semaphore()
    for dev in [zdev[dz] for dz in sorted(range(1, nz), key=lambda dz: -min(dz, nz - dz))] + ydev[1:]:
        pl.semaphore_signal(barrier, inc=1, device_id={"sp": dev}, device_id_type=MESH)
    for dt in range(1, ntp):
        pl.semaphore_signal(barrier, inc=1, device_id={"tp": (mine + dt) % ntp}, device_id_type=MESH)

    small = [
        pltpu.make_async_copy(pre_hbm, pre, insem.at[0]),
        pltpu.make_async_copy(rate_hbm, rate_ref, insem.at[4]),
        pltpu.make_async_copy(qry_hbm, qry, insem.at[1]),
        pltpu.make_async_copy(cot_hbm, cott, insem.at[2]),
        pltpu.make_async_copy(key_hbm, key, insem.at[3]),
    ]
    for copy in small:
        copy.start()
    wcopies = []
    for k in range(steps):
        at = pl.ds(k * depth, depth)
        wcopies.append(pltpu.make_async_copy(w_hbm.at[at, :], wt.at[at, :], wsem.at[k]))
    hload = pltpu.make_async_copy(hid_hbm, hid, insem.at[5])
    hload.start()
    for copy in wcopies:
        copy.start()

    outs = [
        pltpu.make_async_copy(gk_ref, gk_out, outsem.at[0]),
        pltpu.make_async_copy(gq_ref, gq_out, outsem.at[1]),
        pltpu.make_async_copy(gd_ref, gd_out, outsem.at[2]),
        pltpu.make_async_copy(gh_ref, gh_out, outsem.at[3]),
    ]
    for c in range(tiles):
        at = pl.ds(c * LANES, LANES)
        outs.append(pltpu.make_async_copy(gw_ref.at[:, at], gw_out.at[:, at], outsem.at[4]))

    def dcopy(dy, arrive=False):
        slot = (y + dy) % ny if arrive else y
        return remote(decb, ydec.at[slot], dsend, drecv, "sp", ydev[dy])

    def ycopy(m, g, dy):
        there = (y + dy) % ny
        return remote(sbuf.at[m, g, there], ybuf.at[m, g, y], ysend, yrecv.at[g + m * (groups - g)], "sp", ydev[dy])

    def tcopy(m, g, dz):
        there = (z + dz) % nz
        return remote(tz.at[m, g, there], zbuf.at[m, g, z], tsend, trecv.at[g + m * (groups - g)], "sp", zdev[dz])

    def ccopy(m, g, dz):
        there = (z + dz) % nz
        return remote(cz.at[m, g, there], zcar.at[m, g, z], csend, crecv.at[g + m * (groups - g)], "sp", zdev[dz])

    def ocopy(m, g, dy):
        there = (y + dy) % ny
        return remote(ob.at[m, g, there], scr.at[m, g, y], osend, orecv.at[g + m * (groups - g)], "sp", ydev[dy])

    def section(k):
        return pl.ds(pl.multiple_of(k * hz, hz), hz)

    def hcopy(dy, arrive=False):
        there = (y + dy) % ny
        slot = there if arrive else y
        return remote(
            ht.at[there, section(mine)], hg.at[slot, section(mine)], hsend, hrecv, "sp", ydev[dy]
        )

    def share(dy, dt, arrive=False):
        there = (y + dy) % ny
        peer = (mine + dt) % ntp
        which = peer if arrive else mine
        block = hg.at[there, section(which)]
        return remote(block, block, fsend, frecv, "tp", peer)

    def gcopy(c, dy, arrive=False):
        there = (y + dy) % ny
        slot = there if arrive else y
        return remote(gath.at[slot, c], gath.at[slot, c], gsend, grecv.at[c], "sp", ydev[dy])

    def pair():
        return remote(ghp.at[1 - core], pland, psend, precv, "tp", partner)

    def xcopy(dx, arrive=False):
        there = (x + dx) % nx
        slot = there if arrive else x
        return remote(red.at[there], xland.at[slot], xsend, xrecv, "tp", there * halves + core)

    def reach(c, d):
        far = nz // 2
        return far if (c + d) % 2 == 0 else nz - 1 - far

    def fast(c):
        return nz == 8 and c >= tiles - 2

    def ahead(k, d):
        return (z + k) % nz if d == 0 else (z + nz - k) % nz

    def rcopy(c, d, j):
        src = part.at[c, ahead(reach(c, d), d)] if j == 0 else ring.at[d, c, j - 1]
        return remote(
            src, ring.at[d, c, j], rsend, rrecv.at[slot_at(c, d, j)], "sp", zdev[1] if d == 0 else zdev[nz - 1]
        )

    def scopy(c, d, j):
        src, hops = (part.at[c, ahead(j + 2, d)], j + 1) if j < 3 else (ring.at[d, c, 0], 1)
        return remote(
            src, ring.at[d, c, j], rsend, rrecv.at[slot_at(c, d, j)], "sp", zdev[hops if d == 0 else nz - hops]
        )

    def slots(c, d):
        if fast(c):
            return tuple(range(reach(c, d) - 1)) + (3,)
        return tuple(range(reach(c, d)))

    def step_of(c, j):
        return j // 3 if fast(c) else j

    ring_slots = sorted({(c, d, step_of(c, j)) for c in range(tiles) for d in range(2) for j in slots(c, d)})

    def slot_at(c, d, j):
        return ring_slots.index((c, d, step_of(c, j)))

    def bulk(ref, send, recv):
        return remote(ref, ref, send, recv, "sp", ydev[1])

    row_at = lax.broadcasted_iota(jnp.int32, (length, length), 0)
    col_at = lax.broadcasted_iota(jnp.int32, (length, length), 1)
    eye = (row_at == col_at).astype(BF16)
    seg = (
        lax.broadcasted_iota(jnp.int32, (heads, columns), 1) // width
        == lax.broadcasted_iota(jnp.int32, (heads, columns), 0)
    ).astype(F32)
    lane = lax.broadcasted_iota(jnp.int32, (length, LANES), 1) // width

    def tile(q):
        return slice(q * LANES, (q + 1) * LANES)

    same = (
        lax.broadcasted_iota(jnp.int32, (heads, heads), 0) == lax.broadcasted_iota(jnp.int32, (heads, heads), 1)
    ).astype(F32)
    small[0].wait()
    small[1].wait()
    p = pre[...]
    rate = nt(same, jnp.broadcast_to(rate_ref[...], (heads, heads)), HIGH)[:, :1]
    log_decay = -rate * (jnp.maximum(p, 0.0) + jnp.log1p(jnp.exp(-jnp.abs(p))))
    lower = (row_at >= col_at).astype(F32)
    cum = nt(lower, log_decay, HIGH)
    cumt = nt(log_decay, lower, HIGH)
    cumx = nn(cum, seg, HIGH)
    totx = cumx[length - 1:length]
    decx = jnp.exp(totx)
    small[2].wait()
    small[3].wait()
    for q in range(tiles):
        cot[:, tile(q)] = nt(eye, cott[tile(q), :]).astype(BF16)
    ec = jnp.exp(cumx) * cot[...].astype(F32)
    ecot[...] = ec
    qryt = nt(eye, qry[...]).astype(BF16)
    hi, lo = split(ec)
    pull = nn(qryt, hi) + nn(qryt, lo)
    def spread(m, whole):
        for g in range(groups):
            for yy in range(ny):
                for i in range(pack):
                    sbuf[m, g, yy, i * rw:(i + 1) * rw] = whole[yy * rw:(yy + 1) * rw, tile(g * pack + i)]

    spread(0, pull)
    for q in range(tiles):
        decb[q:q + 1, :] = decx[:, tile(q)]

    with jax.named_scope("barrier"):
        pl.semaphore_wait(barrier, ny - 1 + nz - 1 + ntp - 1)
    for dy in range(1, ny):
        dcopy(dy).start()
    for g in range(groups):
        for dy in range(1, ny):
            ycopy(0, g, dy).start()
    ydec[y] = decb[...]
    ybuf[0, :, y] = sbuf[0, :, y]

    hload.wait()
    for b in range(features // LANES):
        block = nt(eye, hid[:, tile(b)])
        for i in range(LANES // rows):
            owner = b * LANES // rows + i
            ht[owner % ny, owner // ny] = block[i * rows:(i + 1) * rows]
    with jax.named_scope("send_h"):
        for dy in range(1, ny):
            hcopy(dy).start()
    tend[...] = jnp.exp(totx - cumx)
    small[4].wait()
    values = jnp.zeros((length, columns), F32)
    for k in range(steps):
        wcopies[k].wait()
        values = values + nn(hid[:, k * depth:(k + 1) * depth], wt[k * depth:(k + 1) * depth, :])
    vals = values.astype(BF16)
    xv = tend[...] * vals.astype(F32)
    xval[...] = xv
    keyt = nt(eye, key[...]).astype(BF16)
    hi, lo = split(xv)
    push = nn(keyt, hi) + nn(keyt, lo)
    spread(1, push)
    with jax.named_scope("send_y1"):
        for g in range(groups):
            for dy in range(1, ny):
                ycopy(1, g, dy).start()
    ybuf[1, :, y] = sbuf[1, :, y]

    hcol[:, :, pl.ds(pl.multiple_of(y * length, LANES), length)] = ht[y].astype(BF16)

    def scan_order(m, count):
        return list(range(count)) if m == 1 else list(reversed(range(count)))

    def stage_y(m, g):
        if m == 0 and g == 0:
            bulk(ydec.at[:ny - 1], dsend, drecv).wait_recv()
        if m == 0:
            bulk(ybuf.at[0, g, :ny - 1], ysend, yrecv.at[g]).wait_recv()
        elif g == 0:
            bulk(ybuf.at[1, :, :ny - 1], ysend, yrecv.at[groups]).wait_recv()
        order = scan_order(m, ny)
        for i in range(pack):
            q, at = g * pack + i, slice(i * rw, (i + 1) * rw)
            run = ybuf[m, g, order[0], at]
            for yy in order[1:]:
                run = ydec[yy, q:q + 1] * run + ybuf[m, g, yy, at]
            prod = ydec[0, q:q + 1]
            for yy in range(1, ny):
                prod = prod * ydec[yy, q:q + 1]
            for k in range(rw // pr):
                tz[m, g, i * (rw // pr) + k, :pr] = run[k * pr:(k + 1) * pr]
                tz[m, g, i * (rw // pr) + k, pr:pr + 1] = prod
        for dz in sorted(range(1, nz), key=lambda dz: -min(dz, nz - dz)):
            tcopy(m, g, dz).start()
        zbuf[m, g, z] = tz[m, g, z]

    def stage_z(m, g):
        if m == 0:
            bulk(zbuf.at[0, g, :nz - 1], tsend, trecv.at[g]).wait_recv()
        elif g == 0:
            bulk(zbuf.at[1, :, :nz - 1], tsend, trecv.at[groups]).wait_recv()
        run = jnp.zeros((pr, LANES), F32)
        for zz in scan_order(m, nz):
            cz[m, g, zz] = run
            run = zbuf[m, g, zz, pr:pr + 1] * run + zbuf[m, g, zz, :pr]
        for dz in sorted(range(1, nz), key=lambda dz: -min(dz, nz - dz)):
            ccopy(m, g, dz).start()
        zcar[m, g, z] = cz[m, g, z]

    def stage_c(m, g):
        if m == 0:
            bulk(zcar.at[0, g, :nz - 1], csend, crecv.at[g]).wait_recv()
        elif g == 0:
            bulk(zcar.at[1, :, :nz - 1], csend, crecv.at[groups]).wait_recv()
        for k in range(nz):
            crow[m, g, k * pr:(k + 1) * pr] = zcar[m, g, k]
        carry = crow[m, g]
        for i in range(pack):
            q, at = g * pack + i, slice(i * rw, (i + 1) * rw)
            now = carry[at]
            for yy in scan_order(m, ny):
                ob[m, g, yy, at] = now
                now = ydec[yy, q:q + 1] * now + ybuf[m, g, yy, at]
        for dy in sorted(range(1, ny), key=lambda dy: -min(dy, ny - dy)):
            ocopy(m, g, dy).start()
        scr[m, g, y] = ob[m, g, y]

    def stage(name, work, m):
        for g in range(groups):
            with jax.named_scope(f"{name}{m}{g}"):
                work(m, g)

    def state_tile(m, q):
        g, i = q // pack, q % pack
        return scr[m, g, :, i * rw:(i + 1) * rw].reshape(state, LANES)

    stage("stage_y", stage_y, 0)

    causal = row_at <= col_at
    scores = nt(key[...], qry[...])
    for q in range(tiles):
        lefts, rights = [], []
        ct = cot[:, tile(q)]
        for i in range(per):
            h = q * per + i
            across = cumt[h:h + 1, :] - cum[:, h:h + 1]
            dm = jnp.where(causal, jnp.exp(jnp.where(causal, across, 0.0)), 0.0)
            damp[h] = dm
            lefts.extend(split(scores * dm))
            masked = jnp.where(lane == i, ct, jnp.zeros_like(ct))
            rights.extend([masked, masked])
        gvloc[q] = nn(jnp.concatenate(lefts, axis=1), jnp.concatenate(rights, axis=0))

    with jax.named_scope("hid_y"):
        bulk(hg.at[:ny - 1, :hz], hsend, hrecv).wait_recv()
        for dt in range(1, ntp):
            for dy in range(1, ny):
                share(dy, dt).start()

    stage("stage_z", stage_z, 0)

    dsum = jnp.zeros((length, length), F32)
    for q in range(tiles):
        vt = vals[:, tile(q)]
        both = nt(
            jnp.concatenate([jnp.where(lane == i, vt, jnp.zeros_like(vt)) for i in range(per)], axis=0),
            cot[:, tile(q)],
        )
        for i in range(per):
            h = q * per + i
            ds = both[i * length:(i + 1) * length] * damp[h]
            flux = ds * scores
            dsum = dsum + ds
            rows8[h:h + 1, :] = jnp.sum(flux, axis=0, keepdims=True)
            cols8[:, h:h + 1] = jnp.sum(flux, axis=1, keepdims=True)

    stage("stage_c", stage_c, 0)

    stage("stage_y", stage_y, 1)

    hi, lo = split(dsum)
    gkl[...] = nn(hi, qry[...]) + nn(lo, qry[...])
    hi, lo = split(dsum.T)
    gql[...] = nn(hi, key[...]) + nn(lo, key[...])
    for g in range(groups):
        with jax.named_scope(f"wait_o0{g}"):
            bulk(scr.at[0, g, :ny - 1], osend, orecv.at[g]).wait_recv()
        for q in range(g * pack, (g + 1) * pack):
            hi, lo = split(state_tile(0, q))
            kg = nn(key[...], hi) + nn(key[...], lo)
            kgs[:, tile(q)] = kg
            gb = (gvloc[q] + tend[:, tile(q)] * kg).astype(BF16)
            gvb[:, tile(q)] = gb
            gath[y, q] = gb.astype(F32)
            for dy in sorted(range(1, ny), key=lambda dy: -min(dy, ny - dy)):
                gcopy(q, dy).start()

    stage("stage_z", stage_z, 1)

    def columns_in():
        if ntp > 1:
            bulk(hg.at[:ny - 1, :nz - hz], fsend, frecv).wait_recv()
        for dy in range(1, ny):
            there = (y + dy) % ny
            hcol[:, :, pl.ds(pl.multiple_of(there * length, LANES), length)] = hg[there].astype(BF16)

    def multiply(c):
        bulk(gath.at[:ny - 1, c], gsend, grecv.at[c]).wait_recv()
        block = gath[:, c].reshape(ny * length, LANES).astype(BF16)
        part[c] = nn(hcol[...].reshape(nz * rows, ny * length), block).reshape(nz, rows, LANES)
        for d in range(2):
            if fast(c):
                for j in reversed(range(reach(c, d) - 1)):
                    scopy(c, d, j).start()
            elif reach(c, d) > 0:
                rcopy(c, d, 0).start()

    def hop(c, d, j):
        rcopy(c, d, j).wait_recv()
        left = reach(c, d) - 1 - j
        if left > 0:
            ring[d, c, j] = ring[d, c, j] + part[c, ahead(left, d)]
            rcopy(c, d, j + 1).start()

    def step(c, d, j):
        if j == 3:
            scopy(c, d, 3).wait_recv()
        else:
            count = reach(c, d) - 1
            bulk(ring.at[d, c, :count], rsend, rrecv.at[slot_at(c, d, 0)]).wait_recv()
            total = part[c, ahead(1, d)]
            for k in range(count):
                total = total + ring[d, c, k]
            ring[d, c, 0] = total
            scopy(c, d, 3).start()

    def total_weight(c):
        total = part[c, z]
        for d in range(2):
            if fast(c):
                total = total + ring[d, c, 3]
            elif reach(c, d) > 0:
                total = total + ring[d, c, reach(c, d) - 1]
        gw_ref[:, tile(c)] = total
        outs[4 + c].start()

    def project():
        block = nt(gvb[...], wt[...])
        for t in range(ntp):
            ghp[t % halves, t // halves] = block[t * own:(t + 1) * own]
        if halves == 2:
            pair().start()

    def pairs():
        if halves == 2:
            pair().wait_recv()
            red[...] = ghp[core] + pland[...]
        else:
            red[...] = ghp[0]
        for dx in range(1, nx):
            xcopy(dx).start()

    def key_grads():
        gk = gkl[...]
        pulled = []
        for q in range(tiles):
            sgh, sgl = split(state_tile(0, q))
            xq = xval[:, tile(q)]
            xh, xl = split(xq)
            gk = gk + (nt(xh, sgh) + nt(xl, sgh) + nt(xh, sgl))
            pulled.append(xq * kgs[:, tile(q)])
        gk_ref[...] = gk.astype(BF16)
        outs[0].start()
        prefix_in = nt(seg, jnp.concatenate(pulled, axis=1), HIGH)
        gd_ref[...] = nn(prefix_in, (row_at < col_at).astype(F32), HIGH)

    def query_grads():
        with jax.named_scope("wait_o1"):
            bulk(scr.at[1, :, :ny - 1], osend, orecv.at[groups]).wait_recv()
        gq = gql[...]
        into, through = [], []
        for q in range(tiles):
            si, sg = state_tile(1, q), state_tile(0, q)
            sih, sil = split(si)
            eq = ecot[:, tile(q)]
            eh, el = split(eq)
            gq = gq + (nt(eh, sih) + nt(el, sih) + nt(eh, sil))
            into.append(eq * (nn(qry[...], sih) + nn(qry[...], sil)))
            through.append(jnp.sum(si * sg, axis=0, keepdims=True))
        gq_ref[...] = gq.astype(BF16)
        outs[1].start()
        suffix_in = nt(seg, jnp.concatenate(into, axis=1), HIGH) - nt(same, cols8[...], HIGH) + rows8[...]
        crossing = nt(seg, jnp.broadcast_to(decx * jnp.concatenate(through, axis=1), (SUB, columns)), HIGH)[:, :1]
        total = nn(suffix_in, lower, HIGH) + gd_ref[...] + crossing
        gd_ref[...] = total * -rate * (1.0 / (1.0 + jnp.exp(-p)))
        outs[2].start()

    def total_hidden():
        total = red[x]
        if nx > 1:
            bulk(xland.at[:nx - 1], xsend, xrecv).wait_recv()
        for dx in range(1, nx):
            total = total + xland[(x + dx) % nx]
        gh_ref[...] = total.astype(gh_ref.dtype)
        outs[3].start()

    def drain():
        bulk(ydec.at[:ny - 1], dsend, drecv).wait_send()
        bulk(ht.at[:ny - 1, :hz], hsend, hrecv).wait_send()
        if ntp > 1:
            bulk(hg.at[:ny - 1, :nz - hz], fsend, frecv).wait_send()
        bulk(sbuf.at[:, :, :ny - 1], ysend, yrecv.at[0]).wait_send()
        bulk(tz.at[:, :, :nz - 1], tsend, trecv.at[0]).wait_send()
        bulk(cz.at[:, :, :nz - 1], csend, crecv.at[0]).wait_send()
        bulk(ob.at[:, :, :ny - 1], osend, orecv.at[0]).wait_send()
        bulk(gath.at[:ny - 1], gsend, grecv.at[0]).wait_send()
        if halves == 2:
            pair().wait_send()

    tasks = [
        (1.0, "project", project), (1.9, "columns_in", columns_in),
        (6.1, "stage_c1", functools.partial(stage, "stage_c", stage_c, 1)), (3.0, "key_grads", key_grads),
        (9.6, "pairs", pairs), (17.9, "query_grads", query_grads), (18.0, "drain", drain),
        (18.2, "total_hidden", total_hidden),
    ]
    arrive = (4.5, 6.0, 8.5, 11.0)
    for c in range(tiles):
        ready = arrive[c % 4] + 7.0 * (c // 4)
        tasks.append((ready, f"multiply{c}", functools.partial(multiply, c)))
        last = ready
        for d in range(2):
            for j in slots(c, d):
                if fast(c) and j not in (0, 3):
                    continue
                if fast(c):
                    at = ready + (4.0 if j < 3 else 8.0) + 0.1 * d
                    tasks.append((at, f"step{c}{d}{j}", functools.partial(step, c, d, j)))
                else:
                    at = ready + 3.5 * (j + 1)
                    tasks.append((at, f"hop{c}{d}{j}", functools.partial(hop, c, d, j)))
                last = max(last, at)
        tasks.append((last + 0.01, f"total{c}", functools.partial(total_weight, c)))
    for _, name, task in sorted(tasks, key=lambda item: item[0]):
        with jax.named_scope(name):
            task()

    with jax.named_scope("drain_ring"):
        bulk(part.at[:, :nz - 1], rsend, rrecv.at[0]).wait_send()
        if nx > 1:
            bulk(red.at[:nx - 1], xsend, xrecv).wait_send()
    with jax.named_scope("outs"):
        for copy in outs[:4]:
            copy.wait()
        pltpu.make_async_copy(gw_ref, gw_out, outsem.at[4]).wait()


def finish_kernel(*refs):
    count = (len(refs) - 1) // 3
    ins, outs, held, sems = refs[:count], refs[count:2 * count], refs[2 * count:3 * count], refs[-1]
    loads = [pltpu.make_async_copy(ins[k], held[k], sems.at[0, k]) for k in range(count)]
    stores = [pltpu.make_async_copy(held[k], outs[k], sems.at[1, k]) for k in range(count)]
    for load in loads:
        load.start()
    for load, store in zip(loads, stores):
        load.wait()
        store.start()
    for store in stores:
        store.wait()


HBM = pl.BlockSpec(memory_space=pltpu.HBM)
LIMIT = 60 * 1024 * 1024


def per_device(sp, tp, hidden, value_weight, key_vecs, queries, decay_pre, decay_rate, cotangent):
    length, features = hidden.shape
    heads = decay_rate.shape[0]
    state = key_vecs.shape[2]
    columns = value_weight.shape[1]
    ny = inner_size(sp)
    nz = sp // ny
    tiles = columns // LANES
    groups = tiles
    pack = tiles // groups
    rw = state // ny
    pr = pack * rw // nz
    rows = features // sp
    own = length // tp
    halves = 2 if tp % 2 == 0 else 1
    nx = tp // halves
    far = nz // 2
    steps = 2
    vm = pltpu.VMEM
    dma = pltpu.SemaphoreType.DMA
    outs = pl.pallas_call(
        functools.partial(mixer_kernel, ny, nz, tp),
        out_shape=(
            jax.ShapeDtypeStruct((length, state), BF16),
            jax.ShapeDtypeStruct((length, state), BF16),
            jax.ShapeDtypeStruct((heads, length), F32),
            jax.ShapeDtypeStruct((own, features), BF16),
            jax.ShapeDtypeStruct((rows, columns), F32),
        ),
        in_specs=[HBM] * 7,
        out_specs=(HBM,) * 5,
        scratch_shapes=[
            vm((length, state), BF16),
            vm((length, state), BF16),
            vm((heads, length), F32),
            vm((own, features), BF16),
            vm((rows, columns), F32),
            vm((length, features), BF16),
            vm((features, columns), BF16),
            vm((length, state), BF16),
            vm((length, state), BF16),
            vm((heads, length), F32),
            vm((1, heads), F32),
            vm((columns, length), BF16),
            vm((length, columns), BF16),
            vm((length, columns), F32),
            vm((length, columns), F32),
            vm((length, columns), F32),
            vm((heads, length, length), F32),
            vm((tiles, length, LANES), F32),
            vm((length, columns), BF16),
            vm((length, columns), F32),
            vm((heads, length), F32),
            vm((length, heads), F32),
            vm((length, state), F32),
            vm((length, state), F32),
            vm((2, groups, ny, pack * rw, LANES), F32),
            vm((SUB, LANES), F32),
            vm((2, groups, ny, pack * rw, LANES), F32),
            vm((ny, SUB, LANES), F32),
            vm((2, groups, nz, -(-(pr + 1) // SUB) * SUB, LANES), F32),
            vm((2, groups, nz, -(-(pr + 1) // SUB) * SUB, LANES), F32),
            vm((2, groups, nz, pr, LANES), F32),
            vm((2, groups, nz, pr, LANES), F32),
            vm((2, groups, pack * rw, LANES), F32),
            vm((2, groups, ny, pack * rw, LANES), F32),
            vm((2, groups, ny, pack * rw, LANES), F32),
            vm((ny, nz, rows, length), F32),
            vm((ny, nz, rows, length), F32),
            vm((nz, rows, ny * length), BF16),
            vm((ny, tiles, length, LANES), F32),
            vm((tiles, nz, rows, LANES), F32),
            vm((2, tiles, far, rows, LANES), F32),
            vm((halves, nx, own, features), F32),
            vm((nx, own, features), F32),
            vm((nx, own, features), F32),
            vm((nx, own, features), F32),
            dma((6,)), dma((steps,)),
            dma, dma,
            dma, dma((groups + 1,)),
            dma, dma((groups + 1,)),
            dma, dma((groups + 1,)),
            dma, dma((groups + 1,)),
            dma, dma,
            dma, dma,
            dma, dma((tiles,)),
            dma, dma((tiles * (nz - 1) - (3 * 2 if nz == 8 else 0),)),
            dma, dma,
            dma, dma,
            dma((5,)),
        ],
        compiler_params=pltpu.CompilerParams(collective_id=0, has_side_effects=True, vmem_limit_bytes=LIMIT),
        name="mixer_backward",
    )(
        hidden, value_weight, key_vecs.reshape(length, state), queries.reshape(length, state), decay_pre.T,
        decay_rate.reshape(1, heads), cotangent.reshape(length, columns).T,
    )
    gk, gq, gd, gh, gw = pl.pallas_call(
        finish_kernel,
        out_shape=tuple(jax.ShapeDtypeStruct(o.shape, o.dtype) for o in outs),
        in_specs=[HBM] * 5,
        out_specs=(HBM,) * 5,
        scratch_shapes=[vm(o.shape, o.dtype) for o in outs] + [dma((2, 5))],
        compiler_params=pltpu.CompilerParams(vmem_limit_bytes=LIMIT),
        name="write_out",
    )(*outs)
    return gk.reshape(key_vecs.shape), gq.reshape(key_vecs.shape), gd.T, gh, gw


def solution(mesh):
    return jax.shard_map(
        functools.partial(per_device, mesh.shape["sp"], mesh.shape["tp"]),
        mesh=mesh,
        in_specs=(
            P("sp", None),
            P(None, "tp"),
            P("sp", "tp", None),
            P("sp", "tp", None),
            P("sp", "tp"),
            P("tp"),
            P("sp", "tp", None),
        ),
        out_specs=(
            P("sp", "tp", None),
            P("sp", "tp", None),
            P("sp", "tp"),
            P(("sp", "tp"), None),
            P("sp", "tp"),
        ),
        check_vma=False,
    )
```

```python
import functools

import jax
import jax.numpy as jnp
from jax import lax
from jax.experimental import pallas as pl
from jax.experimental.pallas import tpu as pltpu
from jax.sharding import PartitionSpec as P

MESH = pl.DeviceIdType.MESH
F32 = jnp.float32
BF16 = jnp.bfloat16
HIGH = lax.Precision.HIGHEST
LANES = 128
SUB = 8


def inner_size(count):
    size = 1
    while size * size * 4 <= count:
        size *= 2
    while count % size:
        size -= 1
    return size


def remote(src, dst, send, recv, axis, index):
    return pltpu.make_async_remote_copy(
        src_ref=src, dst_ref=dst, send_sem=send, recv_sem=recv, device_id={axis: index}, device_id_type=MESH
    )


def nn(a, b, precision=None):
    return jnp.dot(a, b, preferred_element_type=F32, precision=precision)


def nt(a, b, precision=None):
    return lax.dot_general(a, b, (((1,), (1,)), ((), ())), preferred_element_type=F32, precision=precision)


def split(x):
    hi = x.astype(BF16)
    return hi, (x - hi.astype(F32)).astype(BF16)


def mixer_kernel(ny, nz, ntp, hid_hbm, w_hbm, key_hbm, qry_hbm, pre_hbm, rate_hbm, cot_hbm,
                 gk_out, gq_out, gd_out, gh_out, gw_out,
                 gk_ref, gq_ref, gd_ref, gh_ref, gw_ref, hid, wt, key, qry, pre, rate_ref, cott, cot,
                 ecot, tend, xval, damp, gvloc, gvb, kgs, rows8, cols8, gkl, gql,
                 sbuf, decb, ybuf, ydec, tz, zbuf, cz, zcar, crow, ob, scr, ht, hg, hcol,
                 gath, part, ring, ghp, pland, red, xland,
                 insem, wsem, dsend, drecv, ysend, yrecv, tsend, trecv, csend, crecv, osend, orecv,
                 hsend, hrecv, fsend, frecv, gsend, grecv, rsend, rrecv, psend, precv, xsend, xrecv, outsem):
    me = lax.axis_index("sp")
    mine = lax.axis_index("tp")
    z, y = me // ny, me % ny
    length, features = hid.shape
    heads = pre.shape[0]
    columns = cot.shape[1]
    width = columns // heads
    tiles = columns // LANES
    per = LANES // width
    state = key.shape[1]
    groups = sbuf.shape[1]
    pack = tiles // groups
    rw = state // ny
    pr = pack * rw // nz
    rows = gw_ref.shape[0]
    own = gh_ref.shape[0]
    halves = 2 if ntp % 2 == 0 else 1
    core, x, nx = mine % halves, mine // halves, ntp // halves
    partner = mine + 1 - 2 * core
    hz = nz // ntp
    steps = wsem.shape[0]
    depth = features // steps
    ydev = [z * ny + (y + dy) % ny for dy in range(ny)]
    zdev = [((z + dz) % nz) * ny + y for dz in range(nz)]

    barrier = pltpu.get_barrier_semaphore()
    for dev in [zdev[dz] for dz in sorted(range(1, nz), key=lambda dz: -min(dz, nz - dz))] + ydev[1:]:
        pl.semaphore_signal(barrier, inc=1, device_id={"sp": dev}, device_id_type=MESH)
    for dt in range(1, ntp):
        pl.semaphore_signal(barrier, inc=1, device_id={"tp": (mine + dt) % ntp}, device_id_type=MESH)

    small = [
        pltpu.make_async_copy(pre_hbm, pre, insem.at[0]),
        pltpu.make_async_copy(rate_hbm, rate_ref, insem.at[4]),
        pltpu.make_async_copy(qry_hbm, qry, insem.at[1]),
        pltpu.make_async_copy(cot_hbm, cott, insem.at[2]),
        pltpu.make_async_copy(key_hbm, key, insem.at[3]),
    ]
    for copy in small:
        copy.start()
    wcopies = []
    for k in range(steps):
        at = pl.ds(k * depth, depth)
        wcopies.append(pltpu.make_async_copy(w_hbm.at[at, :], wt.at[at, :], wsem.at[k]))
    hload = pltpu.make_async_copy(hid_hbm, hid, insem.at[5])
    hload.start()
    for copy in wcopies:
        copy.start()

    outs = [
        pltpu.make_async_copy(gk_ref, gk_out, outsem.at[0]),
        pltpu.make_async_copy(gq_ref, gq_out, outsem.at[1]),
        pltpu.make_async_copy(gd_ref, gd_out, outsem.at[2]),
        pltpu.make_async_copy(gh_ref, gh_out, outsem.at[3]),
    ]
    for c in range(tiles):
        at = pl.ds(c * LANES, LANES)
        outs.append(pltpu.make_async_copy(gw_ref.at[:, at], gw_out.at[:, at], outsem.at[4]))

    def dcopy(dy, arrive=False):
        slot = (y + dy) % ny if arrive else y
        return remote(decb, ydec.at[slot], dsend, drecv, "sp", ydev[dy])

    def ycopy(m, g, dy):
        there = (y + dy) % ny
        return remote(sbuf.at[m, g, there], ybuf.at[m, g, y], ysend, yrecv.at[g + m * (groups - g)], "sp", ydev[dy])

    def tcopy(m, g, dz):
        there = (z + dz) % nz
        return remote(tz.at[m, g, there], zbuf.at[m, g, z], tsend, trecv.at[g + m * (groups - g)], "sp", zdev[dz])

    def ccopy(m, g, dz):
        there = (z + dz) % nz
        return remote(cz.at[m, g, there], zcar.at[m, g, z], csend, crecv.at[g + m * (groups - g)], "sp", zdev[dz])

    def ocopy(m, g, dy):
        there = (y + dy) % ny
        return remote(ob.at[m, g, there], scr.at[m, g, y], osend, orecv.at[g + m * (groups - g)], "sp", ydev[dy])

    def section(k):
        return pl.ds(pl.multiple_of(k * hz, hz), hz)

    def hcopy(dy, arrive=False):
        there = (y + dy) % ny
        slot = there if arrive else y
        return remote(
            ht.at[there, section(mine)], hg.at[slot, section(mine)], hsend, hrecv, "sp", ydev[dy]
        )

    def share(dy, dt, arrive=False):
        there = (y + dy) % ny
        peer = (mine + dt) % ntp
        which = peer if arrive else mine
        block = hg.at[there, section(which)]
        return remote(block, block, fsend, frecv, "tp", peer)

    def gcopy(c, dy, arrive=False):
        there = (y + dy) % ny
        slot = there if arrive else y
        return remote(gath.at[slot, c], gath.at[slot, c], gsend, grecv.at[c], "sp", ydev[dy])

    def pair():
        return remote(ghp.at[1 - core], pland, psend, precv, "tp", partner)

    def xcopy(dx, arrive=False):
        there = (x + dx) % nx
        slot = there if arrive else x
        return remote(red.at[there], xland.at[slot], xsend, xrecv, "tp", there * halves + core)

    def reach(c, d):
        far = nz // 2
        return far if (c + d) % 2 == 0 else nz - 1 - far

    def fast(c):
        return nz == 8 and c >= tiles - 2

    def ahead(k, d):
        return (z + k) % nz if d == 0 else (z + nz - k) % nz

    def rcopy(c, d, j):
        src = part.at[c, ahead(reach(c, d), d)] if j == 0 else ring.at[d, c, j - 1]
        return remote(
            src, ring.at[d, c, j], rsend, rrecv.at[slot_at(c, d, j)], "sp", zdev[1] if d == 0 else zdev[nz - 1]
        )

    def scopy(c, d, j):
        src, hops = (part.at[c, ahead(j + 2, d)], j + 1) if j < 3 else (ring.at[d, c, 0], 1)
        return remote(
            src, ring.at[d, c, j], rsend, rrecv.at[slot_at(c, d, j)], "sp", zdev[hops if d == 0 else nz - hops]
        )

    def slots(c, d):
        if fast(c):
            return tuple(range(reach(c, d) - 1)) + (3,)
        return tuple(range(reach(c, d)))

    def step_of(c, j):
        return j // 3 if fast(c) else j

    ring_slots = sorted({(c, d, step_of(c, j)) for c in range(tiles) for d in range(2) for j in slots(c, d)})

    def slot_at(c, d, j):
        return ring_slots.index((c, d, step_of(c, j)))

    def bulk(ref, send, recv):
        return remote(ref, ref, send, recv, "sp", ydev[1])

    row_at = lax.broadcasted_iota(jnp.int32, (length, length), 0)
    col_at = lax.broadcasted_iota(jnp.int32, (length, length), 1)
    eye = (row_at == col_at).astype(BF16)
    seg = (
        lax.broadcasted_iota(jnp.int32, (heads, columns), 1) // width
        == lax.broadcasted_iota(jnp.int32, (heads, columns), 0)
    ).astype(F32)
    lane = lax.broadcasted_iota(jnp.int32, (length, LANES), 1) // width

    def tile(q):
        return slice(q * LANES, (q + 1) * LANES)

    same = (
        lax.broadcasted_iota(jnp.int32, (heads, heads), 0) == lax.broadcasted_iota(jnp.int32, (heads, heads), 1)
    ).astype(F32)
    small[0].wait()
    small[1].wait()
    p = pre[...]
    rate = nt(same, jnp.broadcast_to(rate_ref[...], (heads, heads)), HIGH)[:, :1]
    log_decay = -rate * (jnp.maximum(p, 0.0) + jnp.log1p(jnp.exp(-jnp.abs(p))))
    lower = (row_at >= col_at).astype(F32)
    cum = nt(lower, log_decay, HIGH)
    cumt = nt(log_decay, lower, HIGH)
    cumx = nn(cum, seg, HIGH)
    totx = cumx[length - 1:length]
    decx = jnp.exp(totx)
    small[2].wait()
    small[3].wait()
    for q in range(tiles):
        cot[:, tile(q)] = nt(eye, cott[tile(q), :]).astype(BF16)
    ec = jnp.exp(cumx) * cot[...].astype(F32)
    ecot[...] = ec
    qryt = nt(eye, qry[...]).astype(BF16)
    hi, lo = split(ec)
    pull = nn(qryt, hi) + nn(qryt, lo)
    def spread(m, whole):
        for g in range(groups):
            for yy in range(ny):
                for i in range(pack):
                    sbuf[m, g, yy, i * rw:(i + 1) * rw] = whole[yy * rw:(yy + 1) * rw, tile(g * pack + i)]

    spread(0, pull)
    for q in range(tiles):
        decb[q:q + 1, :] = decx[:, tile(q)]

    with jax.named_scope("barrier"):
        pl.semaphore_wait(barrier, ny - 1 + nz - 1 + ntp - 1)
    for dy in range(1, ny):
        dcopy(dy).start()
    for g in range(groups):
        for dy in range(1, ny):
            ycopy(0, g, dy).start()
    ydec[y] = decb[...]
    ybuf[0, :, y] = sbuf[0, :, y]

    hload.wait()
    for b in range(features // LANES):
        block = nt(eye, hid[:, tile(b)])
        for i in range(LANES // rows):
            owner = b * LANES // rows + i
            ht[owner % ny, owner // ny] = block[i * rows:(i + 1) * rows]
    with jax.named_scope("send_h"):
        for dy in range(1, ny):
            hcopy(dy).start()
    tend[...] = jnp.exp(totx - cumx)
    small[4].wait()
    values = jnp.zeros((length, columns), F32)
    for k in range(steps):
        wcopies[k].wait()
        values = values + nn(hid[:, k * depth:(k + 1) * depth], wt[k * depth:(k + 1) * depth, :])
    vals = values.astype(BF16)
    xv = tend[...] * vals.astype(F32)
    xval[...] = xv
    keyt = nt(eye, key[...]).astype(BF16)
    hi, lo = split(xv)
    push = nn(keyt, hi) + nn(keyt, lo)
    spread(1, push)
    with jax.named_scope("send_y1"):
        for g in range(groups):
            for dy in range(1, ny):
                ycopy(1, g, dy).start()
    ybuf[1, :, y] = sbuf[1, :, y]

    hcol[:, :, pl.ds(pl.multiple_of(y * length, LANES), length)] = ht[y].astype(BF16)

    def scan_order(m, count):
        return list(range(count)) if m == 1 else list(reversed(range(count)))

    def stage_y(m, g):
        if m == 0 and g == 0:
            bulk(ydec.at[:ny - 1], dsend, drecv).wait_recv()
        if m == 0:
            bulk(ybuf.at[0, g, :ny - 1], ysend, yrecv.at[g]).wait_recv()
        elif g == 0:
            bulk(ybuf.at[1, :, :ny - 1], ysend, yrecv.at[groups]).wait_recv()
        order = scan_order(m, ny)
        for i in range(pack):
            q, at = g * pack + i, slice(i * rw, (i + 1) * rw)
            run = ybuf[m, g, order[0], at]
            for yy in order[1:]:
                run = ydec[yy, q:q + 1] * run + ybuf[m, g, yy, at]
            prod = ydec[0, q:q + 1]
            for yy in range(1, ny):
                prod = prod * ydec[yy, q:q + 1]
            for k in range(rw // pr):
                tz[m, g, i * (rw // pr) + k, :pr] = run[k * pr:(k + 1) * pr]
                tz[m, g, i * (rw // pr) + k, pr:pr + 1] = prod
        for dz in sorted(range(1, nz), key=lambda dz: -min(dz, nz - dz)):
            tcopy(m, g, dz).start()
        zbuf[m, g, z] = tz[m, g, z]

    def stage_z(m, g):
        if m == 0:
            bulk(zbuf.at[0, g, :nz - 1], tsend, trecv.at[g]).wait_recv()
        elif g == 0:
            bulk(zbuf.at[1, :, :nz - 1], tsend, trecv.at[groups]).wait_recv()
        run = jnp.zeros((pr, LANES), F32)
        for zz in scan_order(m, nz):
            cz[m, g, zz] = run
            run = zbuf[m, g, zz, pr:pr + 1] * run + zbuf[m, g, zz, :pr]
        for dz in sorted(range(1, nz), key=lambda dz: -min(dz, nz - dz)):
            ccopy(m, g, dz).start()
        zcar[m, g, z] = cz[m, g, z]

    def stage_c(m, g):
        if m == 0:
            bulk(zcar.at[0, g, :nz - 1], csend, crecv.at[g]).wait_recv()
        elif g == 0:
            bulk(zcar.at[1, :, :nz - 1], csend, crecv.at[groups]).wait_recv()
        for k in range(nz):
            crow[m, g, k * pr:(k + 1) * pr] = zcar[m, g, k]
        carry = crow[m, g]
        for i in range(pack):
            q, at = g * pack + i, slice(i * rw, (i + 1) * rw)
            now = carry[at]
            for yy in scan_order(m, ny):
                ob[m, g, yy, at] = now
                now = ydec[yy, q:q + 1] * now + ybuf[m, g, yy, at]
        for dy in sorted(range(1, ny), key=lambda dy: -min(dy, ny - dy)):
            ocopy(m, g, dy).start()
        scr[m, g, y] = ob[m, g, y]

    def stage(name, work, m):
        for g in range(groups):
            with jax.named_scope(f"{name}{m}{g}"):
                work(m, g)

    def state_tile(m, q):
        g, i = q // pack, q % pack
        return scr[m, g, :, i * rw:(i + 1) * rw].reshape(state, LANES)

    stage("stage_y", stage_y, 0)

    causal = row_at <= col_at
    scores = nt(key[...], qry[...])
    for q in range(tiles):
        lefts, rights = [], []
        ct = cot[:, tile(q)]
        for i in range(per):
            h = q * per + i
            across = cumt[h:h + 1, :] - cum[:, h:h + 1]
            dm = jnp.where(causal, jnp.exp(jnp.where(causal, across, 0.0)), 0.0)
            damp[h] = dm
            lefts.extend(split(scores * dm))
            masked = jnp.where(lane == i, ct, jnp.zeros_like(ct))
            rights.extend([masked, masked])
        gvloc[q] = nn(jnp.concatenate(lefts, axis=1), jnp.concatenate(rights, axis=0))

    with jax.named_scope("hid_y"):
        bulk(hg.at[:ny - 1, :hz], hsend, hrecv).wait_recv()
        for dt in range(1, ntp):
            for dy in range(1, ny):
                share(dy, dt).start()

    stage("stage_z", stage_z, 0)

    dsum = jnp.zeros((length, length), F32)
    for q in range(tiles):
        vt = vals[:, tile(q)]
        both = nt(
            jnp.concatenate([jnp.where(lane == i, vt, jnp.zeros_like(vt)) for i in range(per)], axis=0),
            cot[:, tile(q)],
        )
        for i in range(per):
            h = q * per + i
            ds = both[i * length:(i + 1) * length] * damp[h]
            flux = ds * scores
            dsum = dsum + ds
            rows8[h:h + 1, :] = jnp.sum(flux, axis=0, keepdims=True)
            cols8[:, h:h + 1] = jnp.sum(flux, axis=1, keepdims=True)

    stage("stage_c", stage_c, 0)

    stage("stage_y", stage_y, 1)

    hi, lo = split(dsum)
    gkl[...] = nn(hi, qry[...]) + nn(lo, qry[...])
    hi, lo = split(dsum.T)
    gql[...] = nn(hi, key[...]) + nn(lo, key[...])
    for g in range(groups):
        with jax.named_scope(f"wait_o0{g}"):
            bulk(scr.at[0, g, :ny - 1], osend, orecv.at[g]).wait_recv()
        for q in range(g * pack, (g + 1) * pack):
            hi, lo = split(state_tile(0, q))
            kg = nn(key[...], hi) + nn(key[...], lo)
            kgs[:, tile(q)] = kg
            gb = (gvloc[q] + tend[:, tile(q)] * kg).astype(BF16)
            gvb[:, tile(q)] = gb
            gath[y, q] = gb.astype(F32)
            for dy in sorted(range(1, ny), key=lambda dy: -min(dy, ny - dy)):
                gcopy(q, dy).start()

    stage("stage_z", stage_z, 1)

    def columns_in():
        if ntp > 1:
            bulk(hg.at[:ny - 1, :nz - hz], fsend, frecv).wait_recv()
        for dy in range(1, ny):
            there = (y + dy) % ny
            hcol[:, :, pl.ds(pl.multiple_of(there * length, LANES), length)] = hg[there].astype(BF16)

    def multiply(c):
        bulk(gath.at[:ny - 1, c], gsend, grecv.at[c]).wait_recv()
        block = gath[:, c].reshape(ny * length, LANES).astype(BF16)
        part[c] = nn(hcol[...].reshape(nz * rows, ny * length), block).reshape(nz, rows, LANES)
        for d in range(2):
            if fast(c):
                for j in reversed(range(reach(c, d) - 1)):
                    scopy(c, d, j).start()
            elif reach(c, d) > 0:
                rcopy(c, d, 0).start()

    def hop(c, d, j):
        rcopy(c, d, j).wait_recv()
        left = reach(c, d) - 1 - j
        if left > 0:
            ring[d, c, j] = ring[d, c, j] + part[c, ahead(left, d)]
            rcopy(c, d, j + 1).start()

    def step(c, d, j):
        if j == 3:
            scopy(c, d, 3).wait_recv()
        else:
            count = reach(c, d) - 1
            bulk(ring.at[d, c, :count], rsend, rrecv.at[slot_at(c, d, 0)]).wait_recv()
            total = part[c, ahead(1, d)]
            for k in range(count):
                total = total + ring[d, c, k]
            ring[d, c, 0] = total
            scopy(c, d, 3).start()

    def total_weight(c):
        total = part[c, z]
        for d in range(2):
            if fast(c):
                total = total + ring[d, c, 3]
            elif reach(c, d) > 0:
                total = total + ring[d, c, reach(c, d) - 1]
        gw_ref[:, tile(c)] = total
        outs[4 + c].start()

    def project():
        block = nt(gvb[...], wt[...])
        for t in range(ntp):
            ghp[t % halves, t // halves] = block[t * own:(t + 1) * own]
        if halves == 2:
            pair().start()

    def pairs():
        if halves == 2:
            pair().wait_recv()
            red[...] = ghp[core] + pland[...]
        else:
            red[...] = ghp[0]
        for dx in range(1, nx):
            xcopy(dx).start()

    def key_grads():
        gk = gkl[...]
        pulled = []
        for q in range(tiles):
            sgh, sgl = split(state_tile(0, q))
            xq = xval[:, tile(q)]
            xh, xl = split(xq)
            gk = gk + (nt(xh, sgh) + nt(xl, sgh) + nt(xh, sgl))
            pulled.append(xq * kgs[:, tile(q)])
        gk_ref[...] = gk.astype(BF16)
        outs[0].start()
        prefix_in = nt(seg, jnp.concatenate(pulled, axis=1), HIGH)
        gd_ref[...] = nn(prefix_in, (row_at < col_at).astype(F32), HIGH)

    def query_grads():
        with jax.named_scope("wait_o1"):
            bulk(scr.at[1, :, :ny - 1], osend, orecv.at[groups]).wait_recv()
        gq = gql[...]
        into, through = [], []
        for q in range(tiles):
            si, sg = state_tile(1, q), state_tile(0, q)
            sih, sil = split(si)
            eq = ecot[:, tile(q)]
            eh, el = split(eq)
            gq = gq + (nt(eh, sih) + nt(el, sih) + nt(eh, sil))
            into.append(eq * (nn(qry[...], sih) + nn(qry[...], sil)))
            through.append(jnp.sum(si * sg, axis=0, keepdims=True))
        gq_ref[...] = gq.astype(BF16)
        outs[1].start()
        suffix_in = nt(seg, jnp.concatenate(into, axis=1), HIGH) - nt(same, cols8[...], HIGH) + rows8[...]
        crossing = nt(seg, jnp.broadcast_to(decx * jnp.concatenate(through, axis=1), (SUB, columns)), HIGH)[:, :1]
        total = nn(suffix_in, lower, HIGH) + gd_ref[...] + crossing
        gd_ref[...] = total * -rate * (1.0 / (1.0 + jnp.exp(-p)))
        outs[2].start()

    def total_hidden():
        total = red[x]
        if nx > 1:
            bulk(xland.at[:nx - 1], xsend, xrecv).wait_recv()
        for dx in range(1, nx):
            total = total + xland[(x + dx) % nx]
        gh_ref[...] = total.astype(gh_ref.dtype)
        outs[3].start()

    def drain():
        bulk(ydec.at[:ny - 1], dsend, drecv).wait_send()
        bulk(ht.at[:ny - 1, :hz], hsend, hrecv).wait_send()
        if ntp > 1:
            bulk(hg.at[:ny - 1, :nz - hz], fsend, frecv).wait_send()
        bulk(sbuf.at[:, :, :ny - 1], ysend, yrecv.at[0]).wait_send()
        bulk(tz.at[:, :, :nz - 1], tsend, trecv.at[0]).wait_send()
        bulk(cz.at[:, :, :nz - 1], csend, crecv.at[0]).wait_send()
        bulk(ob.at[:, :, :ny - 1], osend, orecv.at[0]).wait_send()
        bulk(gath.at[:ny - 1], gsend, grecv.at[0]).wait_send()
        if halves == 2:
            pair().wait_send()

    tasks = [
        (1.0, "project", project), (1.9, "columns_in", columns_in),
        (6.1, "stage_c1", functools.partial(stage, "stage_c", stage_c, 1)), (3.0, "key_grads", key_grads),
        (9.6, "pairs", pairs), (17.9, "query_grads", query_grads), (18.0, "drain", drain),
        (18.2, "total_hidden", total_hidden),
    ]
    arrive = (4.5, 6.0, 8.5, 11.0)
    for c in range(tiles):
        ready = arrive[c % 4] + 7.0 * (c // 4)
        tasks.append((ready, f"multiply{c}", functools.partial(multiply, c)))
        last = ready
        for d in range(2):
            for j in slots(c, d):
                if fast(c) and j not in (0, 3):
                    continue
                if fast(c):
                    at = ready + (4.0 if j < 3 else 8.0) + 0.1 * d
                    tasks.append((at, f"step{c}{d}{j}", functools.partial(step, c, d, j)))
                else:
                    at = ready + 3.5 * (j + 1)
                    tasks.append((at, f"hop{c}{d}{j}", functools.partial(hop, c, d, j)))
                last = max(last, at)
        tasks.append((last + 0.01, f"total{c}", functools.partial(total_weight, c)))
    for _, name, task in sorted(tasks, key=lambda item: item[0]):
        with jax.named_scope(name):
            task()

    with jax.named_scope("drain_ring"):
        bulk(part.at[:, :nz - 1], rsend, rrecv.at[0]).wait_send()
        if nx > 1:
            bulk(red.at[:nx - 1], xsend, xrecv).wait_send()
    with jax.named_scope("outs"):
        for copy in outs[:4]:
            copy.wait()
        pltpu.make_async_copy(gw_ref, gw_out, outsem.at[4]).wait()


def finish_kernel(*refs):
    count = (len(refs) - 1) // 3
    ins, outs, held, sems = refs[:count], refs[count:2 * count], refs[2 * count:3 * count], refs[-1]
    moves = []
    for k in range(count):
        rows = ins[k].shape[0]
        parts = 4 if rows * ins[k].shape[1] > 20000 and rows % (16 * 4) == 0 else 1
        for i in range(parts):
            at = pl.ds(i * (rows // parts), rows // parts)
            n = len(moves)
            moves.append((
                pltpu.make_async_copy(ins[k].at[at], held[k].at[at], sems.at[0, n]),
                pltpu.make_async_copy(held[k].at[at], outs[k].at[at], sems.at[1, n]),
            ))
    for load, _ in moves:
        load.start()
    for load, store in moves:
        load.wait()
        store.start()
    for _, store in moves:
        store.wait()


HBM = pl.BlockSpec(memory_space=pltpu.HBM)
LIMIT = 60 * 1024 * 1024


def per_device(sp, tp, hidden, value_weight, key_vecs, queries, decay_pre, decay_rate, cotangent):
    length, features = hidden.shape
    heads = decay_rate.shape[0]
    state = key_vecs.shape[2]
    columns = value_weight.shape[1]
    ny = inner_size(sp)
    nz = sp // ny
    tiles = columns // LANES
    groups = tiles
    pack = tiles // groups
    rw = state // ny
    pr = pack * rw // nz
    rows = features // sp
    own = length // tp
    halves = 2 if tp % 2 == 0 else 1
    nx = tp // halves
    far = nz // 2
    steps = 2
    vm = pltpu.VMEM
    dma = pltpu.SemaphoreType.DMA
    outs = pl.pallas_call(
        functools.partial(mixer_kernel, ny, nz, tp),
        out_shape=(
            jax.ShapeDtypeStruct((length, state), BF16),
            jax.ShapeDtypeStruct((length, state), BF16),
            jax.ShapeDtypeStruct((heads, length), F32),
            jax.ShapeDtypeStruct((own, features), BF16),
            jax.ShapeDtypeStruct((rows, columns), F32),
        ),
        in_specs=[HBM] * 7,
        out_specs=(HBM,) * 5,
        scratch_shapes=[
            vm((length, state), BF16),
            vm((length, state), BF16),
            vm((heads, length), F32),
            vm((own, features), BF16),
            vm((rows, columns), F32),
            vm((length, features), BF16),
            vm((features, columns), BF16),
            vm((length, state), BF16),
            vm((length, state), BF16),
            vm((heads, length), F32),
            vm((1, heads), F32),
            vm((columns, length), BF16),
            vm((length, columns), BF16),
            vm((length, columns), F32),
            vm((length, columns), F32),
            vm((length, columns), F32),
            vm((heads, length, length), F32),
            vm((tiles, length, LANES), F32),
            vm((length, columns), BF16),
            vm((length, columns), F32),
            vm((heads, length), F32),
            vm((length, heads), F32),
            vm((length, state), F32),
            vm((length, state), F32),
            vm((2, groups, ny, pack * rw, LANES), F32),
            vm((SUB, LANES), F32),
            vm((2, groups, ny, pack * rw, LANES), F32),
            vm((ny, SUB, LANES), F32),
            vm((2, groups, nz, -(-(pr + 1) // SUB) * SUB, LANES), F32),
            vm((2, groups, nz, -(-(pr + 1) // SUB) * SUB, LANES), F32),
            vm((2, groups, nz, pr, LANES), F32),
            vm((2, groups, nz, pr, LANES), F32),
            vm((2, groups, pack * rw, LANES), F32),
            vm((2, groups, ny, pack * rw, LANES), F32),
            vm((2, groups, ny, pack * rw, LANES), F32),
            vm((ny, nz, rows, length), F32),
            vm((ny, nz, rows, length), F32),
            vm((nz, rows, ny * length), BF16),
            vm((ny, tiles, length, LANES), F32),
            vm((tiles, nz, rows, LANES), F32),
            vm((2, tiles, far, rows, LANES), F32),
            vm((halves, nx, own, features), F32),
            vm((nx, own, features), F32),
            vm((nx, own, features), F32),
            vm((nx, own, features), F32),
            dma((6,)), dma((steps,)),
            dma, dma,
            dma, dma((groups + 1,)),
            dma, dma((groups + 1,)),
            dma, dma((groups + 1,)),
            dma, dma((groups + 1,)),
            dma, dma,
            dma, dma,
            dma, dma((tiles,)),
            dma, dma((tiles * (nz - 1) - (3 * 2 if nz == 8 else 0),)),
            dma, dma,
            dma, dma,
            dma((5,)),
        ],
        compiler_params=pltpu.CompilerParams(collective_id=0, has_side_effects=True, vmem_limit_bytes=LIMIT),
        name="mixer_backward",
    )(
        hidden, value_weight, key_vecs.reshape(length, state), queries.reshape(length, state), decay_pre.T,
        decay_rate.reshape(1, heads), cotangent.reshape(length, columns).T,
    )
    gk, gq, gd, gh, gw = pl.pallas_call(
        finish_kernel,
        out_shape=tuple(jax.ShapeDtypeStruct(o.shape, o.dtype) for o in outs),
        in_specs=[HBM] * 5,
        out_specs=(HBM,) * 5,
        scratch_shapes=[vm(o.shape, o.dtype) for o in outs] + [dma((2, 8))],
        compiler_params=pltpu.CompilerParams(vmem_limit_bytes=LIMIT),
        name="write_out",
    )(*outs)
    return gk.reshape(key_vecs.shape), gq.reshape(key_vecs.shape), gd.T, gh, gw


def solution(mesh):
    return jax.shard_map(
        functools.partial(per_device, mesh.shape["sp"], mesh.shape["tp"]),
        mesh=mesh,
        in_specs=(
            P("sp", None),
            P(None, "tp"),
            P("sp", "tp", None),
            P("sp", "tp", None),
            P("sp", "tp"),
            P("tp"),
            P("sp", "tp", None),
        ),
        out_specs=(
            P("sp", "tp", None),
            P("sp", "tp", None),
            P("sp", "tp"),
            P(("sp", "tp"), None),
            P("sp", "tp"),
        ),
        check_vma=False,
    )
```
